32 devices in a mesh: ep: 8 (over z, core), tp: 4 (over y, x).
Axes of the slice: x: 2, y: 2, z: 4, core: 2. Of those that a mesh axis runs over, the one named last changes fastest.
Arguments:
- tokens: bfloat16 [256, 4096], P('ep'), may hold values from -6 to 6
- recur_state: float32 [256, 4096], P('ep', 'tp'), may hold values from -6 to 6
- conv_state: bfloat16 [256, 3, 4096], P('ep', None, 'tp'), may hold values from -6 to 6
- mix_gain: float32 [4096], replicated, may hold values from 0.1 to 1.9
- in_weight: bfloat16 [4096, 4096], P('ep', 'tp'), may hold values from -0.09375 to 0.09375
- gate_weight: bfloat16 [4096, 4096], P('ep', 'tp'), may hold values from -0.09375 to 0.09375
- conv_taps: float32 [4, 4096], P(None, 'tp'), may hold values from -3 to 3
- recur_gate_blocks: bfloat16 [64, 64, 64], P('tp'), may hold values from -0.75 to 0.75
- input_gate_blocks: bfloat16 [64, 64, 64], P('tp'), may hold values from -0.75 to 0.75
- decay_rate: float32 [4096], P('tp'), may hold values from 0.01 to 0.4
- out_weight: bfloat16 [4096, 4096], P('tp', 'ep'), may hold values from -0.09375 to 0.09375
- ffn_gain: float32 [4096], replicated, may hold values from 0.1 to 1.9
- router_weight: bfloat16 [4096, 8], replicated, may hold values from -0.09375 to 0.09375
- routes: int32 [256, 2], P('ep'), may hold values from 0 to 7, as said below
- expert_gate: bfloat16 [8, 4096, 2048], P('ep', None, 'tp'), may hold values from -0.09375 to 0.09375
- expert_up: bfloat16 [8, 4096, 2048], P('ep', None, 'tp'), may hold values from -0.09375 to 0.09375
- expert_down: bfloat16 [8, 2048, 4096], P('ep', 'tp'), may hold values from -0.125 to 0.125
- dense_gate: bfloat16 [4096, 2048], P('ep', 'tp'), may hold values from -0.09375 to 0.09375
- dense_up: bfloat16 [4096, 2048], P('ep', 'tp'), may hold values from -0.09375 to 0.09375
- dense_down: bfloat16 [2048, 4096], P('tp', 'ep'), may hold values from -0.125 to 0.125
- branch_gate: bfloat16 [4096], replicated, may hold values from -0.09375 to 0.09375
Outputs:
- layer_out: bfloat16 [256, 4096], P('ep')
- new_state: float32 [256, 4096], P('ep', 'tp')
- new_conv_state: bfloat16 [256, 3, 4096], P('ep', None, 'tp')
The draws below stay inside these ranges and needn't reach their ends.
Inputs may be any that keep to these rules, and one draw needn't show every extreme that they name: `routes`: A row names two different experts of one group: both have the same e // 4. In the rows of one index of ep no expert is named more than 16 times, and in every draw some expert is named exactly 16 times by the rows of every index of ep.
All inputs are finite; a program needn't handle non-finite values.
Results may differ from the reference program's by a relative error of at most 0.023.
Values may be sent and summed in bfloat16 or wider, within the bound.
A program may use at most 64 MiB of HBM per device.

```python
import math
import jax
import jax.numpy as jnp
from jax import lax

D = 4096
D_A = 4096
BLOCK = 64
FF = 2048
FFD = 2048
CONV_W = 4
TOP_K = 2
E_PER_GROUP = 4
B_DEV = 32
B = 256
EXPERTS = 8
CAP = 16
H_A = 64
N_EP = 8
N_TP = 4


def draw_routes(key, part):
    group_count = EXPERTS // E_PER_GROUP
    group_tokens = 2 * CAP
    slot_count = group_count * group_tokens
    base_group = jax.random.randint(jax.random.fold_in(key, 11), (), 0, group_count)

    def one_block(block):
        block_key = jax.random.fold_in(key, 1000 + block)
        full_group = (block + base_group) % group_count
        scores = jax.random.randint(jax.random.fold_in(block_key, 1), (slot_count,), 0, 1 << 20)
        slot_index = jnp.arange(slot_count, dtype=jnp.int32)
        keyed = jnp.where(slot_index // group_tokens == full_group, 0, scores + 1) * slot_count + slot_index
        chosen = jnp.argsort(keyed)[:B_DEV]
        chosen = chosen[jax.random.permutation(jax.random.fold_in(block_key, 2), B_DEV)]
        group = chosen // group_tokens
        pair = chosen % group_tokens
        member_scores = jax.random.randint(jax.random.fold_in(block_key, 3), (group_count, E_PER_GROUP), 0, 1 << 20) * E_PER_GROUP + jnp.arange(E_PER_GROUP, dtype=jnp.int32)[None, :]
        members = jnp.argsort(member_scores, axis=1).astype(jnp.int32)
        first = members[group, 2 * pair % E_PER_GROUP]
        second = members[group, (2 * pair + 1) % E_PER_GROUP]
        return jnp.stack([group * E_PER_GROUP + first, group * E_PER_GROUP + second], axis=1).astype(jnp.int32)
    return jax.vmap(one_block)(jnp.arange(N_EP, dtype=jnp.int32)).reshape(N_EP * B_DEV, 2)


def block_levels(stream_key, dims, cuts, low, high):
    loudness = 1.0
    for axis_at, blocks in cuts:
        draws = jax.random.uniform(jax.random.fold_in(jax.random.fold_in(stream_key, 6), axis_at), (blocks,), jnp.float32, low / len(cuts), high / len(cuts))
        loudness = loudness * jnp.repeat(jnp.exp(draws), dims[axis_at] // blocks).reshape((-1,) + (1,) * (len(dims) - 1 - axis_at))
    return loudness


def normal_values(stream_key, shape, width, reach, split=(), held_as=jnp.bfloat16):
    entries = width * jax.random.normal(stream_key, shape, jnp.float32)
    if split:
        entries = entries * block_levels(stream_key, shape, split, -0.22, 0.18)
    return jnp.clip(entries, -reach, reach).astype(held_as)


def setup_inputs(seed: int = 0) -> dict:
    streams_of = jax.random.split(jax.random.key(seed), 22)
    tokens = normal_values(streams_of[0], (B, D), 1.0, 6.0, ((0, 8),))
    recur_state = normal_values(streams_of[1], (B, D_A), 1.0, 6.0, ((0, 8), (1, 4)), jnp.float32)
    conv_state = normal_values(streams_of[2], (B, CONV_W - 1, D_A), 1.0, 6.0, ((0, 8), (2, 4)))
    mix_gain = jnp.clip(1.0 + 0.18 * jax.random.normal(streams_of[3], (D,), jnp.float32), 0.1, 1.9)
    in_weight = normal_values(streams_of[4], (D, D_A), D ** -0.5, 0.09375, ((0, 8), (1, 4)))
    gate_weight = normal_values(streams_of[5], (D, D_A), D ** -0.5, 0.09375, ((0, 8), (1, 4)))
    conv_taps = normal_values(streams_of[6], (CONV_W, D_A), 0.5, 3.0, ((1, 4),), jnp.float32)
    recur_gate_blocks = normal_values(streams_of[7], (H_A, BLOCK, BLOCK), BLOCK ** -0.5, 0.75, ((0, 4),))
    input_gate_blocks = normal_values(streams_of[8], (H_A, BLOCK, BLOCK), BLOCK ** -0.5, 0.75, ((0, 4),))
    decay_rate = jnp.clip(jnp.exp(math.log(0.4) - 3.6888795 * jax.random.uniform(streams_of[9], (D_A,), jnp.float32) ** block_levels(streams_of[9], (D_A,), ((0, 4),), -0.2, 0.2)), 0.01, 0.4)
    out_weight = normal_values(streams_of[10], (D_A, D), D_A ** -0.5, 0.09375, ((0, 4), (1, 8)))
    ffn_gain = jnp.clip(1.0 + 0.18 * jax.random.normal(streams_of[11], (D,), jnp.float32), 0.1, 1.9)
    router_weight = normal_values(streams_of[12], (D, EXPERTS), D ** -0.5, 0.09375)
    routes = draw_routes(jax.random.fold_in(streams_of[21], 71), 0)
    expert_gate = normal_values(streams_of[14], (EXPERTS, D, FF), D ** -0.5, 0.09375, ((0, 8), (2, 4)))
    expert_up = normal_values(streams_of[15], (EXPERTS, D, FF), D ** -0.5, 0.09375, ((0, 8), (2, 4)))
    expert_down = normal_values(streams_of[16], (EXPERTS, FF, D), FF ** -0.5, 0.125, ((0, 8), (1, 4)))
    dense_gate = normal_values(streams_of[17], (D, FFD), D ** -0.5, 0.09375, ((0, 8), (1, 4)))
    dense_up = normal_values(streams_of[18], (D, FFD), D ** -0.5, 0.09375, ((0, 8), (1, 4)))
    dense_down = normal_values(streams_of[19], (FFD, D), FFD ** -0.5, 0.125, ((0, 4), (1, 8)))
    branch_gate = normal_values(streams_of[20], (D,), D ** -0.5, 0.09375)
    return dict(tokens=tokens, recur_state=recur_state, conv_state=conv_state, mix_gain=mix_gain, in_weight=in_weight, gate_weight=gate_weight, conv_taps=conv_taps, recur_gate_blocks=recur_gate_blocks, input_gate_blocks=input_gate_blocks, decay_rate=decay_rate, out_weight=out_weight, ffn_gain=ffn_gain, router_weight=router_weight, routes=routes, expert_gate=expert_gate, expert_up=expert_up, expert_down=expert_down, dense_gate=dense_gate, dense_up=dense_up, dense_down=dense_down, branch_gate=branch_gate)


epsilon = 1e-06
decay_scale = 8.0

def rms_scale(rows, gain):
    values = rows.astype(jnp.float32)
    inverse = lax.rsqrt(lax.optimization_barrier(jnp.mean(values * values, axis=-1, keepdims=True)) + epsilon)
    return (values * inverse * gain.astype(jnp.float32)).astype(jnp.bfloat16)

def grouped_product(left, right, groups):
    rows = left.shape[0]
    inner = left.shape[1] // groups
    parts = jnp.einsum('rtf,tfd->trd', left.astype(jnp.float32).reshape(rows, groups, inner), right.astype(jnp.float32).reshape(groups, inner, right.shape[1]))
    rounded = lax.optimization_barrier(parts.astype(jnp.bfloat16))
    return lax.optimization_barrier(jnp.sum(rounded.astype(jnp.float32), axis=0))

def slot_table(routes):
    pairs = routes.reshape(N_EP, B_DEV * TOP_K)
    expert_ids = jnp.arange(EXPERTS, dtype=jnp.int32)
    onehot = (pairs[:, :, None] == expert_ids[None, None, :]).astype(jnp.int32)
    before = jnp.cumsum(onehot, axis=1) - onehot
    rank = lax.optimization_barrier(jnp.sum(before * onehot, axis=2))
    return (pairs * CAP + rank).reshape(N_EP * B_DEV, TOP_K).astype(jnp.int32)

def reference(tokens, recur_state, conv_state, mix_gain, in_weight, gate_weight, conv_taps, recur_gate_blocks, input_gate_blocks, decay_rate, out_weight, ffn_gain, router_weight, routes, expert_gate, expert_up, expert_down, dense_gate, dense_up, dense_down, branch_gate):
    batch_rows = tokens.shape[0]
    normed = rms_scale(tokens, mix_gain)
    x_branch = jnp.dot(normed, in_weight, preferred_element_type=jnp.float32).astype(jnp.bfloat16)
    gate_branch = jnp.dot(normed, gate_weight, preferred_element_type=jnp.float32).astype(jnp.bfloat16)
    window = jnp.concatenate([conv_state, x_branch[:, None, :]], axis=1)
    conv_out = lax.optimization_barrier(jnp.sum(window.astype(jnp.float32) * conv_taps.astype(jnp.float32)[None], axis=1)).astype(jnp.bfloat16)
    new_conv_state = window[:, 1:, :]
    blocks = conv_out.astype(jnp.float32).reshape(batch_rows, H_A, BLOCK)
    recur_gate = jax.nn.sigmoid(jnp.einsum('bhi,hij->bhj', blocks, recur_gate_blocks.astype(jnp.float32)).reshape(batch_rows, D_A))
    input_gate = jax.nn.sigmoid(jnp.einsum('bhi,hij->bhj', blocks, input_gate_blocks.astype(jnp.float32)).reshape(batch_rows, D_A))
    log_decay = -decay_scale * recur_gate * decay_rate
    new_state = jnp.exp(log_decay) * recur_state + jnp.sqrt(-jnp.expm1(2.0 * log_decay)) * input_gate * conv_out.astype(jnp.float32)
    mixer_rows = (new_state * jax.nn.gelu(gate_branch.astype(jnp.float32))).astype(jnp.bfloat16)
    mixed = grouped_product(mixer_rows, out_weight, N_TP)
    resid = (tokens.astype(jnp.float32) + mixed).astype(jnp.bfloat16)
    normed_ffn = rms_scale(resid, ffn_gain)
    router_logits = jnp.dot(normed_ffn, router_weight, preferred_element_type=jnp.float32)
    picked = jnp.take_along_axis(router_logits, routes, axis=1)
    route_weight = jax.nn.sigmoid(picked - picked[:, ::-1]).astype(jnp.bfloat16)
    slots = slot_table(routes)
    global_token = jnp.arange(batch_rows, dtype=jnp.int32)
    source = global_token // B_DEV
    owner = jnp.full((N_EP, EXPERTS * CAP), -1, jnp.int32)
    owner = owner.at[jnp.repeat(source[:, None], TOP_K, axis=1), slots].set(jnp.repeat(global_token[:, None], TOP_K, axis=1))
    table = owner.reshape(N_EP, EXPERTS, CAP).transpose(1, 0, 2).reshape(EXPERTS, N_EP * CAP)

    def serve(item):
        token_index, gate_matrix, up_matrix, down_matrix = item
        valid = token_index >= 0
        rows = jnp.where(valid[:, None], normed_ffn[jnp.maximum(token_index, 0)], jnp.zeros((), jnp.bfloat16))
        first = jnp.dot(rows, gate_matrix, preferred_element_type=jnp.float32)
        second = jnp.dot(rows, up_matrix, preferred_element_type=jnp.float32)
        act = (jax.nn.silu(first) * second).astype(jnp.bfloat16)
        return grouped_product(act, down_matrix, N_TP).astype(jnp.bfloat16)
    expert_rows = lax.map(serve, (table, expert_gate, expert_up, expert_down))
    flat_rows = expert_rows.reshape(EXPERTS * N_EP * CAP, D)
    flat_index = slots // CAP * (N_EP * CAP) + source[:, None] * CAP + slots % CAP
    chosen = flat_rows[flat_index].astype(jnp.float32)
    moe = lax.optimization_barrier(jnp.sum(route_weight.astype(jnp.float32)[:, :, None] * chosen, axis=1))
    dense_first = jnp.dot(normed_ffn, dense_gate, preferred_element_type=jnp.float32)
    dense_second = jnp.dot(normed_ffn, dense_up, preferred_element_type=jnp.float32)
    dense_act = (jax.nn.silu(dense_first) * dense_second).astype(jnp.bfloat16)
    dense_sum = grouped_product(dense_act, dense_down, N_TP)
    branch_weight = jax.nn.sigmoid(jnp.dot(normed_ffn, branch_gate, preferred_element_type=jnp.float32))
    layer_out = (resid.astype(jnp.float32) + moe + branch_weight[:, None] * dense_sum).astype(jnp.bfloat16)
    return (layer_out, new_state, new_conv_state)
```

```python
import functools

import jax
import jax.numpy as jnp
from jax import lax
from jax.experimental import pallas as pl
from jax.experimental.pallas import tpu as pltpu
from jax.sharding import PartitionSpec as P

TOP_K = 2
LANES = 128
F32 = jnp.float32
BF16 = jnp.bfloat16


epsilon = 1e-06
decay_scale = 8.0


def rms_scale(rows, gain):
    values = rows.astype(jnp.float32)
    inverse = lax.rsqrt(jnp.mean(values * values, axis=-1, keepdims=True) + epsilon)
    return (values * inverse * gain).astype(jnp.bfloat16)


def on_device(
    tokens,
    recur_state,
    conv_state,
    mix_gain,
    in_weight,
    gate_weight,
    conv_taps,
    recur_gate_blocks,
    input_gate_blocks,
    decay_rate,
    out_weight,
    ffn_gain,
    router_weight,
    routes,
    expert_gate,
    expert_up,
    expert_down,
    dense_gate,
    dense_up,
    dense_down,
    branch_gate,
):
    batch_rows, width = tokens.shape
    channels = in_weight.shape[1]
    normed = rms_scale(tokens, mix_gain)
    arrived = lax.all_to_all(normed, "ep", split_axis=1, concat_axis=0, tiled=True)
    joined = jnp.concatenate([in_weight, gate_weight], axis=1)
    summed = lax.psum_scatter(
        jnp.dot(arrived, joined, preferred_element_type=jnp.float32).astype(jnp.bfloat16),
        "ep",
        scatter_dimension=0,
        tiled=True,
    ).astype(jnp.float32)
    x_sum, gate_sum = (summed[:, :channels], summed[:, channels:])
    x_branch = x_sum.astype(jnp.bfloat16)
    gate_branch = gate_sum.astype(jnp.bfloat16)
    window = jnp.concatenate([conv_state, x_branch[:, None, :]], axis=1)
    conv_out = jnp.sum(window.astype(jnp.float32) * conv_taps[None], axis=1).astype(jnp.bfloat16)
    new_conv_state = window[:, 1:, :]
    blocks = conv_out.reshape(batch_rows, recur_gate_blocks.shape[0], recur_gate_blocks.shape[1])
    recur_gate = jax.nn.sigmoid(
        jnp.einsum(
            "bhi,hij->bhj", blocks, recur_gate_blocks, preferred_element_type=jnp.float32
        ).reshape(batch_rows, channels)
    )
    input_gate = jax.nn.sigmoid(
        jnp.einsum(
            "bhi,hij->bhj", blocks, input_gate_blocks, preferred_element_type=jnp.float32
        ).reshape(batch_rows, channels)
    )
    log_decay = -decay_scale * recur_gate * decay_rate
    new_state = jnp.exp(log_decay) * recur_state + jnp.sqrt(
        -jnp.expm1(2.0 * log_decay)
    ) * input_gate * conv_out.astype(jnp.float32)
    mixer_rows = (new_state * jax.nn.gelu(gate_branch.astype(jnp.float32))).astype(jnp.bfloat16)
    mixer_part = jnp.dot(
        mixer_rows,
        lax.all_gather(out_weight, "ep", axis=1, tiled=True),
        preferred_element_type=jnp.float32,
    )
    resid = (
        tokens.astype(jnp.float32)
        + lax.psum(mixer_part.astype(jnp.bfloat16), "tp").astype(jnp.float32)
    ).astype(jnp.bfloat16)
    normed_ffn = rms_scale(resid, ffn_gain)
    router_logits = jnp.dot(normed_ffn, router_weight, preferred_element_type=jnp.float32)
    experts = router_logits.shape[1]
    expert_ids = lax.broadcasted_iota(jnp.int32, (batch_rows, TOP_K, experts), 2)
    picked = jnp.sum(
        jnp.where(routes[:, :, None] == expert_ids, router_logits[:, None, :], 0.0), axis=2
    )
    route_weight = jax.nn.sigmoid(picked - picked[:, ::-1]).astype(jnp.bfloat16)
    capacity = 2 * batch_rows * TOP_K // experts
    flat_ids = routes.reshape(batch_rows * TOP_K)
    onehot = (
        flat_ids[:, None] == lax.broadcasted_iota(jnp.int32, (batch_rows * TOP_K, experts), 1)
    ).astype(jnp.int32)
    rank = jnp.sum((jnp.cumsum(onehot, axis=0) - onehot) * onehot, axis=1)
    slot_of = (flat_ids * capacity + rank).reshape(batch_rows, TOP_K)
    slot_rows = lax.broadcasted_iota(jnp.int32, (experts * capacity, batch_rows), 0)
    slot_cols = lax.broadcasted_iota(jnp.int32, (batch_rows, experts * capacity), 1)
    dispatch = jnp.zeros((experts * capacity, batch_rows), jnp.bfloat16)
    combine = jnp.zeros((batch_rows, experts * capacity), jnp.bfloat16)
    for pick in range(TOP_K):
        dispatch = dispatch + (slot_rows == slot_of[None, :, pick]).astype(jnp.bfloat16)
        combine = combine + jnp.where(
            slot_cols == slot_of[:, pick : pick + 1],
            route_weight[:, pick : pick + 1],
            jnp.zeros((), jnp.bfloat16),
        )
    outgoing = (
        jnp.dot(dispatch, normed_ffn, preferred_element_type=jnp.float32)
        .astype(jnp.bfloat16)
        .reshape(experts, capacity, width)
    )
    gate_local = expert_gate[0]
    up_local = expert_up[0]
    down_local = expert_down[0]
    arrived_rows = lax.all_to_all(outgoing, "ep", split_axis=0, concat_axis=0, tiled=True)
    sources, items, features = arrived_rows.shape
    rows = arrived_rows.reshape(sources * items, features)
    first = jnp.dot(rows, gate_local, preferred_element_type=jnp.float32)
    second = jnp.dot(rows, up_local, preferred_element_type=jnp.float32)
    act = (jax.nn.silu(first) * second).astype(jnp.bfloat16)
    partial_value = jnp.dot(act, down_local, preferred_element_type=jnp.float32)
    total = lax.psum(partial_value.astype(jnp.bfloat16), "tp")
    returned = lax.all_to_all(
        total.reshape(sources, items, total.shape[1]), "ep", split_axis=0, concat_axis=0, tiled=True
    )
    moe = jnp.dot(
        combine,
        returned.reshape(experts * capacity, returned.shape[2]),
        preferred_element_type=jnp.float32,
    )
    dense_arrived = lax.all_to_all(normed_ffn, "ep", split_axis=1, concat_axis=0, tiled=True)
    dense_joined = jnp.concatenate([dense_gate, dense_up], axis=1)
    dense_summed = lax.psum_scatter(
        jnp.dot(dense_arrived, dense_joined, preferred_element_type=jnp.float32).astype(
            jnp.bfloat16
        ),
        "ep",
        scatter_dimension=0,
        tiled=True,
    ).astype(jnp.float32)
    dense_first = dense_summed[:, : dense_gate.shape[1]]
    dense_second = dense_summed[:, dense_gate.shape[1] :]
    dense_act = (jax.nn.silu(dense_first) * dense_second).astype(jnp.bfloat16)
    dense_part = jnp.dot(
        dense_act,
        lax.all_gather(dense_down, "ep", axis=1, tiled=True),
        preferred_element_type=jnp.float32,
    )
    branch_weight = jax.nn.sigmoid(
        jnp.dot(normed_ffn, branch_gate, preferred_element_type=jnp.float32)
    )
    dense_sum = lax.psum(dense_part.astype(jnp.bfloat16), "tp").astype(jnp.float32)
    layer_out = (resid.astype(jnp.float32) + moe + branch_weight[:, None] * dense_sum).astype(
        jnp.bfloat16
    )
    return (layer_out, new_state, new_conv_state)


def rcopy(src, dst, send, recv, ep, tp):
    return pltpu.make_async_remote_copy(
        src_ref=src,
        dst_ref=dst,
        send_sem=send,
        recv_sem=recv,
        device_id={"ep": ep, "tp": tp},
        device_id_type=pl.DeviceIdType.MESH,
    )


def dot(left, right):
    return jnp.dot(left, right, preferred_element_type=F32)


def layer_kernel(
    n, m, experts, tok_hbm, mg_hbm, fg_hbm, rt_hbm, st_hbm, cv_hbm, tap_hbm, rg_hbm, ig_hbm, dr_hbm,
    maps_hbm, iw_hbm, gw_hbm, ow_hbm, dg_hbm, du_hbm, dd_hbm, eg, eu, ed, out, st_out, cv_out,
    toks, mgain, gain, rts, state, cvs, taps, rgb, igb, decay, maps, iw, gw, ow, dg, du, dd, wg, wu, wd,
    narr, psend, precv, pkeep, rsend, rrecv, pre, bd, mask, masks, mr, mall, osend, orecv, full, nfm,
    square, lacc, accg, accu, act, dpsend, dprecv, dkeep, drsend, drrecv, dact, dall,
    ysend, yrecv, kq, xsend, xrecv, pbuf, zsend, zrecv, fblk, fin,
    lw, ts, tr, ks, kr, s2, r2, s3, r3, as_, ar, bs, br, os_, or_, zs_, zr, xs, xr, ms, mrv,
    s4, r4, s5, r5, cs, cr, es, er, ys, yr, hs_, hr, gs, gr, fs, fr,
):
    me, tp = lax.axis_index("ep"), lax.axis_index("tp")
    zs = n // 2
    z, c = me // 2, me % 2
    mate = 2 * z + 1 - c
    side = z // 2
    inner = lax.rem(z, 3) != 0
    outer = lax.rem(z, 3) == 0
    rows, width = out.shape
    q, ch = iw.shape
    g = q // m
    half = n * rows // 2
    h = dg.shape[1]

    def zp(k):
        return (z, z + 1 - 2 * lax.rem(z, 2), lax.rem(z + 2, zs), zs - 1 - z)[k]

    def tx(k):
        return (tp, tp + 1 - 2 * lax.rem(tp, 2), lax.rem(tp + 2, m), m - 1 - tp)[k]

    def lanes(e, size):
        return pl.ds(pl.multiple_of(e * size, LANES), size)

    count = [0]

    def load(src, dst):
        cp = pltpu.make_async_copy(src, dst, lw.at[count[0]])
        count[0] += 1
        cp.start()
        return cp

    sends = []

    def send(*args):
        cp = rcopy(*args)
        cp.start()
        sends.append(cp)

    def arrive(buf, sem):
        rcopy(buf, buf, sem, sem, mate, tp).wait_recv()

    ltok = load(tok_hbm, toks)
    lmain = [load(mg_hbm, mgain), load(iw_hbm, iw), load(gw_hbm, gw)]
    lrt = load(rt_hbm, rts)

    barrier = pltpu.get_barrier_semaphore()
    peers = [(lax.rem(me + d, n), tp) for d in range(1, n)]
    for k in range(1, m):
        peers += [(me, tx(k)), (mate, tx(k))]
    for ep, t in peers:
        pl.semaphore_signal(
            barrier, inc=1, device_id={"ep": ep, "tp": t}, device_id_type=pl.DeviceIdType.MESH
        )
    ltok.wait()
    pl.semaphore_wait(barrier, len(peers))

    send(toks.at[:, lanes(mate, q)], narr.at[me], ts.at[mate], tr.at[me], mate, tp)
    for k in range(1, zs):
        for core in range(2):
            to = 2 * zp(k) + core
            send(toks.at[:, lanes(to, q)], narr.at[me], ts.at[to], tr.at[me], to, tp)
    narr[me] = toks[:, lanes(me, q)]
    lrt.wait()
    lane = lax.broadcasted_iota(jnp.int32, (rows, LANES), 1)
    pair = rts[...]
    mask[...] = ((pair[:, 0:1] == lane) | (pair[:, 1:2] == lane)).astype(F32).astype(BF16)
    values = toks[...].astype(F32)
    inverse = lax.rsqrt(jnp.mean(values * values, axis=-1, keepdims=True) + epsilon)
    lsmall = [
        load(a, b)
        for a, b in (
            (cv_hbm, cvs), (tap_hbm, taps), (rg_hbm, rgb), (ig_hbm, igb), (st_hbm, state),
            (dr_hbm, decay), (fg_hbm, gain), (maps_hbm, maps),
        )
    ]
    for cp in lmain:
        cp.wait()

    def reduction(psend, precv, keep, rsend, rrecv, s2, r2, s3, r3, part):
        def first(k):
            y = part(k)
            psend[k] = y[:rows].astype(BF16)
            send(psend.at[k], precv.at[k], s2.at[k], r2.at[k], mate, tp)
            keep[k] = y[rows:]

        def second(k):
            arrive(precv.at[k], r2.at[k])
            if k == 0:
                keep[0] = keep[0] + precv[0].astype(F32)
                return
            if k < 3:
                rsend[k] = (keep[k] + precv[k].astype(F32)).astype(BF16)
            else:

                @pl.when(inner)
                def _():
                    arrive(rrecv.at[2], r3.at[2])
                    total = keep[k] + precv[k].astype(F32) + rrecv[2].astype(F32)
                    rsend[k] = total.astype(BF16)

                @pl.when(outer)
                def _():
                    rsend[k] = (keep[k] + precv[k].astype(F32)).astype(BF16)

            to = jnp.where(inner, zp(2), zp(1)) if k == 2 else zp(k)
            send(rsend.at[k], rrecv.at[k], s3.at[k], r3.at[k], 2 * to + c, tp)

        def finish():
            arrive(rrecv.at[1], r3.at[1])
            keep[0] = keep[0] + rrecv[1].astype(F32)

            @pl.when(outer)
            def _():
                arrive(rrecv.at[2], r3.at[2])
                keep[0] = keep[0] + rrecv[2].astype(F32)

            arrive(rrecv.at[3], r3.at[3])
            return keep[0] + rrecv[3].astype(F32)

        return first, second, finish

    def part(k):
        zz = zp(k)
        for core in range(2):
            slot = 2 * zz + (1 - c if core == 0 else c)
            if k or core == 0:
                arrive(narr.at[slot], tr.at[slot])
        x = jnp.concatenate([narr[2 * zz + 1 - c], narr[2 * zz + c]], axis=0)
        x = (x.astype(F32) * mgain[me]).astype(BF16)
        return jnp.concatenate([dot(x, iw[...]), dot(x, gw[...])], axis=1)

    first, second, finish = reduction(
        psend, precv, pkeep, rsend, rrecv, s2, r2, s3, r3, part
    )
    with jax.named_scope("project"):
        first(0)
        lbig = [load(a, b) for a, b in ((ow_hbm, ow), (dg_hbm, dg), (du_hbm, du), (dd_hbm, dd))]
        lexp = [load(eg, wg), load(eu, wu)]
        ldown = [load(ed.at[:, pl.ds(i * q, q)], wd.at[i]) for i in range(n)]
        for k in range(1, zs):
            first(k)
            second(k)
        second(0)
    with jax.named_scope("prepare"):
        for k in range(zs):
            for core in range(2):
                if k or core:
                    to = 2 * zp(k) + (c if core == 0 else 1 - c)
                    send(mask, masks.at[me], ks.at[to], kr.at[me], to, tp)
        masks[me] = mask[...]
        for cp in lsmall:
            cp.wait()
        per = LANES // rgb.shape[1]
        size = rgb.shape[1]
        place_r = lax.broadcasted_iota(jnp.int32, (size, LANES), 0)
        place_c = lax.broadcasted_iota(jnp.int32, (size, LANES), 1)
        for p in range(ch // LANES):
            for s in range(per):
                move = (place_c == place_r + s * size).astype(F32).astype(BF16)
                for gate, blocks in enumerate((rgb, igb)):
                    bd[p, s * size : (s + 1) * size, gate * LANES : (gate + 1) * LANES] = dot(
                        blocks[p * per + s], move
                    ).astype(BF16)
        taken = cvs.shape[1]
        total = cvs[:, 0, :].astype(F32) * taps[0:1, :]
        for j in range(1, taken):
            total += cvs[:, j, :].astype(F32) * taps[j : j + 1, :]
        pre[...] = total
        for j in range(1, taken):
            cv_out[:, j - 1, :] = cvs[:, j, :]
        accg[...] = jnp.zeros_like(accg)
        accu[...] = jnp.zeros_like(accu)
        lacc[...] = jnp.zeros_like(lacc)
        square[...] = jnp.zeros_like(square)

    with jax.named_scope("recur"):
        both = finish() * inverse
        xb = both[:, :ch].astype(BF16)
        conv = (pre[...] + xb.astype(F32) * taps[taken : taken + 1, :]).astype(BF16)
        cv_out[:, taken - 1, :] = xb
        for p in range(ch // LANES):
            at = slice(p * LANES, (p + 1) * LANES)
            gates = jax.nn.sigmoid(dot(conv[:, at], bd[p]))
            log_decay = -decay_scale * gates[:, :LANES] * decay[:, at]
            ratio = jnp.tanh(-log_decay)
            scale = jnp.sqrt(2.0 * ratio / (1.0 + ratio))
            new = jnp.exp(log_decay) * state[:, at] + scale * gates[:, LANES:] * conv[:, at].astype(F32)
            st_out[:, at] = new
            gb = both[:, ch + p * LANES : ch + (p + 1) * LANES].astype(BF16).astype(F32)
            mr[:, at] = (new * jax.nn.gelu(gb)).astype(BF16)

    with jax.named_scope("mix"):
        send(mr, mall.at[me], bs.at[0], br.at[0], mate, tp)
        for k in range(1, zs):
            send(mr, mall.at[me], as_.at[k], ar.at[k], 2 * zp(k) + c, tp)
        mall[me] = mr[...]
        for cp in lbig:
            cp.wait()

        def pass_on(k):
            slot = 2 * zp(k) + c
            arrive(mall.at[slot], ar.at[k])
            send(mall.at[slot], mall.at[slot], bs.at[k], br.at[k], mate, tp)

        def mixed(i):
            for k in (2 * i, 2 * i + 1):
                arrive(mall.at[2 * zp(k) + 1 - c], br.at[k])
            which = side if i == 0 else 1 - side
            x = mall[pl.ds(which * zs, zs)].reshape(half, ch)
            y = dot(x, ow[...]).astype(BF16)
            for t in range(m):
                osend[t, i] = y[:, t * g : (t + 1) * g]
            for k in (3, 1, 2):
                send(osend.at[tx(k), i], orecv.at[k, i], os_.at[k, i], or_.at[k, i], me, tx(k))

        def summed(i):
            which = side if i == 0 else 1 - side
            raw = narr[pl.ds(which * zs, zs), :, lanes(tp, g)].reshape(half, g)
            total = raw.astype(F32) + osend[tp, i].astype(F32)
            for k in range(1, m):
                arrive(orecv.at[k, i], or_.at[k, i])
                total += orecv[k, i].astype(F32)
            full[tp, me, which] = total.astype(BF16)

    def sided(k, i):
        return side if (k < 2) == (i == 0) else 1 - side

    def spread(k, i):
        slot, s = 2 * zp(k) + c, sided(k, i)
        at = full.at[tp, slot, s]
        for d in (1, 2):
            send(at, at, xs.at[d, k, s], xr.at[d, k, s], me, tx(d))
        send(at, at, ms.at[0, k, s], mrv.at[0, k, s], mate, tp)

    def own(i):
        at = full.at[tp, me, sided(0, i)]
        s = sided(0, i)
        for k in (3, 2, 1):
            send(at, at, zs_.at[k, s], zr.at[k, s], 2 * zp(k) + c, tp)
        spread(0, i)

    def landed(k, i):
        s = sided(k, i)
        arrive(full.at[tp, 2 * zp(k) + c, s], zr.at[k, s])
        spread(k, i)

    def relay(k, i):
        slot, s = 2 * zp(k) + c, sided(k, i)
        early = tx(1) * (1 - s) + tx(2) * s
        late = tx(2) * (1 - s) + tx(1) * s
        at = full.at[early, slot, s]
        arrive(at, xr.at[1 + s, k, s])
        send(at, at, xs.at[3, k, s], xr.at[3, k, s], me, late)
        send(at, at, ms.at[1 + s, k, s], mrv.at[1 + s, k, s], mate, tp)
        at = full.at[late, slot, s]
        arrive(at, xr.at[2 - s, k, s])
        send(at, at, ms.at[2 - s, k, s], mrv.at[2 - s, k, s], mate, tp)

    def relay_far(k, i):
        slot, s = 2 * zp(k) + c, sided(k, i)
        at = full.at[tx(3), slot, s]
        arrive(at, xr.at[3, k, s])
        send(at, at, ms.at[3, k, s], mrv.at[3, k, s], mate, tp)

    def absorb(e, s, keep):
        parts = []
        for t in range(m):
            at = slice(t * g, (t + 1) * g)
            v = full[t, e, s].astype(F32)
            square[s] += v * v
            parts.append((v * gain[e, :, at]).astype(BF16))
        x = jnp.concatenate(parts, axis=1)
        if keep:
            nfm[s] = x
        accg[s] += dot(x, wg[e])
        accu[s] += dot(x, wu[e])
        lacc[s] += lax.dot_general(
            x, maps[:, lanes(e, q)], (((1,), (1,)), ((), ())), preferred_element_type=F32
        )

    def absorb_own(k, i):
        absorb(2 * zp(k) + c, sided(k, i), k == 0)

    def absorb_mate(k, i):
        e, s = 2 * zp(k) + 1 - c, sided(k, i)
        for d in range(m):
            arrive(full.at[tx(d), e, s], mrv.at[d, k, s])
        absorb(e, s, False)

    def dpart(k):
        s = zp(k) // 2
        x = []
        for core in range(2):
            at = lax.rem(zp(k), 2) * 2 + (1 - c if core == 0 else c)
            x.append(nfm[s, pl.ds(pl.multiple_of(at * rows, rows), rows), :])
        x = jnp.concatenate(x, axis=0)
        return jnp.concatenate([dot(x, dg[...]), dot(x, du[...])], axis=1)

    dfirst, dsecond, dfinish = reduction(
        dpsend, dprecv, dkeep, drsend, drrecv, s4, r4, s5, r5, dpart
    )

    with jax.named_scope("mix_near"):
        pass_on(1)
        mixed(0)
    with jax.named_scope("mix_sum"):
        pass_on(2)
        summed(0)
        own(0)
        pass_on(3)
        mixed(1)
    with jax.named_scope("gather_near"):
        for k in range(1, zs):
            landed(k, 0)
        relay(0, 0)
        summed(1)
        own(1)
        relay_far(0, 0)
        for cp in lexp:
            cp.wait()
        absorb_own(0, 0)
        dfirst(0)
        dfirst(1)
        dsecond(1)
        for k in range(1, zs):
            relay(k, 0)
    with jax.named_scope("gather_far"):
        for k in range(1, zs):
            landed(k, 1)
            relay_far(k, 0)
        absorb_mate(0, 0)
        relay(0, 1)
        relay_far(0, 1)
        absorb_own(0, 1)
        dfirst(2)
        dsecond(2)
        dfirst(3)
        for k in range(1, zs):
            relay(k, 1)
        dsecond(3)
        dsecond(0)
        for k in range(1, zs):
            absorb_own(k, 0)
            absorb_mate(k, 0)
            relay_far(k, 1)
        absorb_mate(0, 1)
        for k in range(1, zs):
            absorb_own(k, 1)
            absorb_mate(k, 1)

    with jax.named_scope("weights"):
        inv, weight, branch = [], [], []
        for k in range(zs):
            for core in range(2):
                if k or core:
                    src = 2 * zp(k) + (c if core == 0 else 1 - c)
                    arrive(masks.at[src], kr.at[src])
        for ih in range(2):
            s = 1 - side if ih == 0 else side
            scale = lax.rsqrt(jnp.sum(square[s], axis=-1, keepdims=True) / width + epsilon)
            square[s, :, 0:1] = scale
            logits = lacc[s] * scale
            chosen = masks[pl.ds(s * zs, zs)].reshape(half, LANES)[:, : lacc.shape[2]].astype(F32)
            named = logits * chosen
            other = jnp.sum(named, axis=-1, keepdims=True) - named
            share = (jax.nn.sigmoid(logits - other) * chosen).astype(BF16).astype(F32)
            at = lax.broadcasted_iota(jnp.int32, share.shape, 1)
            weight.append(jnp.sum(jnp.where(at == me, share, 0.0), axis=-1, keepdims=True))
            branch.append(jax.nn.sigmoid(logits[:, experts : experts + 1]))
            gate = accg[s] * scale
            act[ih] = (gate * jax.nn.sigmoid(gate) * (accu[s] * scale)).astype(BF16)

    order = [lax.rem(z + 1 + i, m) for i in range(m)]

    def down(ih):
        for i in range(m):
            y = dot(act[ih], wd[2 * order[i] + 1 - c]) * weight[ih]
            ysend[i, ih] = y.astype(BF16)
            send(ysend.at[i, ih], yrecv.at[i, ih], ys.at[i, ih], yr.at[i, ih], mate, tp)
        for i in range(m):
            y = dot(act[ih], wd[2 * order[i] + c]) * weight[ih]
            for t in range(m):
                kq[i, ih, t] = y[:, t * g : (t + 1) * g]

    def forward(i, ih, extra=None):
        arrive(yrecv.at[i, ih], yr.at[i, ih])
        for t in range(m):
            at = slice(t * g, (t + 1) * g)
            total = kq[i, ih, t] + yrecv[i, ih, :, at].astype(F32)
            if extra is not None:
                total += extra[:, at]
            kq[i, ih, t] = total
            xsend[i, ih, t] = total.astype(BF16)
        for k in (3, 1, 2):
            send(
                xsend.at[i, ih, tx(k)], xrecv.at[k, i, ih], hs_.at[k, i, ih], hr.at[k, i, ih], me, tx(k)
            )

    def settle(i, ih):
        total = kq[i, ih, tp]
        for k in range(1, m):
            arrive(xrecv.at[k, i, ih], hr.at[k, i, ih])
            total += xrecv[k, i, ih].astype(F32)
        pbuf[i, ih] = total.reshape(2, 2 * rows, g)
        for k in (2, 3) if ih == 0 else (1,):
            zsend[k, i] = pbuf[i, ih, lax.rem(zp(k), 2)].astype(BF16)

    def away(k, late):
        at = pl.ds(m - 1, 1) if late else pl.ds(0, m - 1)
        j = 1 if late else 0
        send(zsend.at[k, at], zrecv.at[k, at], gs.at[k, j], gr.at[k, j], 2 * zp(k) + c, tp)

    for cp in ldown:
        cp.wait()
    with jax.named_scope("down_far"):
        down(0)
    with jax.named_scope("dense_act"):
        at = pl.ds(pl.multiple_of(lax.rem(me, zs) * rows, rows), rows)
        both = dfinish() * square[side, at, 0:1]
        lead = both[:, :h]
        dact[...] = (lead * jax.nn.sigmoid(lead) * both[:, h:]).astype(BF16)
        for k in (3, 2, 1):
            send(dact, dall.at[me], cs.at[k], cr.at[k], 2 * zp(k) + c, tp)
        send(dact, dall.at[me], es.at[0], er.at[0], mate, tp)
        dall[me] = dact[...]
    with jax.named_scope("down_near"):
        for i in range(m - 1):
            forward(i, 0)
        down(1)
        for i in range(m - 1):
            forward(i, 1)
    with jax.named_scope("dense_pass"):
        for k in range(1, zs):
            slot = 2 * zp(k) + c
            arrive(dall.at[slot], cr.at[k])
            send(dall.at[slot], dall.at[slot], es.at[k], er.at[k], mate, tp)
    with jax.named_scope("settle_far"):
        for i in range(m - 1):
            settle(i, 0)
        for k in (2, 3):
            away(k, False)
    with jax.named_scope("dense_down"):
        for k in range(zs):
            arrive(dall.at[2 * zp(k) + 1 - c], er.at[k])
        for ih in range(2):
            s = 1 - side if ih == 0 else side
            x = dall[pl.ds(s * zs, zs)].reshape(half, h)
            forward(m - 1, ih, dot(x, dd[...]) * branch[ih])
    with jax.named_scope("settle_near"):
        for i in range(m - 1):
            settle(i, 1)
        away(1, False)
        settle(m - 1, 0)
        for k in (2, 3):
            away(k, True)
        settle(m - 1, 1)
        away(1, True)
    with jax.named_scope("last_sum"):
        for k in range(1, zs):
            arrive(zrecv.at[k, pl.ds(0, m - 1)], gr.at[k, 0])
        for k in range(1, zs):
            arrive(zrecv.at[k, pl.ds(m - 1, 1)], gr.at[k, 1])
        spot = lax.rem(z, 2)
        for j in range(m):
            total = pbuf[lax.rem(j - z - 1 + 2 * m, m), 1, spot]
            for k in range(1, zs):
                total += zrecv[k, lax.rem(j - zp(k) - 1 + 2 * m, m)].astype(F32)
            resid = full[tp, 2 * j + c, side, pl.ds(pl.multiple_of(2 * rows * spot, rows), 2 * rows), :]
            total = (total + resid.astype(F32)).astype(BF16)
            for core in range(2):
                fblk[core, j] = total[core * rows : (core + 1) * rows]
    with jax.named_scope("last_gather"):
        for k in (3, 1, 2, 0):
            for dc in range(2):
                if k or dc:
                    core = c if dc == 0 else 1 - c
                    send(
                        fblk.at[core], fin.at[c, tp], fs.at[dc, k], fr.at[dc, k], 2 * z + core, tx(k)
                    )
        fin[c, tp] = fblk[c]
        for k in (0, 1, 2, 3):
            for dc in range(2):
                if k or dc:
                    core = c if dc == 0 else 1 - c
                    arrive(fin.at[core, tx(k)], fr.at[dc, k])
        for core in range(2):
            for t in range(m):
                for j in range(m):
                    base = (2 * j + core) * q + t * g
                    out[:, base : base + g] = fin[core, t, j]
    for cp in sends:
        cp.wait_send()


def in_kernel(
    n, m, tokens, recur_state, conv_state, mix_gain, in_weight, gate_weight, conv_taps,
    recur_gate_blocks, input_gate_blocks, decay_rate, out_weight, ffn_gain, router_weight, routes,
    expert_gate, expert_up, expert_down, dense_gate, dense_up, dense_down, branch_gate,
):
    rows, width = tokens.shape
    q, ch = in_weight.shape
    experts = router_weight.shape[1]
    h, f = dense_gate.shape[1], expert_down.shape[1]
    g, zs, b = q // m, n // 2, n * rows
    half = b // 2
    lines = 2 * experts
    maps = jnp.concatenate(
        [
            router_weight.T,
            branch_gate[None],
            jnp.zeros((lines - experts - 1, width), BF16),
        ],
        axis=0,
    )
    hbm = pl.BlockSpec(memory_space=pl.ANY)
    vm = pl.BlockSpec(memory_space=pltpu.VMEM)
    v = pltpu.VMEM

    def pairs(*shapes):
        return [pltpu.SemaphoreType.DMA(s) for s in shapes for _ in range(2)]

    operands = (
        tokens, mix_gain.reshape(n, 1, q), ffn_gain.reshape(n, 1, q), routes, recur_state, conv_state,
        conv_taps, recur_gate_blocks, input_gate_blocks, decay_rate.reshape(1, ch), maps,
        in_weight, gate_weight, out_weight, dense_gate, dense_up, dense_down,
        expert_gate.reshape(n, q, f), expert_up.reshape(n, q, f), expert_down[0],
    )
    return pl.pallas_call(
        functools.partial(layer_kernel, n, m, experts),
        out_shape=(
            jax.ShapeDtypeStruct((rows, width), BF16),
            jax.ShapeDtypeStruct((rows, ch), F32),
            jax.ShapeDtypeStruct(conv_state.shape, BF16),
        ),
        in_specs=[hbm] * len(operands),
        out_specs=(vm, vm, vm),
        scratch_shapes=[
            v((rows, width), BF16), v((n, 1, q), F32), v((n, 1, q), F32), v(routes.shape, jnp.int32),
            v((rows, ch), F32), v(conv_state.shape, BF16), v(conv_taps.shape, F32),
            v(recur_gate_blocks.shape, BF16), v(input_gate_blocks.shape, BF16), v((1, ch), F32),
            v((lines, width), BF16), v((q, ch), BF16), v((q, ch), BF16), v((ch, q), BF16),
            v((q, h), BF16), v((q, h), BF16), v((h, q), BF16),
            v((n, q, f), BF16), v((n, q, f), BF16), v((n, f, q), BF16),
            v((n, rows, q), BF16), v((zs, rows, 2 * ch), BF16), v((zs, rows, 2 * ch), BF16),
            v((zs, rows, 2 * ch), F32), v((zs, rows, 2 * ch), BF16), v((zs, rows, 2 * ch), BF16),
            v((rows, ch), F32), v((ch // LANES, LANES, 2 * LANES), BF16),
            v((rows, LANES), BF16), v((n, rows, LANES), BF16),
            v((rows, ch), BF16), v((n, rows, ch), BF16),
            v((m, 2, half, g), BF16), v((m, 2, half, g), BF16),
            v((m, n, 2, half, g), BF16), v((2, half, q), BF16),
            v((2, half, g), F32), v((2, half, lines), F32),
            v((2, half, f), F32), v((2, half, f), F32), v((2, half, f), BF16),
            v((zs, rows, 2 * h), BF16), v((zs, rows, 2 * h), BF16), v((zs, rows, 2 * h), F32),
            v((zs, rows, 2 * h), BF16), v((zs, rows, 2 * h), BF16),
            v((rows, h), BF16), v((n, rows, h), BF16),
            v((m, 2, half, q), BF16), v((m, 2, half, q), BF16), v((m, 2, m, half, g), F32),
            v((m, 2, m, half, g), BF16), v((m, m, 2, half, g), BF16),
            v((m, 2, 2, 2 * rows, g), F32),
            v((zs, m, 2 * rows, g), BF16), v((zs, m, 2 * rows, g), BF16),
            v((2, m, rows, g), BF16), v((2, m, m, rows, g), BF16),
            pltpu.SemaphoreType.DMA((32,)),
        ]
        + pairs(
            (n,), (n,), (zs,), (zs,), (zs,), (zs,), (m, 2), (zs, 2), (m, zs, 2), (m, zs, 2),
            (zs,), (zs,), (zs,), (zs,), (m, 2), (m, m, 2), (zs, 2), (2, m),
        ),
        compiler_params=pltpu.CompilerParams(
            collective_id=0, has_side_effects=True, vmem_limit_bytes=58 * 1024 * 1024
        ),
        name="layer",
    )(*operands)


def solution(mesh):
    in_specs = (
        P("ep", None),
        P("ep", "tp"),
        P("ep", None, "tp"),
        P(),
        P("ep", "tp"),
        P("ep", "tp"),
        P(None, "tp"),
        P("tp", None, None),
        P("tp", None, None),
        P("tp"),
        P("tp", "ep"),
        P(),
        P(),
        P("ep", None),
        P("ep", None, "tp"),
        P("ep", None, "tp"),
        P("ep", "tp", None),
        P("ep", "tp"),
        P("ep", "tp"),
        P("tp", "ep"),
        P(),
    )
    out_specs = (P("ep", None), P("ep", "tp"), P("ep", None, "tp"))
    n, m = mesh.shape["ep"], mesh.shape["tp"]

    def body(*args):
        tokens, blocks, router, dense = args[0], args[7], args[12], args[17]
        q = tokens.shape[1] // n
        fits = m == 4 and n == 2 * m and n == router.shape[1] and q % (m * LANES) == 0
        fits = fits and tokens.shape[0] % 16 == 0 and dense.shape[1] % LANES == 0
        fits = fits and LANES % blocks.shape[1] == 0
        if fits:
            return in_kernel(n, m, *args)
        return on_device(*args)

    return jax.shard_map(
        body, mesh=mesh, in_specs=in_specs, out_specs=out_specs, check_vma=False
    )
```

```python
import functools

import jax
import jax.numpy as jnp
from jax import lax
from jax.experimental import pallas as pl
from jax.experimental.pallas import tpu as pltpu
from jax.sharding import PartitionSpec as P

TOP_K = 2
LANES = 128
F32 = jnp.float32
BF16 = jnp.bfloat16


epsilon = 1e-06
decay_scale = 8.0


def rms_scale(rows, gain):
    values = rows.astype(jnp.float32)
    inverse = lax.rsqrt(jnp.mean(values * values, axis=-1, keepdims=True) + epsilon)
    return (values * inverse * gain).astype(jnp.bfloat16)


def on_device(
    tokens,
    recur_state,
    conv_state,
    mix_gain,
    in_weight,
    gate_weight,
    conv_taps,
    recur_gate_blocks,
    input_gate_blocks,
    decay_rate,
    out_weight,
    ffn_gain,
    router_weight,
    routes,
    expert_gate,
    expert_up,
    expert_down,
    dense_gate,
    dense_up,
    dense_down,
    branch_gate,
):
    batch_rows, width = tokens.shape
    channels = in_weight.shape[1]
    normed = rms_scale(tokens, mix_gain)
    arrived = lax.all_to_all(normed, "ep", split_axis=1, concat_axis=0, tiled=True)
    joined = jnp.concatenate([in_weight, gate_weight], axis=1)
    summed = lax.psum_scatter(
        jnp.dot(arrived, joined, preferred_element_type=jnp.float32).astype(jnp.bfloat16),
        "ep",
        scatter_dimension=0,
        tiled=True,
    ).astype(jnp.float32)
    x_sum, gate_sum = (summed[:, :channels], summed[:, channels:])
    x_branch = x_sum.astype(jnp.bfloat16)
    gate_branch = gate_sum.astype(jnp.bfloat16)
    window = jnp.concatenate([conv_state, x_branch[:, None, :]], axis=1)
    conv_out = jnp.sum(window.astype(jnp.float32) * conv_taps[None], axis=1).astype(jnp.bfloat16)
    new_conv_state = window[:, 1:, :]
    blocks = conv_out.reshape(batch_rows, recur_gate_blocks.shape[0], recur_gate_blocks.shape[1])
    recur_gate = jax.nn.sigmoid(
        jnp.einsum(
            "bhi,hij->bhj", blocks, recur_gate_blocks, preferred_element_type=jnp.float32
        ).reshape(batch_rows, channels)
    )
    input_gate = jax.nn.sigmoid(
        jnp.einsum(
            "bhi,hij->bhj", blocks, input_gate_blocks, preferred_element_type=jnp.float32
        ).reshape(batch_rows, channels)
    )
    log_decay = -decay_scale * recur_gate * decay_rate
    new_state = jnp.exp(log_decay) * recur_state + jnp.sqrt(
        -jnp.expm1(2.0 * log_decay)
    ) * input_gate * conv_out.astype(jnp.float32)
    mixer_rows = (new_state * jax.nn.gelu(gate_branch.astype(jnp.float32))).astype(jnp.bfloat16)
    mixer_part = jnp.dot(
        mixer_rows,
        lax.all_gather(out_weight, "ep", axis=1, tiled=True),
        preferred_element_type=jnp.float32,
    )
    resid = (
        tokens.astype(jnp.float32)
        + lax.psum(mixer_part.astype(jnp.bfloat16), "tp").astype(jnp.float32)
    ).astype(jnp.bfloat16)
    normed_ffn = rms_scale(resid, ffn_gain)
    router_logits = jnp.dot(normed_ffn, router_weight, preferred_element_type=jnp.float32)
    experts = router_logits.shape[1]
    expert_ids = lax.broadcasted_iota(jnp.int32, (batch_rows, TOP_K, experts), 2)
    picked = jnp.sum(
        jnp.where(routes[:, :, None] == expert_ids, router_logits[:, None, :], 0.0), axis=2
    )
    route_weight = jax.nn.sigmoid(picked - picked[:, ::-1]).astype(jnp.bfloat16)
    capacity = 2 * batch_rows * TOP_K // experts
    flat_ids = routes.reshape(batch_rows * TOP_K)
    onehot = (
        flat_ids[:, None] == lax.broadcasted_iota(jnp.int32, (batch_rows * TOP_K, experts), 1)
    ).astype(jnp.int32)
    rank = jnp.sum((jnp.cumsum(onehot, axis=0) - onehot) * onehot, axis=1)
    slot_of = (flat_ids * capacity + rank).reshape(batch_rows, TOP_K)
    slot_rows = lax.broadcasted_iota(jnp.int32, (experts * capacity, batch_rows), 0)
    slot_cols = lax.broadcasted_iota(jnp.int32, (batch_rows, experts * capacity), 1)
    dispatch = jnp.zeros((experts * capacity, batch_rows), jnp.bfloat16)
    combine = jnp.zeros((batch_rows, experts * capacity), jnp.bfloat16)
    for pick in range(TOP_K):
        dispatch = dispatch + (slot_rows == slot_of[None, :, pick]).astype(jnp.bfloat16)
        combine = combine + jnp.where(
            slot_cols == slot_of[:, pick : pick + 1],
            route_weight[:, pick : pick + 1],
            jnp.zeros((), jnp.bfloat16),
        )
    outgoing = (
        jnp.dot(dispatch, normed_ffn, preferred_element_type=jnp.float32)
        .astype(jnp.bfloat16)
        .reshape(experts, capacity, width)
    )
    gate_local = expert_gate[0]
    up_local = expert_up[0]
    down_local = expert_down[0]
    arrived_rows = lax.all_to_all(outgoing, "ep", split_axis=0, concat_axis=0, tiled=True)
    sources, items, features = arrived_rows.shape
    rows = arrived_rows.reshape(sources * items, features)
    first = jnp.dot(rows, gate_local, preferred_element_type=jnp.float32)
    second = jnp.dot(rows, up_local, preferred_element_type=jnp.float32)
    act = (jax.nn.silu(first) * second).astype(jnp.bfloat16)
    partial_value = jnp.dot(act, down_local, preferred_element_type=jnp.float32)
    total = lax.psum(partial_value.astype(jnp.bfloat16), "tp")
    returned = lax.all_to_all(
        total.reshape(sources, items, total.shape[1]), "ep", split_axis=0, concat_axis=0, tiled=True
    )
    moe = jnp.dot(
        combine,
        returned.reshape(experts * capacity, returned.shape[2]),
        preferred_element_type=jnp.float32,
    )
    dense_arrived = lax.all_to_all(normed_ffn, "ep", split_axis=1, concat_axis=0, tiled=True)
    dense_joined = jnp.concatenate([dense_gate, dense_up], axis=1)
    dense_summed = lax.psum_scatter(
        jnp.dot(dense_arrived, dense_joined, preferred_element_type=jnp.float32).astype(
            jnp.bfloat16
        ),
        "ep",
        scatter_dimension=0,
        tiled=True,
    ).astype(jnp.float32)
    dense_first = dense_summed[:, : dense_gate.shape[1]]
    dense_second = dense_summed[:, dense_gate.shape[1] :]
    dense_act = (jax.nn.silu(dense_first) * dense_second).astype(jnp.bfloat16)
    dense_part = jnp.dot(
        dense_act,
        lax.all_gather(dense_down, "ep", axis=1, tiled=True),
        preferred_element_type=jnp.float32,
    )
    branch_weight = jax.nn.sigmoid(
        jnp.dot(normed_ffn, branch_gate, preferred_element_type=jnp.float32)
    )
    dense_sum = lax.psum(dense_part.astype(jnp.bfloat16), "tp").astype(jnp.float32)
    layer_out = (resid.astype(jnp.float32) + moe + branch_weight[:, None] * dense_sum).astype(
        jnp.bfloat16
    )
    return (layer_out, new_state, new_conv_state)


def rcopy(src, dst, send, recv, ep, tp):
    return pltpu.make_async_remote_copy(
        src_ref=src,
        dst_ref=dst,
        send_sem=send,
        recv_sem=recv,
        device_id={"ep": ep, "tp": tp},
        device_id_type=pl.DeviceIdType.MESH,
    )


def dot(left, right):
    return jnp.dot(left, right, preferred_element_type=F32)


def layer_kernel(
    n, m, experts, tok_hbm, mg_hbm, fg_hbm, rt_hbm, st_hbm, cv_hbm, tap_hbm, rg_hbm, ig_hbm, dr_hbm,
    rw_hbm, bw_hbm, iw_hbm, gw_hbm, ow_hbm, dg_hbm, du_hbm, dd_hbm, eg, eu, ed, out, st_out, cv_out,
    toks, mgain, gain, rts, state, cvs, taps, rgb, igb, decay, rw, bw, maps, iw, gw, ow, dg, du, dd, wg, wu, wd,
    narr, psend, precv, pkeep, rsend, rrecv, pre, bd, mask, masks, mr, mall, osend, orecv, full, nfm,
    square, lacc, accg, accu, act, dpsend, dprecv, dkeep, drsend, drrecv, dact, dall,
    ysend, yrecv, kq, xsend, xrecv, xjoin, pbuf, zsend, zrecv, fblk, fin,
    lw, ts, tr, ks, kr, s2, r2, s3, r3, as_, ar, bs, br, os_, or_, zs_, zr, xs, xr, ms, mrv,
    s4, r4, s5, r5, cs, cr, es, er, ys, yr, hs_, hr, gs, gr, fs, fr,
):
    me, tp = lax.axis_index("ep"), lax.axis_index("tp")
    zs = n // 2
    z, c = me // 2, me % 2
    mate = 2 * z + 1 - c
    side = z // 2
    inner = lax.rem(z, 3) != 0
    outer = lax.rem(z, 3) == 0
    rows, width = out.shape
    q, ch = iw.shape
    g = q // m
    half = n * rows // 2
    h = dg.shape[1]

    def zp(k):
        return (z, z + 1 - 2 * lax.rem(z, 2), lax.rem(z + 2, zs), zs - 1 - z)[k]

    def tx(k):
        return (tp, tp + 1 - 2 * lax.rem(tp, 2), lax.rem(tp + 2, m), m - 1 - tp)[k]

    def lanes(e, size):
        return pl.ds(pl.multiple_of(e * size, LANES), size)

    count = [0]

    def load(src, dst):
        cp = pltpu.make_async_copy(src, dst, lw.at[count[0]])
        count[0] += 1
        cp.start()
        return cp

    sends = []

    def send(*args):
        cp = rcopy(*args)
        cp.start()
        sends.append(cp)

    def arrive(buf, sem):
        rcopy(buf, buf, sem, sem, mate, tp).wait_recv()

    with jax.named_scope('enter'):
        ltok = load(tok_hbm, toks)
    lmain = [load(mg_hbm, mgain), load(iw_hbm, iw), load(gw_hbm, gw)]
    lrt = load(rt_hbm, rts)

    barrier = pltpu.get_barrier_semaphore()
    peers = [(lax.rem(me + d, n), tp) for d in range(1, n)]
    for k in range(1, m):
        peers += [(me, tx(k)), (mate, tx(k))]
    for ep, t in peers:
        pl.semaphore_signal(
            barrier, inc=1, device_id={"ep": ep, "tp": t}, device_id_type=pl.DeviceIdType.MESH
        )
    with jax.named_scope('tokwait'):
        ltok.wait()
    with jax.named_scope('greet'):
        pl.semaphore_wait(barrier, len(peers))

    send(toks.at[:, lanes(mate, q)], narr.at[me], ts.at[mate], tr.at[me], mate, tp)
    for k in (2, 1, 3):
        for core in range(2):
            to = 2 * zp(k) + core
            send(toks.at[:, lanes(to, q)], narr.at[me], ts.at[to], tr.at[me], to, tp)
    narr[me] = toks[:, lanes(me, q)]
    lrt.wait()
    pair = jnp.concatenate([rts[...]] * zs, axis=1)
    line = lax.broadcasted_iota(jnp.int32, mask.shape, 0)
    lane = lax.broadcasted_iota(jnp.int32, mask.shape, 1) - lax.rem(me, zs) * rows
    taken = ((pair[0:1] == line) | (pair[1:2] == line)) & (lane >= 0) & (lane < rows)
    mask[...] = taken.astype(F32).astype(BF16)
    values = toks[...].astype(F32)
    inverse = lax.rsqrt(jnp.mean(values * values, axis=-1, keepdims=True) + epsilon)
    lsmall = [
        load(a, b)
        for a, b in (
            (cv_hbm, cvs), (tap_hbm, taps), (rg_hbm, rgb), (ig_hbm, igb), (st_hbm, state),
            (dr_hbm, decay), (fg_hbm, gain), (rw_hbm, rw), (bw_hbm, bw),
        )
    ]
    with jax.named_scope('lmain'):
        for cp in lmain:
            cp.wait()

    def reduction(psend, precv, keep, rsend, rrecv, s2, r2, s3, r3, part):
        def first(k):
            y = part(k)
            psend[k] = y[:rows].astype(BF16)
            send(psend.at[k], precv.at[k], s2.at[k], r2.at[k], mate, tp)
            keep[k] = y[rows:]

        def second(k):
            arrive(precv.at[k], r2.at[k])
            if k == 0:
                keep[0] = keep[0] + precv[0].astype(F32)
                return
            if k < 3:
                rsend[k] = (keep[k] + precv[k].astype(F32)).astype(BF16)
            else:

                @pl.when(inner)
                def _():
                    arrive(rrecv.at[2], r3.at[2])
                    total = keep[k] + precv[k].astype(F32) + rrecv[2].astype(F32)
                    rsend[k] = total.astype(BF16)

                @pl.when(outer)
                def _():
                    rsend[k] = (keep[k] + precv[k].astype(F32)).astype(BF16)

            to = jnp.where(inner, zp(2), zp(1)) if k == 2 else zp(k)
            send(rsend.at[k], rrecv.at[k], s3.at[k], r3.at[k], 2 * to + c, tp)

        def finish():
            with jax.named_scope("fin1"):
                arrive(rrecv.at[1], r3.at[1])
            keep[0] = keep[0] + rrecv[1].astype(F32)

            @pl.when(outer)
            def _():
                arrive(rrecv.at[2], r3.at[2])
                keep[0] = keep[0] + rrecv[2].astype(F32)

            with jax.named_scope("fin3"):
                arrive(rrecv.at[3], r3.at[3])
            return keep[0] + rrecv[3].astype(F32)

        return first, second, finish

    def part(k):
        zz = zp(k)
        for core in range(2):
            slot = 2 * zz + (1 - c if core == 0 else c)
            if k or core == 0:
                arrive(narr.at[slot], tr.at[slot])
        x = jnp.concatenate([narr[2 * zz + 1 - c], narr[2 * zz + c]], axis=0)
        x = (x.astype(F32) * mgain[me]).astype(BF16)
        return jnp.concatenate([dot(x, iw[...]), dot(x, gw[...])], axis=1)

    first, second, finish = reduction(
        psend, precv, pkeep, rsend, rrecv, s2, r2, s3, r3, part
    )
    with jax.named_scope("project"):
        first(0)
        lbig = [load(a, b) for a, b in ((ow_hbm, ow), (dg_hbm, dg), (du_hbm, du), (dd_hbm, dd))]
        lexp = [load(eg, wg), load(eu, wu)]
        ldown = [load(ed.at[:, pl.ds(i * q, q)], wd.at[i]) for i in range(n)]
        for k in (2, 1, 3):
            first(k)
            second(k)
        second(0)
    with jax.named_scope("prepare"):
        for cp in lsmall:
            cp.wait()
        per = LANES // rgb.shape[1]
        size = rgb.shape[1]
        place_r = lax.broadcasted_iota(jnp.int32, (size, LANES), 0)
        place_c = lax.broadcasted_iota(jnp.int32, (size, LANES), 1)
        for p in range(ch // LANES):
            for s in range(per):
                move = (place_c == place_r + s * size).astype(F32).astype(BF16)
                for gate, blocks in enumerate((rgb, igb)):
                    bd[p, s * size : (s + 1) * size, gate * LANES : (gate + 1) * LANES] = dot(
                        blocks[p * per + s], move
                    ).astype(BF16)
        taken = cvs.shape[0]
        total = cvs[0].astype(F32) * taps[0:1, :]
        for j in range(1, taken):
            total += cvs[j].astype(F32) * taps[j : j + 1, :]
        pre[...] = total
        for j in range(1, taken):
            cv_out[j - 1] = cvs[j]
        for e in range(n):
            at = slice(e * q, (e + 1) * q)
            line = jnp.broadcast_to(bw[...].astype(F32).reshape(1, width)[:, at], (experts, q))
            maps[:, at] = jnp.concatenate([rw[:, at].astype(F32), line], axis=0).astype(BF16)
        accg[...] = jnp.zeros_like(accg)
        accu[...] = jnp.zeros_like(accu)
        lacc[...] = jnp.zeros_like(lacc)
        square[...] = jnp.zeros_like(square)

    with jax.named_scope("recur"):
        both = finish() * inverse
        xb = both[:, :ch].astype(BF16)
        conv = (pre[...] + xb.astype(F32) * taps[taken : taken + 1, :]).astype(BF16)
        cv_out[taken - 1] = xb
        for p in range(ch // LANES):
            at = slice(p * LANES, (p + 1) * LANES)
            gates = jax.nn.sigmoid(dot(conv[:, at], bd[p]))
            log_decay = -decay_scale * gates[:, :LANES] * decay[:, at]
            ratio = jnp.tanh(-log_decay)
            scale = jnp.sqrt(2.0 * ratio / (1.0 + ratio))
            new = jnp.exp(log_decay) * state[:, at] + scale * gates[:, LANES:] * conv[:, at].astype(F32)
            st_out[:, at] = new
            gb = both[:, ch + p * LANES : ch + (p + 1) * LANES].astype(BF16).astype(F32)
            mr[:, at] = (new * jax.nn.gelu(gb)).astype(BF16)

    with jax.named_scope("mix"):
        send(mr, mall.at[me], bs.at[0], br.at[0], mate, tp)
        for k in range(1, zs):
            send(mr, mall.at[me], as_.at[k], ar.at[k], 2 * zp(k) + c, tp)
        mall[me] = mr[...]
        for cp in lbig:
            cp.wait()

        def pass_on(k):
            slot = 2 * zp(k) + c
            arrive(mall.at[slot], ar.at[k])
            send(mall.at[slot], mall.at[slot], bs.at[k], br.at[k], mate, tp)

        def mixed(i):
            for k in (2 * i, 2 * i + 1):
                arrive(mall.at[2 * zp(k) + 1 - c], br.at[k])
            which = side if i == 0 else 1 - side
            x = mall[pl.ds(which * zs, zs)].reshape(half, ch)
            y = dot(x, ow[...]).astype(BF16)
            for t in range(m):
                osend[t, i] = y[:, t * g : (t + 1) * g]
            for k in (3, 1, 2):
                send(osend.at[tx(k), i], orecv.at[k, i], os_.at[k, i], or_.at[k, i], me, tx(k))

        def summed(i):
            which = side if i == 0 else 1 - side
            raw = narr[pl.ds(which * zs, zs), :, lanes(tp, g)].reshape(half, g)
            total = raw.astype(F32) + osend[tp, i].astype(F32)
            for k in range(1, m):
                arrive(orecv.at[k, i], or_.at[k, i])
                total += orecv[k, i].astype(F32)
            full[tp, me, which] = total.astype(BF16)

    def sided(k, i):
        return side if (k < 2) == (i == 0) else 1 - side

    def spread(k, i):
        slot, s = 2 * zp(k) + c, sided(k, i)
        at = full.at[tp, slot, s]
        for d in (1, 2):
            send(at, at, xs.at[d, k, s], xr.at[d, k, s], me, tx(d))
        send(at, at, ms.at[0, k, s], mrv.at[0, k, s], mate, tp)

    def own(i):
        at = full.at[tp, me, sided(0, i)]
        s = sided(0, i)
        for k in (3, 2, 1):
            send(at, at, zs_.at[k, s], zr.at[k, s], 2 * zp(k) + c, tp)
        spread(0, i)

    def landed(k, i):
        s = sided(k, i)
        arrive(full.at[tp, 2 * zp(k) + c, s], zr.at[k, s])
        spread(k, i)

    def relay(k, i):
        slot, s = 2 * zp(k) + c, sided(k, i)
        early = tx(1) * (1 - s) + tx(2) * s
        late = tx(2) * (1 - s) + tx(1) * s
        at = full.at[early, slot, s]
        arrive(at, xr.at[1 + s, k, s])
        send(at, at, xs.at[3, k, s], xr.at[3, k, s], me, late)
        send(at, at, ms.at[1 + s, k, s], mrv.at[1 + s, k, s], mate, tp)
        at = full.at[late, slot, s]
        arrive(at, xr.at[2 - s, k, s])
        send(at, at, ms.at[2 - s, k, s], mrv.at[2 - s, k, s], mate, tp)

    def relay_far(k, i):
        slot, s = 2 * zp(k) + c, sided(k, i)
        at = full.at[tx(3), slot, s]
        arrive(at, xr.at[3, k, s])
        send(at, at, ms.at[3, k, s], mrv.at[3, k, s], mate, tp)

    def absorb(e, s, keep):
        parts = []
        for t in range(m):
            at = slice(t * g, (t + 1) * g)
            v = full[t, e, s].astype(F32)
            square[s] += v * v
            parts.append((v * gain[e, :, at]).astype(BF16))
        x = jnp.concatenate(parts, axis=1)
        if keep:
            nfm[s] = x
        accg[s] += dot(x, wg[e])
        accu[s] += dot(x, wu[e])
        lacc[s] += lax.dot_general(
            x, maps[:, lanes(e, q)], (((1,), (1,)), ((), ())), preferred_element_type=F32
        )

    def absorb_own(k, i):
        absorb(2 * zp(k) + c, sided(k, i), k == 0)

    def absorb_mate(k, i):
        e, s = 2 * zp(k) + 1 - c, sided(k, i)
        for d in range(m):
            arrive(full.at[tx(d), e, s], mrv.at[d, k, s])
        absorb(e, s, False)

    def dpart(k):
        s = zp(k) // 2
        x = []
        for core in range(2):
            at = lax.rem(zp(k), 2) * 2 + (1 - c if core == 0 else c)
            x.append(nfm[s, pl.ds(pl.multiple_of(at * rows, rows), rows), :])
        x = jnp.concatenate(x, axis=0)
        return jnp.concatenate([dot(x, dg[...]), dot(x, du[...])], axis=1)

    dfirst, dsecond, dfinish = reduction(
        dpsend, dprecv, dkeep, drsend, drrecv, s4, r4, s5, r5, dpart
    )

    with jax.named_scope("mix_near"):
        pass_on(1)
        mixed(0)
        for k in range(zs):
            for core in range(2):
                if k or core:
                    to = 2 * zp(k) + (c if core == 0 else 1 - c)
                    send(mask, masks.at[me], ks.at[to], kr.at[me], to, tp)
        masks[me] = mask[...]
    with jax.named_scope("mix_sum"):
        pass_on(2)
        summed(0)
    with jax.named_scope("gather"):
        own(0)
        pass_on(3)
        mixed(1)
        landed(1, 0)
        relay(0, 0)
        landed(2, 0)
        landed(3, 0)
        relay(1, 0)
        summed(1)
        own(1)
        relay(2, 0)
        relay_far(0, 0)
        for cp in lexp:
            cp.wait()
        absorb_own(0, 0)
        dfirst(0)
        relay(3, 0)
        relay_far(1, 0)
        absorb_own(1, 0)
        dfirst(1)
        absorb_mate(0, 0)
        relay(0, 1)
        landed(1, 1)
        relay_far(2, 0)
        dsecond(1)
        absorb_own(2, 0)
        absorb_mate(1, 0)
        landed(2, 1)
        landed(3, 1)
        relay(1, 1)
        relay_far(3, 0)
        absorb_own(3, 0)
        absorb_mate(2, 0)
        relay_far(0, 1)
        absorb_own(0, 1)
        dfirst(2)
        relay(2, 1)
        absorb_mate(3, 0)
        relay_far(1, 1)
        absorb_own(1, 1)
        dfirst(3)
        dsecond(2)
        relay(3, 1)
        absorb_mate(0, 1)
        relay_far(2, 1)
        absorb_own(2, 1)
        absorb_mate(1, 1)
        dsecond(3)
        relay_far(3, 1)
        absorb_own(3, 1)
        absorb_mate(2, 1)
        dsecond(0)
        absorb_mate(3, 1)

    with jax.named_scope("weights"):
        inv, weight, branch = [], [], []
        for k in range(zs):
            for core in range(2):
                if k or core:
                    src = 2 * zp(k) + (c if core == 0 else 1 - c)
                    arrive(masks.at[src], kr.at[src])
        for ih in range(2):
            s = 1 - side if ih == 0 else side
            scale = lax.rsqrt(jnp.sum(square[s], axis=-1, keepdims=True) / width + epsilon)
            square[s, :, 0:1] = scale
            logits = lacc[s] * scale
            chosen = jnp.sum(masks[pl.ds(s * zs, zs)].astype(F32), axis=0).T
            named = logits * chosen
            other = jnp.sum(named, axis=-1, keepdims=True) - named
            share = (jax.nn.sigmoid(logits - other) * chosen).astype(BF16).astype(F32)
            at = lax.broadcasted_iota(jnp.int32, share.shape, 1)
            weight.append(jnp.sum(jnp.where(at == me, share, 0.0), axis=-1, keepdims=True))
            branch.append(jax.nn.sigmoid(logits[:, experts : experts + 1]))
            gate = accg[s] * scale
            act[ih] = (gate * jax.nn.sigmoid(gate) * (accu[s] * scale)).astype(BF16)

    order = [lax.rem(z + 1 + i, m) for i in range(m)]

    def down(ih):
        for i in range(m):
            y = dot(act[ih], wd[2 * order[i] + 1 - c]) * weight[ih]
            ysend[i, ih] = y.astype(BF16)
            send(ysend.at[i, ih], yrecv.at[i, ih], ys.at[i, ih], yr.at[i, ih], mate, tp)
        for i in range(m):
            y = dot(act[ih], wd[2 * order[i] + c]) * weight[ih]
            for t in range(m):
                kq[i, ih, t] = y[:, t * g : (t + 1) * g]

    def pass_part(k, i, ih, part, to):
        send(part, xrecv.at[k, i, ih], hs_.at[k, i, ih], hr.at[k, i, ih], me, tx(to))

    def join(i, ih):
        lead = 1 + (i + ih) % 2
        arrive(xrecv.at[3, i, ih], hr.at[3, i, ih])
        total = kq[i, ih, tx(3 - lead)] + xrecv[3, i, ih].astype(F32)
        xjoin[i, ih] = total.astype(BF16)
        pass_part(3 - lead, i, ih, xjoin.at[i, ih], 3 - lead)

    def forward(i, ih, extra=None):
        arrive(yrecv.at[i, ih], yr.at[i, ih])
        for t in range(m):
            at = slice(t * g, (t + 1) * g)
            total = kq[i, ih, t] + yrecv[i, ih, :, at].astype(F32)
            if extra is not None:
                total += extra[:, at]
            kq[i, ih, t] = total
            xsend[i, ih, t] = total.astype(BF16)
        if i == m - 1:
            for k in (3, 1, 2):
                pass_part(k, i, ih, xsend.at[i, ih, tx(k)], k)
        else:
            lead = 1 + (i + ih) % 2
            pass_part(3, i, ih, xsend.at[i, ih, tx(3)], lead)
            pass_part(lead, i, ih, xsend.at[i, ih, tx(lead)], lead)

    def settle(i, ih):
        total = kq[i, ih, tp]
        for k in range(1, m) if i == m - 1 else (1, 2):
            arrive(xrecv.at[k, i, ih], hr.at[k, i, ih])
            total += xrecv[k, i, ih].astype(F32)
        pbuf[i, ih] = total.reshape(2, 2 * rows, g)
        for k in (2, 3) if ih == 0 else (1,):
            zsend[k, i] = pbuf[i, ih, lax.rem(zp(k), 2)].astype(BF16)

    def away(k, late):
        at = pl.ds(m - 1, 1) if late else pl.ds(0, m - 1)
        j = 1 if late else 0
        send(zsend.at[k, at], zrecv.at[k, at], gs.at[k, j], gr.at[k, j], 2 * zp(k) + c, tp)

    for cp in ldown:
        cp.wait()
    with jax.named_scope("down_far"):
        down(0)
    with jax.named_scope("dense_act"):
        at = pl.ds(pl.multiple_of(lax.rem(me, zs) * rows, rows), rows)
        both = dfinish() * square[side, at, 0:1]
        lead = both[:, :h]
        dact[...] = (lead * jax.nn.sigmoid(lead) * both[:, h:]).astype(BF16)
        for k in (3, 2, 1):
            send(dact, dall.at[me], cs.at[k], cr.at[k], 2 * zp(k) + c, tp)
        send(dact, dall.at[me], es.at[0], er.at[0], mate, tp)
        dall[me] = dact[...]
    with jax.named_scope("down_near"):
        for i in range(m - 1):
            forward(i, 0)
        down(1)
        for i in range(m - 1):
            forward(i, 1)
            join(i, 0)
    with jax.named_scope("dense_pass"):
        for k in range(1, zs):
            slot = 2 * zp(k) + c
            arrive(dall.at[slot], cr.at[k])
            send(dall.at[slot], dall.at[slot], es.at[k], er.at[k], mate, tp)
    with jax.named_scope("settle_far"):
        for i in range(m - 1):
            join(i, 1)
        for i in range(m - 1):
            settle(i, 0)
        for k in (2, 3):
            away(k, False)
    with jax.named_scope("dense_down"):
        for k in range(zs):
            arrive(dall.at[2 * zp(k) + 1 - c], er.at[k])
        for ih in range(2):
            s = 1 - side if ih == 0 else side
            x = dall[pl.ds(s * zs, zs)].reshape(half, h)
            forward(m - 1, ih, dot(x, dd[...]) * branch[ih])
    with jax.named_scope("settle_near"):
        for i in range(m - 1):
            settle(i, 1)
        away(1, False)
        settle(m - 1, 0)
        for k in (2, 3):
            away(k, True)
        settle(m - 1, 1)
        away(1, True)
    with jax.named_scope("last_sum"):
        for k in range(1, zs):
            arrive(zrecv.at[k, pl.ds(0, m - 1)], gr.at[k, 0])
        for k in range(1, zs):
            arrive(zrecv.at[k, pl.ds(m - 1, 1)], gr.at[k, 1])
        spot = lax.rem(z, 2)
        for j in range(m):
            total = pbuf[lax.rem(j - z - 1 + 2 * m, m), 1, spot]
            for k in range(1, zs):
                total += zrecv[k, lax.rem(j - zp(k) - 1 + 2 * m, m)].astype(F32)
            resid = full[tp, 2 * j + c, side, pl.ds(pl.multiple_of(2 * rows * spot, rows), 2 * rows), :]
            total = (total + resid.astype(F32)).astype(BF16)
            for core in range(2):
                fblk[core, j] = total[core * rows : (core + 1) * rows]
    with jax.named_scope("last_gather"):
        for k in (3, 1, 2, 0):
            for dc in range(2):
                if k or dc:
                    core = c if dc == 0 else 1 - c
                    send(
                        fblk.at[core], fin.at[c, tp], fs.at[dc, k], fr.at[dc, k], 2 * z + core, tx(k)
                    )
        fin[c, tp] = fblk[c]
        for k in (0, 1, 2, 3):
            for dc in range(2):
                if k or dc:
                    core = c if dc == 0 else 1 - c
                    arrive(fin.at[core, tx(k)], fr.at[dc, k])
        for core in range(2):
            for t in range(m):
                for j in range(m):
                    base = (2 * j + core) * q + t * g
                    out[:, base : base + g] = fin[core, t, j]
    for cp in sends:
        cp.wait_send()


def in_kernel(
    n, m, tokens, recur_state, conv_state, mix_gain, in_weight, gate_weight, conv_taps,
    recur_gate_blocks, input_gate_blocks, decay_rate, out_weight, ffn_gain, router_weight, routes,
    expert_gate, expert_up, expert_down, dense_gate, dense_up, dense_down, branch_gate,
):
    rows, width = tokens.shape
    q, ch = in_weight.shape
    experts = router_weight.shape[1]
    h, f = dense_gate.shape[1], expert_down.shape[1]
    g, zs, b = q // m, n // 2, n * rows
    half = b // 2
    lines = 2 * experts
    past = (conv_state.shape[1], rows, ch)
    hbm = pl.BlockSpec(memory_space=pl.ANY)
    vm = pl.BlockSpec(memory_space=pltpu.VMEM)
    v = pltpu.VMEM

    def pairs(*shapes):
        return [pltpu.SemaphoreType.DMA(s) for s in shapes for _ in range(2)]

    operands = (
        tokens, mix_gain.reshape(n, 1, q), ffn_gain.reshape(n, 1, q), routes.T, recur_state,
        conv_state.transpose(1, 0, 2), conv_taps, recur_gate_blocks, input_gate_blocks,
        decay_rate.reshape(1, ch), router_weight.T, branch_gate,
        in_weight, gate_weight, out_weight, dense_gate, dense_up, dense_down,
        expert_gate.reshape(n, q, f), expert_up.reshape(n, q, f), expert_down[0],
    )
    results = (
        jax.ShapeDtypeStruct((rows, width), BF16),
        jax.ShapeDtypeStruct((rows, ch), F32),
        jax.ShapeDtypeStruct(past, BF16),
    )
    layer_out, new_state, window = pl.pallas_call(
        functools.partial(layer_kernel, n, m, experts),
        out_shape=tuple(pltpu.VMEM(r.shape, r.dtype) for r in results),
        in_specs=[hbm] * len(operands),
        out_specs=(vm, vm, vm),
        scratch_shapes=[
            v((rows, width), BF16), v((n, 1, q), F32), v((n, 1, q), F32), v(routes.shape[::-1], jnp.int32),
            v((rows, ch), F32), v(past, BF16), v(conv_taps.shape, F32),
            v(recur_gate_blocks.shape, BF16), v(input_gate_blocks.shape, BF16), v((1, ch), F32),
            v((experts, width), BF16), v((width,), BF16), v((lines, width), BF16), v((q, ch), BF16), v((q, ch), BF16), v((ch, q), BF16),
            v((q, h), BF16), v((q, h), BF16), v((h, q), BF16),
            v((n, q, f), BF16), v((n, q, f), BF16), v((n, f, q), BF16),
            v((n, rows, q), BF16), v((zs, rows, 2 * ch), BF16), v((zs, rows, 2 * ch), BF16),
            v((zs, rows, 2 * ch), F32), v((zs, rows, 2 * ch), BF16), v((zs, rows, 2 * ch), BF16),
            v((rows, ch), F32), v((ch // LANES, LANES, 2 * LANES), BF16),
            v((lines, half), BF16), v((n, lines, half), BF16),
            v((rows, ch), BF16), v((n, rows, ch), BF16),
            v((m, 2, half, g), BF16), v((m, 2, half, g), BF16),
            v((m, n, 2, half, g), BF16), v((2, half, q), BF16),
            v((2, half, g), F32), v((2, half, lines), F32),
            v((2, half, f), F32), v((2, half, f), F32), v((2, half, f), BF16),
            v((zs, rows, 2 * h), BF16), v((zs, rows, 2 * h), BF16), v((zs, rows, 2 * h), F32),
            v((zs, rows, 2 * h), BF16), v((zs, rows, 2 * h), BF16),
            v((rows, h), BF16), v((n, rows, h), BF16),
            v((m, 2, half, q), BF16), v((m, 2, half, q), BF16), v((m, 2, m, half, g), F32),
            v((m, 2, m, half, g), BF16), v((m, m, 2, half, g), BF16), v((m - 1, 2, half, g), BF16),
            v((m, 2, 2, 2 * rows, g), F32),
            v((zs, m, 2 * rows, g), BF16), v((zs, m, 2 * rows, g), BF16),
            v((2, m, rows, g), BF16), v((2, m, m, rows, g), BF16),
            pltpu.SemaphoreType.DMA((32,)),
        ]
        + pairs(
            (n,), (n,), (zs,), (zs,), (zs,), (zs,), (m, 2), (zs, 2), (m, zs, 2), (m, zs, 2),
            (zs,), (zs,), (zs,), (zs,), (m, 2), (m, m, 2), (zs, 2), (2, m),
        ),
        compiler_params=pltpu.CompilerParams(
            collective_id=0, has_side_effects=True, vmem_limit_bytes=58 * 1024 * 1024
        ),
        name="layer",
    )(*operands)
    return (layer_out, new_state, window.transpose(1, 0, 2))


def solution(mesh):
    in_specs = (
        P("ep", None),
        P("ep", "tp"),
        P("ep", None, "tp"),
        P(),
        P("ep", "tp"),
        P("ep", "tp"),
        P(None, "tp"),
        P("tp", None, None),
        P("tp", None, None),
        P("tp"),
        P("tp", "ep"),
        P(),
        P(),
        P("ep", None),
        P("ep", None, "tp"),
        P("ep", None, "tp"),
        P("ep", "tp", None),
        P("ep", "tp"),
        P("ep", "tp"),
        P("tp", "ep"),
        P(),
    )
    out_specs = (P("ep", None), P("ep", "tp"), P("ep", None, "tp"))
    n, m = mesh.shape["ep"], mesh.shape["tp"]

    def body(*args):
        tokens, blocks, router, dense = args[0], args[7], args[12], args[17]
        q = tokens.shape[1] // n
        fits = m == 4 and n == 2 * m and n == router.shape[1] and q % (m * LANES) == 0
        fits = fits and tokens.shape[0] % 16 == 0 and dense.shape[1] % LANES == 0
        fits = fits and LANES % blocks.shape[1] == 0
        if fits:
            return in_kernel(n, m, *args)
        return on_device(*args)

    return jax.shard_map(
        body, mesh=mesh, in_specs=in_specs, out_specs=out_specs, check_vma=False
    )
```

```python
import functools

import jax
import jax.numpy as jnp
from jax import lax
from jax.experimental import pallas as pl
from jax.experimental.pallas import tpu as pltpu
from jax.sharding import PartitionSpec as P

TOP_K = 2
LANES = 128
F32 = jnp.float32
BF16 = jnp.bfloat16


epsilon = 1e-06
decay_scale = 8.0


def rms_scale(rows, gain):
    values = rows.astype(jnp.float32)
    inverse = lax.rsqrt(jnp.mean(values * values, axis=-1, keepdims=True) + epsilon)
    return (values * inverse * gain).astype(jnp.bfloat16)


def on_device(
    tokens,
    recur_state,
    conv_state,
    mix_gain,
    in_weight,
    gate_weight,
    conv_taps,
    recur_gate_blocks,
    input_gate_blocks,
    decay_rate,
    out_weight,
    ffn_gain,
    router_weight,
    routes,
    expert_gate,
    expert_up,
    expert_down,
    dense_gate,
    dense_up,
    dense_down,
    branch_gate,
):
    batch_rows, width = tokens.shape
    channels = in_weight.shape[1]
    normed = rms_scale(tokens, mix_gain)
    arrived = lax.all_to_all(normed, "ep", split_axis=1, concat_axis=0, tiled=True)
    joined = jnp.concatenate([in_weight, gate_weight], axis=1)
    summed = lax.psum_scatter(
        jnp.dot(arrived, joined, preferred_element_type=jnp.float32).astype(jnp.bfloat16),
        "ep",
        scatter_dimension=0,
        tiled=True,
    ).astype(jnp.float32)
    x_sum, gate_sum = (summed[:, :channels], summed[:, channels:])
    x_branch = x_sum.astype(jnp.bfloat16)
    gate_branch = gate_sum.astype(jnp.bfloat16)
    window = jnp.concatenate([conv_state, x_branch[:, None, :]], axis=1)
    conv_out = jnp.sum(window.astype(jnp.float32) * conv_taps[None], axis=1).astype(jnp.bfloat16)
    new_conv_state = window[:, 1:, :]
    blocks = conv_out.reshape(batch_rows, recur_gate_blocks.shape[0], recur_gate_blocks.shape[1])
    recur_gate = jax.nn.sigmoid(
        jnp.einsum(
            "bhi,hij->bhj", blocks, recur_gate_blocks, preferred_element_type=jnp.float32
        ).reshape(batch_rows, channels)
    )
    input_gate = jax.nn.sigmoid(
        jnp.einsum(
            "bhi,hij->bhj", blocks, input_gate_blocks, preferred_element_type=jnp.float32
        ).reshape(batch_rows, channels)
    )
    log_decay = -decay_scale * recur_gate * decay_rate
    new_state = jnp.exp(log_decay) * recur_state + jnp.sqrt(
        -jnp.expm1(2.0 * log_decay)
    ) * input_gate * conv_out.astype(jnp.float32)
    mixer_rows = (new_state * jax.nn.gelu(gate_branch.astype(jnp.float32))).astype(jnp.bfloat16)
    mixer_part = jnp.dot(
        mixer_rows,
        lax.all_gather(out_weight, "ep", axis=1, tiled=True),
        preferred_element_type=jnp.float32,
    )
    resid = (
        tokens.astype(jnp.float32)
        + lax.psum(mixer_part.astype(jnp.bfloat16), "tp").astype(jnp.float32)
    ).astype(jnp.bfloat16)
    normed_ffn = rms_scale(resid, ffn_gain)
    router_logits = jnp.dot(normed_ffn, router_weight, preferred_element_type=jnp.float32)
    experts = router_logits.shape[1]
    expert_ids = lax.broadcasted_iota(jnp.int32, (batch_rows, TOP_K, experts), 2)
    picked = jnp.sum(
        jnp.where(routes[:, :, None] == expert_ids, router_logits[:, None, :], 0.0), axis=2
    )
    route_weight = jax.nn.sigmoid(picked - picked[:, ::-1]).astype(jnp.bfloat16)
    capacity = 2 * batch_rows * TOP_K // experts
    flat_ids = routes.reshape(batch_rows * TOP_K)
    onehot = (
        flat_ids[:, None] == lax.broadcasted_iota(jnp.int32, (batch_rows * TOP_K, experts), 1)
    ).astype(jnp.int32)
    rank = jnp.sum((jnp.cumsum(onehot, axis=0) - onehot) * onehot, axis=1)
    slot_of = (flat_ids * capacity + rank).reshape(batch_rows, TOP_K)
    slot_rows = lax.broadcasted_iota(jnp.int32, (experts * capacity, batch_rows), 0)
    slot_cols = lax.broadcasted_iota(jnp.int32, (batch_rows, experts * capacity), 1)
    dispatch = jnp.zeros((experts * capacity, batch_rows), jnp.bfloat16)
    combine = jnp.zeros((batch_rows, experts * capacity), jnp.bfloat16)
    for pick in range(TOP_K):
        dispatch = dispatch + (slot_rows == slot_of[None, :, pick]).astype(jnp.bfloat16)
        combine = combine + jnp.where(
            slot_cols == slot_of[:, pick : pick + 1],
            route_weight[:, pick : pick + 1],
            jnp.zeros((), jnp.bfloat16),
        )
    outgoing = (
        jnp.dot(dispatch, normed_ffn, preferred_element_type=jnp.float32)
        .astype(jnp.bfloat16)
        .reshape(experts, capacity, width)
    )
    gate_local = expert_gate[0]
    up_local = expert_up[0]
    down_local = expert_down[0]
    arrived_rows = lax.all_to_all(outgoing, "ep", split_axis=0, concat_axis=0, tiled=True)
    sources, items, features = arrived_rows.shape
    rows = arrived_rows.reshape(sources * items, features)
    first = jnp.dot(rows, gate_local, preferred_element_type=jnp.float32)
    second = jnp.dot(rows, up_local, preferred_element_type=jnp.float32)
    act = (jax.nn.silu(first) * second).astype(jnp.bfloat16)
    partial_value = jnp.dot(act, down_local, preferred_element_type=jnp.float32)
    total = lax.psum(partial_value.astype(jnp.bfloat16), "tp")
    returned = lax.all_to_all(
        total.reshape(sources, items, total.shape[1]), "ep", split_axis=0, concat_axis=0, tiled=True
    )
    moe = jnp.dot(
        combine,
        returned.reshape(experts * capacity, returned.shape[2]),
        preferred_element_type=jnp.float32,
    )
    dense_arrived = lax.all_to_all(normed_ffn, "ep", split_axis=1, concat_axis=0, tiled=True)
    dense_joined = jnp.concatenate([dense_gate, dense_up], axis=1)
    dense_summed = lax.psum_scatter(
        jnp.dot(dense_arrived, dense_joined, preferred_element_type=jnp.float32).astype(
            jnp.bfloat16
        ),
        "ep",
        scatter_dimension=0,
        tiled=True,
    ).astype(jnp.float32)
    dense_first = dense_summed[:, : dense_gate.shape[1]]
    dense_second = dense_summed[:, dense_gate.shape[1] :]
    dense_act = (jax.nn.silu(dense_first) * dense_second).astype(jnp.bfloat16)
    dense_part = jnp.dot(
        dense_act,
        lax.all_gather(dense_down, "ep", axis=1, tiled=True),
        preferred_element_type=jnp.float32,
    )
    branch_weight = jax.nn.sigmoid(
        jnp.dot(normed_ffn, branch_gate, preferred_element_type=jnp.float32)
    )
    dense_sum = lax.psum(dense_part.astype(jnp.bfloat16), "tp").astype(jnp.float32)
    layer_out = (resid.astype(jnp.float32) + moe + branch_weight[:, None] * dense_sum).astype(
        jnp.bfloat16
    )
    return (layer_out, new_state, new_conv_state)


def rcopy(src, dst, send, recv, ep, tp):
    return pltpu.make_async_remote_copy(
        src_ref=src,
        dst_ref=dst,
        send_sem=send,
        recv_sem=recv,
        device_id={"ep": ep, "tp": tp},
        device_id_type=pl.DeviceIdType.MESH,
    )


def dot(left, right):
    return jnp.dot(left, right, preferred_element_type=F32)


def layer_kernel(
    n, m, experts, tok_hbm, mg_hbm, fg_hbm, rt_hbm, st_hbm, cv_hbm, tap_hbm, rg_hbm, ig_hbm, dr_hbm,
    rw_hbm, bw_hbm, iw_hbm, gw_hbm, ow_hbm, dg_hbm, du_hbm, dd_hbm, eg, eu, ed, out, st_out, cv_out,
    toks, mgain, gain, rts, state, cvs, taps, rgb, igb, decay, rw, bw, maps, iw, gw, ow, dg, du, dd, wg, wu, wd,
    narr, psend, precv, pkeep, rsend, rrecv, pre, bd, mask, masks, mr, mall, osend, orecv, full, nfm,
    square, lacc, accg, accu, act, dpsend, dprecv, dkeep, drsend, drrecv, dact, dall,
    ysend, yrecv, kq, xsend, xrecv, xjoin, pbuf, zsend, zrecv, fblk, fin,
    lw, sent, tr, kr, r2, r3, ar, br, or_, zr, xr, mrv, r4, r5, cr, er, yr, hr, gr, fr,
):
    me, tp = lax.axis_index("ep"), lax.axis_index("tp")
    zs = n // 2
    z, c = me // 2, me % 2
    mate = 2 * z + 1 - c
    side = z // 2
    inner = lax.rem(z, 3) != 0
    outer = lax.rem(z, 3) == 0
    rows, width = out.shape
    q, ch = iw.shape
    g = q // m
    half = n * rows // 2
    h = dg.shape[1]

    def zp(k):
        return (z, z + 1 - 2 * lax.rem(z, 2), lax.rem(z + 2, zs), zs - 1 - z)[k]

    def tx(k):
        return (tp, tp + 1 - 2 * lax.rem(tp, 2), lax.rem(tp + 2, m), m - 1 - tp)[k]

    def lanes(e, size):
        return pl.ds(pl.multiple_of(e * size, LANES), size)

    count = [0]

    def load(src, dst):
        cp = pltpu.make_async_copy(src, dst, lw.at[count[0]])
        count[0] += 1
        cp.start()
        return cp

    sends = []

    def send(src, dst, recv, ep, t):
        cp = rcopy(src, dst, sent.at[0], recv, ep, t)
        cp.start()
        sends.append(cp)

    def arrive(buf, sem):
        rcopy(buf, buf, sem, sem, mate, tp).wait_recv()

    with jax.named_scope('enter'):
        ltok = load(tok_hbm, toks)
    lmain = [load(mg_hbm, mgain), load(iw_hbm, iw), load(gw_hbm, gw)]
    lrt = load(rt_hbm, rts)

    barrier = pltpu.get_barrier_semaphore()
    peers = [(lax.rem(me + d, n), tp) for d in range(1, n)]
    for k in range(1, m):
        peers += [(me, tx(k)), (mate, tx(k))]
    for ep, t in peers:
        pl.semaphore_signal(
            barrier, inc=1, device_id={"ep": ep, "tp": t}, device_id_type=pl.DeviceIdType.MESH
        )
    with jax.named_scope('tokwait'):
        ltok.wait()
    with jax.named_scope('greet'):
        pl.semaphore_wait(barrier, len(peers))

    send(toks.at[:, lanes(mate, q)], narr.at[me], tr.at[me], mate, tp)
    for k in (2, 1, 3):
        for core in range(2):
            to = 2 * zp(k) + core
            send(toks.at[:, lanes(to, q)], narr.at[me], tr.at[me], to, tp)
    narr[me] = toks[:, lanes(me, q)]
    lrt.wait()
    pair = jnp.concatenate([rts[...]] * zs, axis=1)
    line = lax.broadcasted_iota(jnp.int32, mask.shape, 0)
    lane = lax.broadcasted_iota(jnp.int32, mask.shape, 1) - lax.rem(me, zs) * rows
    taken = ((pair[0:1] == line) | (pair[1:2] == line)) & (lane >= 0) & (lane < rows)
    mask[...] = taken.astype(F32).astype(BF16)
    values = toks[...].astype(F32)
    inverse = lax.rsqrt(jnp.mean(values * values, axis=-1, keepdims=True) + epsilon)
    lsmall = [
        load(a, b)
        for a, b in (
            (cv_hbm, cvs), (tap_hbm, taps), (rg_hbm, rgb), (ig_hbm, igb), (st_hbm, state),
            (dr_hbm, decay), (fg_hbm, gain), (rw_hbm, rw), (bw_hbm, bw),
        )
    ]
    with jax.named_scope('lmain'):
        for cp in lmain:
            cp.wait()

    def reduction(psend, precv, keep, rsend, rrecv, r2, r3, part):
        def first(k):
            y = part(k)
            psend[k] = y[:rows].astype(BF16)
            send(psend.at[k], precv.at[k], r2.at[k], mate, tp)
            keep[k] = y[rows:]

        def target(k):
            return jnp.where(inner, zp(2), zp(1)) if k == 2 else zp(k)

        def out_of(k):
            return rcopy(
                rsend.at[k], rrecv.at[k], sent.at[0], r3.at[k], 2 * target(k) + c, tp
            )

        def second(k):
            arrive(precv.at[k], r2.at[k])
            if k == 0:
                keep[0] = keep[0] + precv[0].astype(F32)
                return
            rsend[k] = (keep[k] + precv[k].astype(F32)).astype(BF16)
            send(rsend.at[k], rrecv.at[k], r3.at[k], 2 * target(k) + c, tp)

        def last_outer():
            @pl.when(outer)
            def _():
                arrive(precv.at[3], r2.at[3])
                rsend[3] = (keep[3] + precv[3].astype(F32)).astype(BF16)
                out_of(3).start()

        def last_inner():
            @pl.when(inner)
            def _():
                arrive(precv.at[3], r2.at[3])
                arrive(rrecv.at[2], r3.at[2])
                total = keep[3] + precv[3].astype(F32) + rrecv[2].astype(F32)
                rsend[3] = total.astype(BF16)
                out_of(3).start()

            sends.append(out_of(3))

        def finish():
            with jax.named_scope("fin1"):
                arrive(rrecv.at[1], r3.at[1])
            keep[0] = keep[0] + rrecv[1].astype(F32)

            @pl.when(outer)
            def _():
                arrive(rrecv.at[2], r3.at[2])
                keep[0] = keep[0] + rrecv[2].astype(F32)

            with jax.named_scope("fin3"):
                arrive(rrecv.at[3], r3.at[3])
            return keep[0] + rrecv[3].astype(F32)

        return first, second, last_outer, last_inner, finish

    def part(k):
        zz = zp(k)
        for core in range(2):
            slot = 2 * zz + (1 - c if core == 0 else c)
            if k or core == 0:
                arrive(narr.at[slot], tr.at[slot])
        x = jnp.concatenate([narr[2 * zz + 1 - c], narr[2 * zz + c]], axis=0)
        x = (x.astype(F32) * mgain[me]).astype(BF16)
        return jnp.concatenate([dot(x, iw[...]), dot(x, gw[...])], axis=1)

    first, second, last_outer, last_inner, finish = reduction(
        psend, precv, pkeep, rsend, rrecv, r2, r3, part
    )
    with jax.named_scope("project"):
        first(0)
        lbig = [load(a, b) for a, b in ((ow_hbm, ow), (dg_hbm, dg), (du_hbm, du), (dd_hbm, dd))]
        lexp = [load(eg, wg), load(eu, wu)]
        ldown = [load(ed.at[:, pl.ds(i * q, q)], wd.at[i]) for i in range(n)]
        for k in (2, 1):
            first(k)
            second(k)
        first(3)
        last_outer()
        last_inner()
        second(0)
    with jax.named_scope("prepare"):
        for cp in lsmall:
            cp.wait()
        per = LANES // rgb.shape[1]
        size = rgb.shape[1]
        place_r = lax.broadcasted_iota(jnp.int32, (size, LANES), 0)
        place_c = lax.broadcasted_iota(jnp.int32, (size, LANES), 1)
        for p in range(ch // LANES):
            for s in range(per):
                move = (place_c == place_r + s * size).astype(F32).astype(BF16)
                for gate, blocks in enumerate((rgb, igb)):
                    bd[p, s * size : (s + 1) * size, gate * LANES : (gate + 1) * LANES] = dot(
                        blocks[p * per + s], move
                    ).astype(BF16)
        taken = cvs.shape[0]
        total = cvs[0].astype(F32) * taps[0:1, :]
        for j in range(1, taken):
            total += cvs[j].astype(F32) * taps[j : j + 1, :]
        pre[...] = total
        for j in range(1, taken):
            cv_out[j - 1] = cvs[j]
        for e in range(n):
            at = slice(e * q, (e + 1) * q)
            line = jnp.broadcast_to(bw[...].astype(F32).reshape(1, width)[:, at], (experts, q))
            maps[:, at] = jnp.concatenate([rw[:, at].astype(F32), line], axis=0).astype(BF16)
        accg[...] = jnp.zeros_like(accg)
        accu[...] = jnp.zeros_like(accu)
        lacc[...] = jnp.zeros_like(lacc)
        square[...] = jnp.zeros_like(square)

    with jax.named_scope("recur"):
        both = finish() * inverse
        xb = both[:, :ch].astype(BF16)
        conv = (pre[...] + xb.astype(F32) * taps[taken : taken + 1, :]).astype(BF16)
        cv_out[taken - 1] = xb
        for p in range(ch // LANES):
            at = slice(p * LANES, (p + 1) * LANES)
            gates = jax.nn.sigmoid(dot(conv[:, at], bd[p]))
            log_decay = -decay_scale * gates[:, :LANES] * decay[:, at]
            ratio = jnp.tanh(-log_decay)
            scale = jnp.sqrt(2.0 * ratio / (1.0 + ratio))
            new = jnp.exp(log_decay) * state[:, at] + scale * gates[:, LANES:] * conv[:, at].astype(F32)
            st_out[:, at] = new
            gb = both[:, ch + p * LANES : ch + (p + 1) * LANES].astype(BF16).astype(F32)
            mr[:, at] = (new * jax.nn.gelu(gb)).astype(BF16)

    with jax.named_scope("mix"):
        send(mr, mall.at[me], br.at[0], mate, tp)
        for k in range(1, zs):
            send(mr, mall.at[me], ar.at[k], 2 * zp(k) + c, tp)
        mall[me] = mr[...]
        for cp in lbig:
            cp.wait()

        def pass_on(k):
            slot = 2 * zp(k) + c
            arrive(mall.at[slot], ar.at[k])
            send(mall.at[slot], mall.at[slot], br.at[k], mate, tp)

        def mixed(i):
            for k in (2 * i, 2 * i + 1):
                arrive(mall.at[2 * zp(k) + 1 - c], br.at[k])
            which = side if i == 0 else 1 - side
            x = mall[pl.ds(which * zs, zs)].reshape(half, ch)
            y = dot(x, ow[...]).astype(BF16)
            for t in range(m):
                osend[t, i] = y[:, t * g : (t + 1) * g]
            for k in (3, 1, 2):
                send(osend.at[tx(k), i], orecv.at[k, i], or_.at[k, i], me, tx(k))

        def summed(i):
            which = side if i == 0 else 1 - side
            raw = narr[pl.ds(which * zs, zs), :, lanes(tp, g)].reshape(half, g)
            total = raw.astype(F32) + osend[tp, i].astype(F32)
            for k in range(1, m):
                arrive(orecv.at[k, i], or_.at[k, i])
                total += orecv[k, i].astype(F32)
            full[tp, me, which] = total.astype(BF16)

    direct = [(k, 1) for k in range(zs)]

    def sided(k, i):
        return side if (k < 2) == (i == 0) else 1 - side

    def spread(k, i):
        slot, s = 2 * zp(k) + c, sided(k, i)
        at = full.at[tp, slot, s]
        for d in (3, 1, 2) if (k, i) in direct else (1, 2):
            send(at, at, xr.at[d, k, s], me, tx(d))
        send(at, at, mrv.at[0, k, s], mate, tp)

    def own(i):
        at = full.at[tp, me, sided(0, i)]
        s = sided(0, i)
        for k in (3, 2, 1):
            send(at, at, zr.at[k, s], 2 * zp(k) + c, tp)
        spread(0, i)

    def landed(k, i):
        s = sided(k, i)
        arrive(full.at[tp, 2 * zp(k) + c, s], zr.at[k, s])
        spread(k, i)

    def relay(k, i):
        slot, s = 2 * zp(k) + c, sided(k, i)
        early = tx(1) * (1 - s) + tx(2) * s
        late = tx(2) * (1 - s) + tx(1) * s
        at = full.at[early, slot, s]
        arrive(at, xr.at[1 + s, k, s])
        if (k, i) not in direct:
            send(at, at, xr.at[3, k, s], me, late)
        send(at, at, mrv.at[1 + s, k, s], mate, tp)
        at = full.at[late, slot, s]
        arrive(at, xr.at[2 - s, k, s])
        send(at, at, mrv.at[2 - s, k, s], mate, tp)

    def relay_far(k, i):
        slot, s = 2 * zp(k) + c, sided(k, i)
        at = full.at[tx(3), slot, s]
        arrive(at, xr.at[3, k, s])
        send(at, at, mrv.at[3, k, s], mate, tp)

    def absorb(e, s, keep):
        parts = []
        for t in range(m):
            at = slice(t * g, (t + 1) * g)
            v = full[t, e, s].astype(F32)
            square[s] += v * v
            parts.append((v * gain[e, :, at]).astype(BF16))
        x = jnp.concatenate(parts, axis=1)
        if keep:
            nfm[s] = x
        accg[s] += dot(x, wg[e])
        accu[s] += dot(x, wu[e])
        lacc[s] += lax.dot_general(
            x, maps[:, lanes(e, q)], (((1,), (1,)), ((), ())), preferred_element_type=F32
        )

    def absorb_own(k, i):
        absorb(2 * zp(k) + c, sided(k, i), k == 0)

    def absorb_mate(k, i):
        e, s = 2 * zp(k) + 1 - c, sided(k, i)
        for d in range(m):
            arrive(full.at[tx(d), e, s], mrv.at[d, k, s])
        absorb(e, s, False)

    def dpart(k):
        s = zp(k) // 2
        x = []
        for core in range(2):
            at = lax.rem(zp(k), 2) * 2 + (1 - c if core == 0 else c)
            x.append(nfm[s, pl.ds(pl.multiple_of(at * rows, rows), rows), :])
        x = jnp.concatenate(x, axis=0)
        return jnp.concatenate([dot(x, dg[...]), dot(x, du[...])], axis=1)

    dfirst, dsecond, dlast_outer, dlast_inner, dfinish = reduction(
        dpsend, dprecv, dkeep, drsend, drrecv, r4, r5, dpart
    )

    with jax.named_scope("mix_near"):
        pass_on(1)
        mixed(0)
        for k in range(zs):
            for core in range(2):
                if k or core:
                    to = 2 * zp(k) + (c if core == 0 else 1 - c)
                    send(mask, masks.at[me], kr.at[me], to, tp)
        masks[me] = mask[...]
    with jax.named_scope("mix_sum"):
        pass_on(2)
        summed(0)
    with jax.named_scope("gather"):
        own(0)
        pass_on(3)
        mixed(1)
        landed(1, 0)
        relay(0, 0)
        landed(2, 0)
        landed(3, 0)
        relay(1, 0)
        summed(1)
        own(1)
        relay(2, 0)
        relay_far(0, 0)
        for cp in lexp:
            cp.wait()
        absorb_own(0, 0)
        dfirst(0)
        relay(3, 0)
        relay_far(1, 0)
        dfirst(1)
        absorb_own(1, 0)
        absorb_mate(0, 0)
        relay(0, 1)
        relay_far(0, 1)
        absorb_own(0, 1)
        dfirst(2)
        dsecond(1)
        dfirst(3)
        landed(1, 1)
        relay_far(2, 0)
        dsecond(2)
        dlast_outer()
        absorb_own(2, 0)
        absorb_mate(1, 0)
        landed(2, 1)
        landed(3, 1)
        relay(1, 1)
        relay_far(3, 0)
        absorb_own(3, 0)
        absorb_mate(2, 0)
        relay(2, 1)
        absorb_mate(3, 0)
        relay_far(1, 1)
        absorb_own(1, 1)
        relay(3, 1)
        dlast_inner()
        absorb_mate(0, 1)
        relay_far(2, 1)
        absorb_own(2, 1)
        absorb_mate(1, 1)
        relay_far(3, 1)
        absorb_own(3, 1)
        absorb_mate(2, 1)
        dsecond(0)
        absorb_mate(3, 1)

    scale = []
    with jax.named_scope("dense_act"):
        for s in (1 - side, side):
            scale.append(
                lax.rsqrt(jnp.sum(square[s], axis=-1, keepdims=True) / width + epsilon)
            )
            square[s, :, 0:1] = scale[-1]
        at = pl.ds(pl.multiple_of(lax.rem(me, zs) * rows, rows), rows)
        both = dfinish() * square[side, at, 0:1]
        first_half = both[:, :h]
        dact[...] = (first_half * jax.nn.sigmoid(first_half) * both[:, h:]).astype(BF16)
        for k in (3, 2, 1):
            send(dact, dall.at[me], cr.at[k], 2 * zp(k) + c, tp)
        send(dact, dall.at[me], er.at[0], mate, tp)
        dall[me] = dact[...]
        for k in range(zs):
            for core in range(2):
                if k or core:
                    src = 2 * zp(k) + (c if core == 0 else 1 - c)
                    arrive(masks.at[src], kr.at[src])
    weight, branch = [], []

    def activate(ih):
        s = 1 - side if ih == 0 else side
        logits = lacc[s] * scale[ih]
        chosen = jnp.sum(masks[pl.ds(s * zs, zs)].astype(F32), axis=0).T
        named = logits * chosen
        other = jnp.sum(named, axis=-1, keepdims=True) - named
        share = (jax.nn.sigmoid(logits - other) * chosen).astype(BF16).astype(F32)
        at = lax.broadcasted_iota(jnp.int32, share.shape, 1)
        weight.append(jnp.sum(jnp.where(at == me, share, 0.0), axis=-1, keepdims=True))
        branch.append(jax.nn.sigmoid(logits[:, experts : experts + 1]))
        gate = accg[s] * scale[ih]
        act[ih] = (gate * jax.nn.sigmoid(gate) * (accu[s] * scale[ih])).astype(BF16)

    order = [lax.rem(z + 1 + i, m) for i in range(m)]

    def down(ih):
        for i in range(m):
            y = dot(act[ih], wd[2 * order[i] + 1 - c]) * weight[ih]
            ysend[i, ih] = y.astype(BF16)
            send(ysend.at[i, ih], yrecv.at[i, ih], yr.at[i, ih], mate, tp)
        for i in range(m):
            y = dot(act[ih], wd[2 * order[i] + c]) * weight[ih]
            for t in range(m):
                kq[i, ih, t] = y[:, t * g : (t + 1) * g]

    joined = [(i, 1) for i in range(m - 1)]

    def pass_part(k, i, ih, part, to):
        send(part, xrecv.at[k, i, ih], hr.at[k, i, ih], me, tx(to))

    def join(i, ih):
        lead = 1 + (i + ih) % 2
        arrive(xrecv.at[3, i, ih], hr.at[3, i, ih])
        total = kq[i, ih, tx(3 - lead)] + xrecv[3, i, ih].astype(F32)
        xjoin[i, ih] = total.astype(BF16)
        pass_part(3 - lead, i, ih, xjoin.at[i, ih], 3 - lead)

    def forward(i, ih, extra=None):
        arrive(yrecv.at[i, ih], yr.at[i, ih])
        for t in range(m):
            at = slice(t * g, (t + 1) * g)
            total = kq[i, ih, t] + yrecv[i, ih, :, at].astype(F32)
            if extra is not None:
                total += extra[:, at]
            kq[i, ih, t] = total
            xsend[i, ih, t] = total.astype(BF16)
        if (i, ih) not in joined:
            for k in (3, 1, 2):
                pass_part(k, i, ih, xsend.at[i, ih, tx(k)], k)
        else:
            lead = 1 + (i + ih) % 2
            pass_part(3, i, ih, xsend.at[i, ih, tx(3)], lead)
            pass_part(lead, i, ih, xsend.at[i, ih, tx(lead)], lead)

    def settle(i, ih):
        total = kq[i, ih, tp]
        for k in (1, 2) if (i, ih) in joined else range(1, m):
            arrive(xrecv.at[k, i, ih], hr.at[k, i, ih])
            total += xrecv[k, i, ih].astype(F32)
        pbuf[i, ih] = total.reshape(2, 2 * rows, g)
        for k in (2, 3) if ih == 0 else (1,):
            zsend[k, i] = pbuf[i, ih, lax.rem(zp(k), 2)].astype(BF16)

    def away(k, i):
        send(zsend.at[k, i], zrecv.at[k, i], gr.at[k, i], 2 * zp(k) + c, tp)

    for cp in ldown:
        cp.wait()
    with jax.named_scope("down_far"):
        activate(0)
        down(0)
        activate(1)
    def dense_pass():
        for k in (1, 2, 3):
            slot = 2 * zp(k) + c
            arrive(dall.at[slot], cr.at[k])
            send(dall.at[slot], dall.at[slot], er.at[k], mate, tp)

    def dense_ready():
        for k in range(zs):
            arrive(dall.at[2 * zp(k) + 1 - c], er.at[k])

    def dense_forward(ih):
        s = 1 - side if ih == 0 else side
        x = dall[pl.ds(s * zs, zs)].reshape(half, h)
        forward(m - 1, ih, dot(x, dd[...]) * branch[ih])

    def leave(i, ih):
        settle(i, ih)
        for k in (3, 2) if ih == 0 else (1,):
            away(k, i)

    with jax.named_scope("tail"):
        with jax.named_scope("f00"):
            forward(0, 0)
        with jax.named_scope("f10"):
            forward(1, 0)
        with jax.named_scope("f20"):
            forward(2, 0)
        with jax.named_scope("d1"):
            down(1)
        with jax.named_scope("f01"):
            forward(0, 1)
        with jax.named_scope("f11"):
            forward(1, 1)
        with jax.named_scope("f21"):
            forward(2, 1)
        with jax.named_scope("l00"):
            leave(0, 0)
        with jax.named_scope("dp"):
            dense_pass()
        with jax.named_scope("l10"):
            leave(1, 0)
        with jax.named_scope("l20"):
            leave(2, 0)
        with jax.named_scope("dr"):
            dense_ready()
        with jax.named_scope("df0"):
            dense_forward(0)
        with jax.named_scope("df1"):
            dense_forward(1)
        with jax.named_scope("j01"):
            join(0, 1)
        with jax.named_scope("j11"):
            join(1, 1)
        with jax.named_scope("j21"):
            join(2, 1)
        with jax.named_scope("l30"):
            leave(3, 0)
        with jax.named_scope("l01"):
            leave(0, 1)
        with jax.named_scope("l11"):
            leave(1, 1)
        with jax.named_scope("l21"):
            leave(2, 1)
        with jax.named_scope("l31"):
            leave(3, 1)

    with jax.named_scope("last_sum"):
        for k in range(1, zs):
            for i in range(m):
                arrive(zrecv.at[k, i], gr.at[k, i])
        spot = lax.rem(z, 2)
        for j in range(m):
            total = pbuf[lax.rem(j - z - 1 + 2 * m, m), 1, spot]
            for k in range(1, zs):
                total += zrecv[k, lax.rem(j - zp(k) - 1 + 2 * m, m)].astype(F32)
            resid = full[tp, 2 * j + c, side, pl.ds(pl.multiple_of(2 * rows * spot, rows), 2 * rows), :]
            total = (total + resid.astype(F32)).astype(BF16)
            for core in range(2):
                fblk[core, j] = total[core * rows : (core + 1) * rows]
    with jax.named_scope("last_gather"):
        for k in (3, 1, 2, 0):
            for dc in range(2):
                if k or dc:
                    core = c if dc == 0 else 1 - c
                    send(
                        fblk.at[core], fin.at[c, tp], fr.at[dc, k], 2 * z + core, tx(k)
                    )
        fin[c, tp] = fblk[c]
        for k in (0, 1, 2, 3):
            for dc in range(2):
                if k or dc:
                    core = c if dc == 0 else 1 - c
                    arrive(fin.at[core, tx(k)], fr.at[dc, k])
        for core in range(2):
            for t in range(m):
                for j in range(m):
                    base = (2 * j + core) * q + t * g
                    out[:, base : base + g] = fin[core, t, j]
    with jax.named_scope("drain"):
        for cp in sends:
            cp.wait_send()


def deliver_kernel(a, b, c, to_a, to_b, to_c, sems):
    copies = [
        pltpu.make_async_copy(src, dst, sems.at[i])
        for i, (src, dst) in enumerate(((a, to_a), (b, to_b), (c, to_c)))
    ]
    for cp in copies:
        cp.start()
    for cp in copies:
        cp.wait()


def in_kernel(
    n, m, tokens, recur_state, conv_state, mix_gain, in_weight, gate_weight, conv_taps,
    recur_gate_blocks, input_gate_blocks, decay_rate, out_weight, ffn_gain, router_weight, routes,
    expert_gate, expert_up, expert_down, dense_gate, dense_up, dense_down, branch_gate,
):
    rows, width = tokens.shape
    q, ch = in_weight.shape
    experts = router_weight.shape[1]
    h, f = dense_gate.shape[1], expert_down.shape[1]
    g, zs, b = q // m, n // 2, n * rows
    half = b // 2
    lines = 2 * experts
    past = (conv_state.shape[1], rows, ch)
    hbm = pl.BlockSpec(memory_space=pl.ANY)
    vm = pl.BlockSpec(memory_space=pltpu.VMEM)
    v = pltpu.VMEM

    def flags(*shapes):
        return [pltpu.SemaphoreType.DMA(s) for s in shapes]

    operands = (
        tokens, mix_gain.reshape(n, 1, q), ffn_gain.reshape(n, 1, q), routes.T, recur_state,
        conv_state.transpose(1, 0, 2), conv_taps, recur_gate_blocks, input_gate_blocks,
        decay_rate.reshape(1, ch), router_weight.T, branch_gate,
        in_weight, gate_weight, out_weight, dense_gate, dense_up, dense_down,
        expert_gate.reshape(n, q, f), expert_up.reshape(n, q, f), expert_down[0],
    )
    results = (
        jax.ShapeDtypeStruct((rows, width), BF16),
        jax.ShapeDtypeStruct((rows, ch), F32),
        jax.ShapeDtypeStruct(past, BF16),
    )
    layer_out, new_state, window = pl.pallas_call(
        functools.partial(layer_kernel, n, m, experts),
        out_shape=tuple(pltpu.VMEM(r.shape, r.dtype) for r in results),
        in_specs=[hbm] * len(operands),
        out_specs=(vm, vm, vm),
        scratch_shapes=[
            v((rows, width), BF16), v((n, 1, q), F32), v((n, 1, q), F32), v(routes.shape[::-1], jnp.int32),
            v((rows, ch), F32), v(past, BF16), v(conv_taps.shape, F32),
            v(recur_gate_blocks.shape, BF16), v(input_gate_blocks.shape, BF16), v((1, ch), F32),
            v((experts, width), BF16), v((width,), BF16), v((lines, width), BF16), v((q, ch), BF16), v((q, ch), BF16), v((ch, q), BF16),
            v((q, h), BF16), v((q, h), BF16), v((h, q), BF16),
            v((n, q, f), BF16), v((n, q, f), BF16), v((n, f, q), BF16),
            v((n, rows, q), BF16), v((zs, rows, 2 * ch), BF16), v((zs, rows, 2 * ch), BF16),
            v((zs, rows, 2 * ch), F32), v((zs, rows, 2 * ch), BF16), v((zs, rows, 2 * ch), BF16),
            v((rows, ch), F32), v((ch // LANES, LANES, 2 * LANES), BF16),
            v((lines, half), BF16), v((n, lines, half), BF16),
            v((rows, ch), BF16), v((n, rows, ch), BF16),
            v((m, 2, half, g), BF16), v((m, 2, half, g), BF16),
            v((m, n, 2, half, g), BF16), v((2, half, q), BF16),
            v((2, half, g), F32), v((2, half, lines), F32),
            v((2, half, f), F32), v((2, half, f), F32), v((2, half, f), BF16),
            v((zs, rows, 2 * h), BF16), v((zs, rows, 2 * h), BF16), v((zs, rows, 2 * h), F32),
            v((zs, rows, 2 * h), BF16), v((zs, rows, 2 * h), BF16),
            v((rows, h), BF16), v((n, rows, h), BF16),
            v((m, 2, half, q), BF16), v((m, 2, half, q), BF16), v((m, 2, m, half, g), F32),
            v((m, 2, m, half, g), BF16), v((m, m, 2, half, g), BF16), v((m - 1, 2, half, g), BF16),
            v((m, 2, 2, 2 * rows, g), F32),
            v((zs, m, 2 * rows, g), BF16), v((zs, m, 2 * rows, g), BF16),
            v((2, m, rows, g), BF16), v((2, m, m, rows, g), BF16),
        ]
        + flags(
            (32,), (1,), (n,), (n,), (zs,), (zs,), (zs,), (zs,), (m, 2), (zs, 2), (m, zs, 2), (m, zs, 2),
            (zs,), (zs,), (zs,), (zs,), (m, 2), (m, m, 2), (zs, m), (2, m),
        ),
        compiler_params=pltpu.CompilerParams(
            collective_id=0, has_side_effects=True, vmem_limit_bytes=58 * 1024 * 1024
        ),
        name="layer",
    )(*operands)
    held = [pltpu.with_memory_space_constraint(a, pltpu.VMEM) for a in (layer_out, new_state, window)]
    layer_out, new_state, window = pl.pallas_call(
        deliver_kernel,
        out_shape=results,
        in_specs=[vm] * 3,
        out_specs=(hbm,) * 3,
        scratch_shapes=[pltpu.SemaphoreType.DMA((3,))],
        name="deliver",
    )(*held)
    return (layer_out, new_state, window.transpose(1, 0, 2))


def solution(mesh):
    in_specs = (
        P("ep", None),
        P("ep", "tp"),
        P("ep", None, "tp"),
        P(),
        P("ep", "tp"),
        P("ep", "tp"),
        P(None, "tp"),
        P("tp", None, None),
        P("tp", None, None),
        P("tp"),
        P("tp", "ep"),
        P(),
        P(),
        P("ep", None),
        P("ep", None, "tp"),
        P("ep", None, "tp"),
        P("ep", "tp", None),
        P("ep", "tp"),
        P("ep", "tp"),
        P("tp", "ep"),
        P(),
    )
    out_specs = (P("ep", None), P("ep", "tp"), P("ep", None, "tp"))
    n, m = mesh.shape["ep"], mesh.shape["tp"]

    def body(*args):
        tokens, blocks, router, dense = args[0], args[7], args[12], args[17]
        q = tokens.shape[1] // n
        fits = m == 4 and n == 2 * m and n == router.shape[1] and q % (m * LANES) == 0
        fits = fits and tokens.shape[0] % 16 == 0 and dense.shape[1] % LANES == 0
        fits = fits and LANES % blocks.shape[1] == 0
        if fits:
            return in_kernel(n, m, *args)
        return on_device(*args)

    return jax.shard_map(
        body, mesh=mesh, in_specs=in_specs, out_specs=out_specs, check_vma=False
    )
```

```python
import functools

import jax
import jax.numpy as jnp
from jax import lax
from jax.experimental import pallas as pl
from jax.experimental.pallas import tpu as pltpu
from jax.sharding import PartitionSpec as P

TOP_K = 2
LANES = 128
F32 = jnp.float32
BF16 = jnp.bfloat16


epsilon = 1e-06
decay_scale = 8.0


def rms_scale(rows, gain):
    values = rows.astype(jnp.float32)
    inverse = lax.rsqrt(jnp.mean(values * values, axis=-1, keepdims=True) + epsilon)
    return (values * inverse * gain).astype(jnp.bfloat16)


def on_device(
    tokens,
    recur_state,
    conv_state,
    mix_gain,
    in_weight,
    gate_weight,
    conv_taps,
    recur_gate_blocks,
    input_gate_blocks,
    decay_rate,
    out_weight,
    ffn_gain,
    router_weight,
    routes,
    expert_gate,
    expert_up,
    expert_down,
    dense_gate,
    dense_up,
    dense_down,
    branch_gate,
):
    batch_rows, width = tokens.shape
    channels = in_weight.shape[1]
    normed = rms_scale(tokens, mix_gain)
    arrived = lax.all_to_all(normed, "ep", split_axis=1, concat_axis=0, tiled=True)
    joined = jnp.concatenate([in_weight, gate_weight], axis=1)
    summed = lax.psum_scatter(
        jnp.dot(arrived, joined, preferred_element_type=jnp.float32).astype(jnp.bfloat16),
        "ep",
        scatter_dimension=0,
        tiled=True,
    ).astype(jnp.float32)
    x_sum, gate_sum = (summed[:, :channels], summed[:, channels:])
    x_branch = x_sum.astype(jnp.bfloat16)
    gate_branch = gate_sum.astype(jnp.bfloat16)
    window = jnp.concatenate([conv_state, x_branch[:, None, :]], axis=1)
    conv_out = jnp.sum(window.astype(jnp.float32) * conv_taps[None], axis=1).astype(jnp.bfloat16)
    new_conv_state = window[:, 1:, :]
    blocks = conv_out.reshape(batch_rows, recur_gate_blocks.shape[0], recur_gate_blocks.shape[1])
    recur_gate = jax.nn.sigmoid(
        jnp.einsum(
            "bhi,hij->bhj", blocks, recur_gate_blocks, preferred_element_type=jnp.float32
        ).reshape(batch_rows, channels)
    )
    input_gate = jax.nn.sigmoid(
        jnp.einsum(
            "bhi,hij->bhj", blocks, input_gate_blocks, preferred_element_type=jnp.float32
        ).reshape(batch_rows, channels)
    )
    log_decay = -decay_scale * recur_gate * decay_rate
    new_state = jnp.exp(log_decay) * recur_state + jnp.sqrt(
        -jnp.expm1(2.0 * log_decay)
    ) * input_gate * conv_out.astype(jnp.float32)
    mixer_rows = (new_state * jax.nn.gelu(gate_branch.astype(jnp.float32))).astype(jnp.bfloat16)
    mixer_part = jnp.dot(
        mixer_rows,
        lax.all_gather(out_weight, "ep", axis=1, tiled=True),
        preferred_element_type=jnp.float32,
    )
    resid = (
        tokens.astype(jnp.float32)
        + lax.psum(mixer_part.astype(jnp.bfloat16), "tp").astype(jnp.float32)
    ).astype(jnp.bfloat16)
    normed_ffn = rms_scale(resid, ffn_gain)
    router_logits = jnp.dot(normed_ffn, router_weight, preferred_element_type=jnp.float32)
    experts = router_logits.shape[1]
    expert_ids = lax.broadcasted_iota(jnp.int32, (batch_rows, TOP_K, experts), 2)
    picked = jnp.sum(
        jnp.where(routes[:, :, None] == expert_ids, router_logits[:, None, :], 0.0), axis=2
    )
    route_weight = jax.nn.sigmoid(picked - picked[:, ::-1]).astype(jnp.bfloat16)
    capacity = 2 * batch_rows * TOP_K // experts
    flat_ids = routes.reshape(batch_rows * TOP_K)
    onehot = (
        flat_ids[:, None] == lax.broadcasted_iota(jnp.int32, (batch_rows * TOP_K, experts), 1)
    ).astype(jnp.int32)
    rank = jnp.sum((jnp.cumsum(onehot, axis=0) - onehot) * onehot, axis=1)
    slot_of = (flat_ids * capacity + rank).reshape(batch_rows, TOP_K)
    slot_rows = lax.broadcasted_iota(jnp.int32, (experts * capacity, batch_rows), 0)
    slot_cols = lax.broadcasted_iota(jnp.int32, (batch_rows, experts * capacity), 1)
    dispatch = jnp.zeros((experts * capacity, batch_rows), jnp.bfloat16)
    combine = jnp.zeros((batch_rows, experts * capacity), jnp.bfloat16)
    for pick in range(TOP_K):
        dispatch = dispatch + (slot_rows == slot_of[None, :, pick]).astype(jnp.bfloat16)
        combine = combine + jnp.where(
            slot_cols == slot_of[:, pick : pick + 1],
            route_weight[:, pick : pick + 1],
            jnp.zeros((), jnp.bfloat16),
        )
    outgoing = (
        jnp.dot(dispatch, normed_ffn, preferred_element_type=jnp.float32)
        .astype(jnp.bfloat16)
        .reshape(experts, capacity, width)
    )
    gate_local = expert_gate[0]
    up_local = expert_up[0]
    down_local = expert_down[0]
    arrived_rows = lax.all_to_all(outgoing, "ep", split_axis=0, concat_axis=0, tiled=True)
    sources, items, features = arrived_rows.shape
    rows = arrived_rows.reshape(sources * items, features)
    first = jnp.dot(rows, gate_local, preferred_element_type=jnp.float32)
    second = jnp.dot(rows, up_local, preferred_element_type=jnp.float32)
    act = (jax.nn.silu(first) * second).astype(jnp.bfloat16)
    partial_value = jnp.dot(act, down_local, preferred_element_type=jnp.float32)
    total = lax.psum(partial_value.astype(jnp.bfloat16), "tp")
    returned = lax.all_to_all(
        total.reshape(sources, items, total.shape[1]), "ep", split_axis=0, concat_axis=0, tiled=True
    )
    moe = jnp.dot(
        combine,
        returned.reshape(experts * capacity, returned.shape[2]),
        preferred_element_type=jnp.float32,
    )
    dense_arrived = lax.all_to_all(normed_ffn, "ep", split_axis=1, concat_axis=0, tiled=True)
    dense_joined = jnp.concatenate([dense_gate, dense_up], axis=1)
    dense_summed = lax.psum_scatter(
        jnp.dot(dense_arrived, dense_joined, preferred_element_type=jnp.float32).astype(
            jnp.bfloat16
        ),
        "ep",
        scatter_dimension=0,
        tiled=True,
    ).astype(jnp.float32)
    dense_first = dense_summed[:, : dense_gate.shape[1]]
    dense_second = dense_summed[:, dense_gate.shape[1] :]
    dense_act = (jax.nn.silu(dense_first) * dense_second).astype(jnp.bfloat16)
    dense_part = jnp.dot(
        dense_act,
        lax.all_gather(dense_down, "ep", axis=1, tiled=True),
        preferred_element_type=jnp.float32,
    )
    branch_weight = jax.nn.sigmoid(
        jnp.dot(normed_ffn, branch_gate, preferred_element_type=jnp.float32)
    )
    dense_sum = lax.psum(dense_part.astype(jnp.bfloat16), "tp").astype(jnp.float32)
    layer_out = (resid.astype(jnp.float32) + moe + branch_weight[:, None] * dense_sum).astype(
        jnp.bfloat16
    )
    return (layer_out, new_state, new_conv_state)


def rcopy(src, dst, send, recv, ep, tp):
    return pltpu.make_async_remote_copy(
        src_ref=src,
        dst_ref=dst,
        send_sem=send,
        recv_sem=recv,
        device_id={"ep": ep, "tp": tp},
        device_id_type=pl.DeviceIdType.MESH,
    )


def dot(left, right):
    return jnp.dot(left, right, preferred_element_type=F32)


def layer_kernel(
    n, m, experts, tok_hbm, mg_hbm, fg_hbm, rt_hbm, st_hbm, cv_hbm, tap_hbm, rg_hbm, ig_hbm, dr_hbm,
    rw_hbm, bw_hbm, iw_hbm, gw_hbm, ow_hbm, dg_hbm, du_hbm, dd_hbm, eg, eu, ed, out, st_out, cv_out,
    toks, mgain, gain, rts, state, cvs, taps, rgb, igb, decay, rw, bw, maps, iw, gw, ow, dg, du, dd, wg, wu, wd,
    narr, psend, precv, pkeep, rsend, rrecv, pre, bd, mask, masks, mr, mall, osend, orecv, full, nfm,
    square, lacc, accg, accu, act, dpsend, dprecv, dkeep, drsend, drrecv, dact, dall,
    ysend, yrecv, kq, xsend, xrecv, xjoin, pbuf, zsend, zrecv, fblk, fin,
    lw, sent, tr, kr, r2, r3, ar, br, or_, zr, xr, mrv, r4, r5, cr, er, yr, hr, gr, fr,
):
    me, tp = lax.axis_index("ep"), lax.axis_index("tp")
    zs = n // 2
    z, c = me // 2, me % 2
    mate = 2 * z + 1 - c
    side = z // 2
    inner = lax.rem(z, 3) != 0
    outer = lax.rem(z, 3) == 0
    rows, width = out.shape
    q, ch = iw.shape
    g = q // m
    half = n * rows // 2
    h = dg.shape[1]

    def zp(k):
        return (z, z + 1 - 2 * lax.rem(z, 2), lax.rem(z + 2, zs), zs - 1 - z)[k]

    def tx(k):
        return (tp, tp + 1 - 2 * lax.rem(tp, 2), lax.rem(tp + 2, m), m - 1 - tp)[k]

    def lanes(e, size):
        return pl.ds(pl.multiple_of(e * size, LANES), size)

    count = [0]

    def load(src, dst):
        cp = pltpu.make_async_copy(src, dst, lw.at[count[0]])
        count[0] += 1
        cp.start()
        return cp

    sends = []

    def send(src, dst, recv, ep, t):
        cp = rcopy(src, dst, sent.at[0], recv, ep, t)
        cp.start()
        sends.append(cp)

    def arrive(buf, sem):
        rcopy(buf, buf, sem, sem, mate, tp).wait_recv()

    with jax.named_scope('enter'):
        ltok = load(tok_hbm, toks)
    lmain = [load(mg_hbm, mgain), load(iw_hbm, iw), load(gw_hbm, gw)]
    lrt = load(rt_hbm, rts)

    barrier = pltpu.get_barrier_semaphore()
    peers = [(lax.rem(me + d, n), tp) for d in range(1, n)]
    for k in range(1, m):
        peers += [(me, tx(k)), (mate, tx(k))]
    for ep, t in peers:
        pl.semaphore_signal(
            barrier, inc=1, device_id={"ep": ep, "tp": t}, device_id_type=pl.DeviceIdType.MESH
        )
    with jax.named_scope('tokwait'):
        ltok.wait()
    with jax.named_scope('greet'):
        pl.semaphore_wait(barrier, len(peers))

    send(toks.at[:, lanes(mate, q)], narr.at[me], tr.at[0], mate, tp)
    for k in (2, 1, 3):
        for core in range(2):
            to = 2 * zp(k) + core
            send(toks.at[:, lanes(to, q)], narr.at[me], tr.at[k], to, tp)
    narr[me] = toks[:, lanes(me, q)]
    lrt.wait()
    pair = jnp.concatenate([rts[...]] * zs, axis=1)
    line = lax.broadcasted_iota(jnp.int32, mask.shape, 0)
    lane = lax.broadcasted_iota(jnp.int32, mask.shape, 1) - lax.rem(me, zs) * rows
    taken = ((pair[0:1] == line) | (pair[1:2] == line)) & (lane >= 0) & (lane < rows)
    mask[...] = taken.astype(F32).astype(BF16)
    values = toks[...].astype(F32)
    inverse = lax.rsqrt(jnp.mean(values * values, axis=-1, keepdims=True) + epsilon)
    lsmall = [
        load(a, b)
        for a, b in (
            (cv_hbm, cvs), (tap_hbm, taps), (rg_hbm, rgb), (ig_hbm, igb), (st_hbm, state),
            (dr_hbm, decay), (fg_hbm, gain), (rw_hbm, rw), (bw_hbm, bw),
        )
    ]
    with jax.named_scope('lmain'):
        for cp in lmain:
            cp.wait()

    def reduction(psend, precv, keep, rsend, rrecv, r2, r3, part):
        def first(k):
            y = part(k)
            psend[k] = y[:rows].astype(BF16)
            send(psend.at[k], precv.at[k], r2.at[k], mate, tp)
            keep[k] = y[rows:]

        def target(k):
            return jnp.where(inner, zp(2), zp(1)) if k == 2 else zp(k)

        def out_of(k):
            return rcopy(
                rsend.at[k], rrecv.at[k], sent.at[0], r3.at[k], 2 * target(k) + c, tp
            )

        def second(k):
            arrive(precv.at[k], r2.at[k])
            if k == 0:
                keep[0] = keep[0] + precv[0].astype(F32)
                return
            rsend[k] = (keep[k] + precv[k].astype(F32)).astype(BF16)
            send(rsend.at[k], rrecv.at[k], r3.at[k], 2 * target(k) + c, tp)

        def last_outer():
            @pl.when(outer)
            def _():
                arrive(precv.at[3], r2.at[3])
                rsend[3] = (keep[3] + precv[3].astype(F32)).astype(BF16)
                out_of(3).start()

        def last_inner():
            @pl.when(inner)
            def _():
                arrive(precv.at[3], r2.at[3])
                arrive(rrecv.at[2], r3.at[2])
                total = keep[3] + precv[3].astype(F32) + rrecv[2].astype(F32)
                rsend[3] = total.astype(BF16)
                out_of(3).start()

            sends.append(out_of(3))

        def finish():
            with jax.named_scope("fin1"):
                arrive(rrecv.at[1], r3.at[1])
            keep[0] = keep[0] + rrecv[1].astype(F32)

            @pl.when(outer)
            def _():
                arrive(rrecv.at[2], r3.at[2])
                keep[0] = keep[0] + rrecv[2].astype(F32)

            with jax.named_scope("fin3"):
                arrive(rrecv.at[3], r3.at[3])
            return keep[0] + rrecv[3].astype(F32)

        return first, second, last_outer, last_inner, finish

    def part(k):
        zz = zp(k)
        arrive(narr.at[pl.ds(2 * zz, 2)] if k else narr.at[mate], tr.at[k])
        x = jnp.concatenate([narr[2 * zz + 1 - c], narr[2 * zz + c]], axis=0)
        x = (x.astype(F32) * mgain[me]).astype(BF16)
        return jnp.concatenate([dot(x, iw[...]), dot(x, gw[...])], axis=1)

    first, second, last_outer, last_inner, finish = reduction(
        psend, precv, pkeep, rsend, rrecv, r2, r3, part
    )
    with jax.named_scope("project"):
        first(0)
        lbig = [load(a, b) for a, b in ((ow_hbm, ow), (dg_hbm, dg), (du_hbm, du), (dd_hbm, dd))]
        lexp = [load(eg, wg), load(eu, wu)]
        for i in range(n):
            pltpu.make_async_copy(ed.at[:, pl.ds(i * q, q)], wd.at[i], lw.at[lw.shape[0] - 1]).start()
        for k in (2, 1):
            first(k)
            second(k)
        first(3)
        last_outer()
        last_inner()
        second(0)
    with jax.named_scope("prepare"):
        for cp in lsmall:
            cp.wait()
        per = LANES // rgb.shape[1]
        size = rgb.shape[1]
        place_r = lax.broadcasted_iota(jnp.int32, (size, LANES), 0)
        place_c = lax.broadcasted_iota(jnp.int32, (size, LANES), 1)
        for p in range(ch // LANES):
            for s in range(per):
                move = (place_c == place_r + s * size).astype(F32).astype(BF16)
                for gate, blocks in enumerate((rgb, igb)):
                    bd[p, s * size : (s + 1) * size, gate * LANES : (gate + 1) * LANES] = dot(
                        blocks[p * per + s], move
                    ).astype(BF16)
        taken = cvs.shape[0]
        total = cvs[0].astype(F32) * taps[0:1, :]
        for j in range(1, taken):
            total += cvs[j].astype(F32) * taps[j : j + 1, :]
        pre[...] = total
        for j in range(1, taken):
            cv_out[j - 1] = cvs[j]
        for e in range(n):
            at = slice(e * q, (e + 1) * q)
            line = jnp.broadcast_to(bw[...].astype(F32).reshape(1, width)[:, at], (experts, q))
            maps[:, at] = jnp.concatenate([rw[:, at].astype(F32), line], axis=0).astype(BF16)
        accg[...] = jnp.zeros_like(accg)
        accu[...] = jnp.zeros_like(accu)
        lacc[...] = jnp.zeros_like(lacc)
        square[...] = jnp.zeros_like(square)

    with jax.named_scope("recur"):
        both = finish() * inverse
        xb = both[:, :ch].astype(BF16)
        conv = (pre[...] + xb.astype(F32) * taps[taken : taken + 1, :]).astype(BF16)
        cv_out[taken - 1] = xb
        for p in range(ch // LANES):
            at = slice(p * LANES, (p + 1) * LANES)
            gates = jax.nn.sigmoid(dot(conv[:, at], bd[p]))
            log_decay = -decay_scale * gates[:, :LANES] * decay[:, at]
            ratio = jnp.tanh(-log_decay)
            scale = jnp.sqrt(2.0 * ratio / (1.0 + ratio))
            new = jnp.exp(log_decay) * state[:, at] + scale * gates[:, LANES:] * conv[:, at].astype(F32)
            st_out[:, at] = new
            gb = both[:, ch + p * LANES : ch + (p + 1) * LANES].astype(BF16).astype(F32)
            mr[:, at] = (new * jax.nn.gelu(gb)).astype(BF16)

    with jax.named_scope("mix"):
        send(mr, mall.at[me], br.at[0], mate, tp)
        for k in range(1, zs):
            send(mr, mall.at[me], ar.at[k], 2 * zp(k) + c, tp)
        mall[me] = mr[...]
        for cp in lbig:
            cp.wait()

        def pass_on(k):
            slot = 2 * zp(k) + c
            arrive(mall.at[slot], ar.at[k])
            send(mall.at[slot], mall.at[slot], br.at[k // 2], mate, tp)

        def mixed(i):
            arrive(mall.at[pl.ds(0, 2)], br.at[i])
            which = side if i == 0 else 1 - side
            x = mall[pl.ds(which * zs, zs)].reshape(half, ch)
            y = dot(x, ow[...]).astype(BF16)
            for t in range(m):
                osend[t, i] = y[:, t * g : (t + 1) * g]
            for k in (3, 1, 2):
                send(osend.at[tx(k), i], orecv.at[k, i], or_.at[i], me, tx(k))

        def summed(i):
            which = side if i == 0 else 1 - side
            raw = narr[pl.ds(which * zs, zs), :, lanes(tp, g)].reshape(half, g)
            total = raw.astype(F32) + osend[tp, i].astype(F32)
            arrive(orecv.at[pl.ds(1, m - 1), i], or_.at[i])
            for k in range(1, m):
                total += orecv[k, i].astype(F32)
            full[tp, me, which] = total.astype(BF16)

    direct = [(k, 1) for k in range(zs)]

    def sided(k, i):
        return side if (k < 2) == (i == 0) else 1 - side

    def spread(k, i):
        slot, s = 2 * zp(k) + c, sided(k, i)
        at = full.at[tp, slot, s]
        for d in (3, 1, 2) if (k, i) in direct else (1, 2):
            send(at, at, xr.at[d - 1, k, s], me, tx(d))
        send(at, at, mrv.at[k, s], mate, tp)

    def own(i):
        at = full.at[tp, me, sided(0, i)]
        s = sided(0, i)
        for k in (3, 2, 1):
            send(at, at, zr.at[k, s], 2 * zp(k) + c, tp)
        spread(0, i)

    def landed(k, i):
        s = sided(k, i)
        arrive(full.at[tp, 2 * zp(k) + c, s], zr.at[k, s])
        spread(k, i)

    def relay(k, i):
        slot, s = 2 * zp(k) + c, sided(k, i)
        early = tx(1) * (1 - s) + tx(2) * s
        late = tx(2) * (1 - s) + tx(1) * s
        at = full.at[early, slot, s]
        arrive(at, xr.at[s, k, s])
        if (k, i) not in direct:
            send(at, at, xr.at[2, k, s], me, late)
        send(at, at, mrv.at[k, s], mate, tp)
        at = full.at[late, slot, s]
        arrive(at, xr.at[1 - s, k, s])
        send(at, at, mrv.at[k, s], mate, tp)

    def relay_far(k, i):
        slot, s = 2 * zp(k) + c, sided(k, i)
        at = full.at[tx(3), slot, s]
        arrive(at, xr.at[2, k, s])
        send(at, at, mrv.at[k, s], mate, tp)

    def absorb(e, s, keep):
        parts = []
        for t in range(m):
            at = slice(t * g, (t + 1) * g)
            v = full[t, e, s].astype(F32)
            square[s] += v * v
            parts.append((v * gain[e, :, at]).astype(BF16))
        x = jnp.concatenate(parts, axis=1)
        if keep:
            nfm[s] = x
        accg[s] += dot(x, wg[e])
        accu[s] += dot(x, wu[e])
        lacc[s] += lax.dot_general(
            x, maps[:, lanes(e, q)], (((1,), (1,)), ((), ())), preferred_element_type=F32
        )

    def absorb_own(k, i):
        absorb(2 * zp(k) + c, sided(k, i), k == 0)

    def absorb_mate(k, i):
        e, s = 2 * zp(k) + 1 - c, sided(k, i)
        arrive(full.at[:, e, s], mrv.at[k, s])
        absorb(e, s, False)

    def dpart(k):
        s = zp(k) // 2
        x = []
        for core in range(2):
            at = lax.rem(zp(k), 2) * 2 + (1 - c if core == 0 else c)
            x.append(nfm[s, pl.ds(pl.multiple_of(at * rows, rows), rows), :])
        x = jnp.concatenate(x, axis=0)
        return jnp.concatenate([dot(x, dg[...]), dot(x, du[...])], axis=1)

    dfirst, dsecond, dlast_outer, dlast_inner, dfinish = reduction(
        dpsend, dprecv, dkeep, drsend, drrecv, r4, r5, dpart
    )

    with jax.named_scope("mix_near"):
        pass_on(1)
        mixed(0)
        for k in range(zs):
            for core in range(2):
                if k or core:
                    to = 2 * zp(k) + (c if core == 0 else 1 - c)
                    send(mask, masks.at[me], kr.at[0], to, tp)
        masks[me] = mask[...]
    with jax.named_scope("mix_sum"):
        pass_on(2)
        summed(0)
    with jax.named_scope("gather"):
        own(0)
        pass_on(3)
        mixed(1)
        landed(1, 0)
        relay(0, 0)
        landed(2, 0)
        landed(3, 0)
        relay(1, 0)
        summed(1)
        own(1)
        relay(2, 0)
        relay_far(0, 0)
        for cp in lexp:
            cp.wait()
        absorb_own(0, 0)
        dfirst(0)
        relay(3, 0)
        absorb_mate(0, 0)
        relay_far(1, 0)
        dfirst(1)
        relay(0, 1)
        relay_far(0, 1)
        landed(1, 1)
        absorb_own(0, 1)
        dfirst(2)
        landed(2, 1)
        landed(3, 1)
        dsecond(1)
        dfirst(3)
        relay_far(2, 0)
        dsecond(2)
        dlast_outer()
        absorb_own(1, 0)
        absorb_mate(1, 0)
        relay(1, 1)
        absorb_own(2, 0)
        relay_far(3, 0)
        relay(2, 1)
        absorb_mate(2, 0)
        relay_far(1, 1)
        absorb_own(3, 0)
        relay(3, 1)
        relay_far(2, 1)
        absorb_mate(3, 0)
        relay_far(3, 1)
        dlast_inner()
        absorb_own(1, 1)
        absorb_mate(0, 1)
        absorb_own(2, 1)
        absorb_mate(1, 1)
        absorb_own(3, 1)
        absorb_mate(2, 1)
        dsecond(0)
        absorb_mate(3, 1)

    scale = []
    with jax.named_scope("dense_act"):
        for s in (1 - side, side):
            scale.append(
                lax.rsqrt(jnp.sum(square[s], axis=-1, keepdims=True) / width + epsilon)
            )
            square[s, :, 0:1] = scale[-1]
        at = pl.ds(pl.multiple_of(lax.rem(me, zs) * rows, rows), rows)
        both = dfinish() * square[side, at, 0:1]
        first_half = both[:, :h]
        dact[...] = (first_half * jax.nn.sigmoid(first_half) * both[:, h:]).astype(BF16)
        for k in (3, 2, 1):
            send(dact, dall.at[me], cr.at[k], 2 * zp(k) + c, tp)
        send(dact, dall.at[me], er.at[0], mate, tp)
        dall[me] = dact[...]
        arrive(masks.at[pl.ds(0, n - 1)], kr.at[0])
    weight, branch = [], []

    def activate(ih):
        s = 1 - side if ih == 0 else side
        logits = lacc[s] * scale[ih]
        chosen = jnp.sum(masks[pl.ds(s * zs, zs)].astype(F32), axis=0).T
        named = logits * chosen
        other = jnp.sum(named, axis=-1, keepdims=True) - named
        share = (jax.nn.sigmoid(logits - other) * chosen).astype(BF16).astype(F32)
        at = lax.broadcasted_iota(jnp.int32, share.shape, 1)
        weight.append(jnp.sum(jnp.where(at == me, share, 0.0), axis=-1, keepdims=True))
        branch.append(jax.nn.sigmoid(logits[:, experts : experts + 1]))
        gate = accg[s] * scale[ih]
        act[ih] = (gate * jax.nn.sigmoid(gate) * (accu[s] * scale[ih])).astype(BF16)

    order = [lax.rem(z + 1 + i, m) for i in range(m)]

    def down(ih):
        for i in range(m):
            y = dot(act[ih], wd[2 * order[i] + 1 - c]) * weight[ih]
            ysend[i, ih] = y.astype(BF16)
            send(ysend.at[i, ih], yrecv.at[i, ih], yr.at[i, ih], mate, tp)
        for i in range(m):
            y = dot(act[ih], wd[2 * order[i] + c]) * weight[ih]
            for t in range(m):
                kq[i, ih, t] = y[:, t * g : (t + 1) * g]

    joined = [(i, 1) for i in range(m - 1)]

    def pass_part(k, i, ih, part, to):
        send(part, xrecv.at[k, i, ih], hr.at[1 if k == 3 and (i, ih) in joined else 0, i, ih], me, tx(to))

    def join(i, ih):
        lead = 1 + (i + ih) % 2
        arrive(xrecv.at[3, i, ih], hr.at[1, i, ih])
        total = kq[i, ih, tx(3 - lead)] + xrecv[3, i, ih].astype(F32)
        xjoin[i, ih] = total.astype(BF16)
        pass_part(3 - lead, i, ih, xjoin.at[i, ih], 3 - lead)

    def forward(i, ih, extra=None):
        arrive(yrecv.at[i, ih], yr.at[i, ih])
        for t in range(m):
            at = slice(t * g, (t + 1) * g)
            total = kq[i, ih, t] + yrecv[i, ih, :, at].astype(F32)
            if extra is not None:
                total += extra[:, at]
            kq[i, ih, t] = total
            xsend[i, ih, t] = total.astype(BF16)
        if (i, ih) not in joined:
            for k in (3, 1, 2):
                pass_part(k, i, ih, xsend.at[i, ih, tx(k)], k)
        else:
            lead = 1 + (i + ih) % 2
            pass_part(3, i, ih, xsend.at[i, ih, tx(3)], lead)
            pass_part(lead, i, ih, xsend.at[i, ih, tx(lead)], lead)

    def settle(i, ih):
        total = kq[i, ih, tp]
        many = 2 if (i, ih) in joined else m - 1
        arrive(xrecv.at[pl.ds(1, many), i, ih], hr.at[0, i, ih])
        for k in (1, 2) if (i, ih) in joined else range(1, m):
            total += xrecv[k, i, ih].astype(F32)
        pbuf[i, ih] = total.reshape(2, 2 * rows, g)
        for k in (2, 3) if ih == 0 else (1,):
            zsend[k, i] = pbuf[i, ih, lax.rem(zp(k), 2)].astype(BF16)

    def away(k, i):
        send(zsend.at[k, i], zrecv.at[k, i], gr.at[0], 2 * zp(k) + c, tp)

    pltpu.make_async_copy(wd, wd, lw.at[lw.shape[0] - 1]).wait()
    with jax.named_scope("down_far"):
        activate(0)
        down(0)
        activate(1)
    def dense_pass():
        for k in (1, 2, 3):
            slot = 2 * zp(k) + c
            arrive(dall.at[slot], cr.at[k])
            send(dall.at[slot], dall.at[slot], er.at[0], mate, tp)

    def dense_ready():
        arrive(dall.at[pl.ds(0, zs)], er.at[0])

    def dense_forward(ih):
        s = 1 - side if ih == 0 else side
        x = dall[pl.ds(s * zs, zs)].reshape(half, h)
        forward(m - 1, ih, dot(x, dd[...]) * branch[ih])

    def leave(i, ih):
        settle(i, ih)
        for k in (3, 2) if ih == 0 else (1,):
            away(k, i)

    with jax.named_scope("tail"):
        with jax.named_scope("f00"):
            forward(0, 0)
        with jax.named_scope("f10"):
            forward(1, 0)
        with jax.named_scope("f20"):
            forward(2, 0)
        with jax.named_scope("d1"):
            down(1)
        with jax.named_scope("f01"):
            forward(0, 1)
        with jax.named_scope("f11"):
            forward(1, 1)
        with jax.named_scope("f21"):
            forward(2, 1)
        with jax.named_scope("l00"):
            leave(0, 0)
        with jax.named_scope("dp"):
            dense_pass()
        with jax.named_scope("l10"):
            leave(1, 0)
        with jax.named_scope("l20"):
            leave(2, 0)
        with jax.named_scope("dr"):
            dense_ready()
        with jax.named_scope("df0"):
            dense_forward(0)
        with jax.named_scope("df1"):
            dense_forward(1)
        with jax.named_scope("j01"):
            join(0, 1)
        with jax.named_scope("j11"):
            join(1, 1)
        with jax.named_scope("j21"):
            join(2, 1)
        with jax.named_scope("l30"):
            leave(3, 0)
        with jax.named_scope("l01"):
            leave(0, 1)
        with jax.named_scope("l11"):
            leave(1, 1)
        with jax.named_scope("l21"):
            leave(2, 1)
        with jax.named_scope("l31"):
            leave(3, 1)

    with jax.named_scope("last_sum"):
        arrive(zrecv.at[pl.ds(1, zs - 1)], gr.at[0])
        spot = lax.rem(z, 2)
        for j in range(m):
            total = pbuf[lax.rem(j - z - 1 + 2 * m, m), 1, spot]
            for k in range(1, zs):
                total += zrecv[k, lax.rem(j - zp(k) - 1 + 2 * m, m)].astype(F32)
            resid = full[tp, 2 * j + c, side, pl.ds(pl.multiple_of(2 * rows * spot, rows), 2 * rows), :]
            total = (total + resid.astype(F32)).astype(BF16)
            for core in range(2):
                fblk[core, j] = total[core * rows : (core + 1) * rows]
    with jax.named_scope("last_gather"):
        for k in (3, 1, 2, 0):
            for dc in range(2):
                if k or dc:
                    core = c if dc == 0 else 1 - c
                    send(
                        fblk.at[core], fin.at[c * m + tp], fr.at[0], 2 * z + core, tx(k)
                    )
        fin[c * m + tp] = fblk[c]
        arrive(fin.at[pl.ds(0, 2 * m - 1)], fr.at[0])
        for core in range(2):
            for t in range(m):
                for j in range(m):
                    base = (2 * j + core) * q + t * g
                    out[:, base : base + g] = fin[core * m + t, j]
    with jax.named_scope("drain"):
        for cp in sends:
            cp.wait_send()


def deliver_kernel(a, b, c, to_a, to_b, to_c, sems):
    copies = [
        pltpu.make_async_copy(src, dst, sems.at[i])
        for i, (src, dst) in enumerate(((a, to_a), (b, to_b), (c, to_c)))
    ]
    for cp in copies:
        cp.start()
    for cp in copies:
        cp.wait()


def in_kernel(
    n, m, tokens, recur_state, conv_state, mix_gain, in_weight, gate_weight, conv_taps,
    recur_gate_blocks, input_gate_blocks, decay_rate, out_weight, ffn_gain, router_weight, routes,
    expert_gate, expert_up, expert_down, dense_gate, dense_up, dense_down, branch_gate,
):
    rows, width = tokens.shape
    q, ch = in_weight.shape
    experts = router_weight.shape[1]
    h, f = dense_gate.shape[1], expert_down.shape[1]
    g, zs, b = q // m, n // 2, n * rows
    half = b // 2
    lines = 2 * experts
    past = (conv_state.shape[1], rows, ch)
    hbm = pl.BlockSpec(memory_space=pl.ANY)
    vm = pl.BlockSpec(memory_space=pltpu.VMEM)
    v = pltpu.VMEM

    def flags(*shapes):
        return [pltpu.SemaphoreType.DMA(s) for s in shapes]

    operands = (
        tokens, mix_gain.reshape(n, 1, q), ffn_gain.reshape(n, 1, q), routes.T, recur_state,
        conv_state.transpose(1, 0, 2), conv_taps, recur_gate_blocks, input_gate_blocks,
        decay_rate.reshape(1, ch), router_weight.T, branch_gate,
        in_weight, gate_weight, out_weight, dense_gate, dense_up, dense_down,
        expert_gate.reshape(n, q, f), expert_up.reshape(n, q, f), expert_down[0],
    )
    results = (
        jax.ShapeDtypeStruct((rows, width), BF16),
        jax.ShapeDtypeStruct((rows, ch), F32),
        jax.ShapeDtypeStruct(past, BF16),
    )
    layer_out, new_state, window = pl.pallas_call(
        functools.partial(layer_kernel, n, m, experts),
        out_shape=tuple(pltpu.VMEM(r.shape, r.dtype) for r in results),
        in_specs=[hbm] * len(operands),
        out_specs=(vm, vm, vm),
        scratch_shapes=[
            v((rows, width), BF16), v((n, 1, q), F32), v((n, 1, q), F32), v(routes.shape[::-1], jnp.int32),
            v((rows, ch), F32), v(past, BF16), v(conv_taps.shape, F32),
            v(recur_gate_blocks.shape, BF16), v(input_gate_blocks.shape, BF16), v((1, ch), F32),
            v((experts, width), BF16), v((width,), BF16), v((lines, width), BF16), v((q, ch), BF16), v((q, ch), BF16), v((ch, q), BF16),
            v((q, h), BF16), v((q, h), BF16), v((h, q), BF16),
            v((n, q, f), BF16), v((n, q, f), BF16), v((n, f, q), BF16),
            v((n, rows, q), BF16), v((zs, rows, 2 * ch), BF16), v((zs, rows, 2 * ch), BF16),
            v((zs, rows, 2 * ch), F32), v((zs, rows, 2 * ch), BF16), v((zs, rows, 2 * ch), BF16),
            v((rows, ch), F32), v((ch // LANES, LANES, 2 * LANES), BF16),
            v((lines, half), BF16), v((n, lines, half), BF16),
            v((rows, ch), BF16), v((n, rows, ch), BF16),
            v((m, 2, half, g), BF16), v((m, 2, half, g), BF16),
            v((m, n, 2, half, g), BF16), v((2, half, q), BF16),
            v((2, half, g), F32), v((2, half, lines), F32),
            v((2, half, f), F32), v((2, half, f), F32), v((2, half, f), BF16),
            v((zs, rows, 2 * h), BF16), v((zs, rows, 2 * h), BF16), v((zs, rows, 2 * h), F32),
            v((zs, rows, 2 * h), BF16), v((zs, rows, 2 * h), BF16),
            v((rows, h), BF16), v((n, rows, h), BF16),
            v((m, 2, half, q), BF16), v((m, 2, half, q), BF16), v((m, 2, m, half, g), F32),
            v((m, 2, m, half, g), BF16), v((m, m, 2, half, g), BF16), v((m - 1, 2, half, g), BF16),
            v((m, 2, 2, 2 * rows, g), F32),
            v((zs, m, 2 * rows, g), BF16), v((zs, m, 2 * rows, g), BF16),
            v((2, m, rows, g), BF16), v((2 * m, m, rows, g), BF16),
        ]
        + flags(
            (21,), (1,), (zs,), (1,), (zs,), (zs,), (zs,), (2,), (2,), (zs, 2), (m - 1, zs, 2), (zs, 2),
            (zs,), (zs,), (zs,), (1,), (m, 2), (2, m, 2), (1,), (1,),
        ),
        compiler_params=pltpu.CompilerParams(
            collective_id=0, has_side_effects=True, vmem_limit_bytes=58 * 1024 * 1024
        ),
        name="layer",
    )(*operands)
    held = [pltpu.with_memory_space_constraint(a, pltpu.VMEM) for a in (layer_out, new_state, window)]
    layer_out, new_state, window = pl.pallas_call(
        deliver_kernel,
        out_shape=results,
        in_specs=[vm] * 3,
        out_specs=(hbm,) * 3,
        scratch_shapes=[pltpu.SemaphoreType.DMA((3,))],
        name="deliver",
    )(*held)
    return (layer_out, new_state, window.transpose(1, 0, 2))


def solution(mesh):
    in_specs = (
        P("ep", None),
        P("ep", "tp"),
        P("ep", None, "tp"),
        P(),
        P("ep", "tp"),
        P("ep", "tp"),
        P(None, "tp"),
        P("tp", None, None),
        P("tp", None, None),
        P("tp"),
        P("tp", "ep"),
        P(),
        P(),
        P("ep", None),
        P("ep", None, "tp"),
        P("ep", None, "tp"),
        P("ep", "tp", None),
        P("ep", "tp"),
        P("ep", "tp"),
        P("tp", "ep"),
        P(),
    )
    out_specs = (P("ep", None), P("ep", "tp"), P("ep", None, "tp"))
    n, m = mesh.shape["ep"], mesh.shape["tp"]

    def body(*args):
        tokens, blocks, router, dense = args[0], args[7], args[12], args[17]
        q = tokens.shape[1] // n
        fits = m == 4 and n == 2 * m and n == router.shape[1] and q % (m * LANES) == 0
        fits = fits and tokens.shape[0] % 16 == 0 and dense.shape[1] % LANES == 0
        fits = fits and LANES % blocks.shape[1] == 0
        if fits:
            return in_kernel(n, m, *args)
        return on_device(*args)

    return jax.shard_map(
        body, mesh=mesh, in_specs=in_specs, out_specs=out_specs, check_vma=False
    )
```

```python
import functools

import jax
import jax.numpy as jnp
from jax import lax
from jax.experimental import pallas as pl
from jax.experimental.pallas import tpu as pltpu
from jax.sharding import PartitionSpec as P

TOP_K = 2
LANES = 128
F32 = jnp.float32
BF16 = jnp.bfloat16


epsilon = 1e-06
decay_scale = 8.0


def rms_scale(rows, gain):
    values = rows.astype(jnp.float32)
    inverse = lax.rsqrt(jnp.mean(values * values, axis=-1, keepdims=True) + epsilon)
    return (values * inverse * gain).astype(jnp.bfloat16)


def on_device(
    tokens,
    recur_state,
    conv_state,
    mix_gain,
    in_weight,
    gate_weight,
    conv_taps,
    recur_gate_blocks,
    input_gate_blocks,
    decay_rate,
    out_weight,
    ffn_gain,
    router_weight,
    routes,
    expert_gate,
    expert_up,
    expert_down,
    dense_gate,
    dense_up,
    dense_down,
    branch_gate,
):
    batch_rows, width = tokens.shape
    channels = in_weight.shape[1]
    normed = rms_scale(tokens, mix_gain)
    arrived = lax.all_to_all(normed, "ep", split_axis=1, concat_axis=0, tiled=True)
    joined = jnp.concatenate([in_weight, gate_weight], axis=1)
    summed = lax.psum_scatter(
        jnp.dot(arrived, joined, preferred_element_type=jnp.float32).astype(jnp.bfloat16),
        "ep",
        scatter_dimension=0,
        tiled=True,
    ).astype(jnp.float32)
    x_sum, gate_sum = (summed[:, :channels], summed[:, channels:])
    x_branch = x_sum.astype(jnp.bfloat16)
    gate_branch = gate_sum.astype(jnp.bfloat16)
    window = jnp.concatenate([conv_state, x_branch[:, None, :]], axis=1)
    conv_out = jnp.sum(window.astype(jnp.float32) * conv_taps[None], axis=1).astype(jnp.bfloat16)
    new_conv_state = window[:, 1:, :]
    blocks = conv_out.reshape(batch_rows, recur_gate_blocks.shape[0], recur_gate_blocks.shape[1])
    recur_gate = jax.nn.sigmoid(
        jnp.einsum(
            "bhi,hij->bhj", blocks, recur_gate_blocks, preferred_element_type=jnp.float32
        ).reshape(batch_rows, channels)
    )
    input_gate = jax.nn.sigmoid(
        jnp.einsum(
            "bhi,hij->bhj", blocks, input_gate_blocks, preferred_element_type=jnp.float32
        ).reshape(batch_rows, channels)
    )
    log_decay = -decay_scale * recur_gate * decay_rate
    new_state = jnp.exp(log_decay) * recur_state + jnp.sqrt(
        -jnp.expm1(2.0 * log_decay)
    ) * input_gate * conv_out.astype(jnp.float32)
    mixer_rows = (new_state * jax.nn.gelu(gate_branch.astype(jnp.float32))).astype(jnp.bfloat16)
    mixer_part = jnp.dot(
        mixer_rows,
        lax.all_gather(out_weight, "ep", axis=1, tiled=True),
        preferred_element_type=jnp.float32,
    )
    resid = (
        tokens.astype(jnp.float32)
        + lax.psum(mixer_part.astype(jnp.bfloat16), "tp").astype(jnp.float32)
    ).astype(jnp.bfloat16)
    normed_ffn = rms_scale(resid, ffn_gain)
    router_logits = jnp.dot(normed_ffn, router_weight, preferred_element_type=jnp.float32)
    experts = router_logits.shape[1]
    expert_ids = lax.broadcasted_iota(jnp.int32, (batch_rows, TOP_K, experts), 2)
    picked = jnp.sum(
        jnp.where(routes[:, :, None] == expert_ids, router_logits[:, None, :], 0.0), axis=2
    )
    route_weight = jax.nn.sigmoid(picked - picked[:, ::-1]).astype(jnp.bfloat16)
    capacity = 2 * batch_rows * TOP_K // experts
    flat_ids = routes.reshape(batch_rows * TOP_K)
    onehot = (
        flat_ids[:, None] == lax.broadcasted_iota(jnp.int32, (batch_rows * TOP_K, experts), 1)
    ).astype(jnp.int32)
    rank = jnp.sum((jnp.cumsum(onehot, axis=0) - onehot) * onehot, axis=1)
    slot_of = (flat_ids * capacity + rank).reshape(batch_rows, TOP_K)
    slot_rows = lax.broadcasted_iota(jnp.int32, (experts * capacity, batch_rows), 0)
    slot_cols = lax.broadcasted_iota(jnp.int32, (batch_rows, experts * capacity), 1)
    dispatch = jnp.zeros((experts * capacity, batch_rows), jnp.bfloat16)
    combine = jnp.zeros((batch_rows, experts * capacity), jnp.bfloat16)
    for pick in range(TOP_K):
        dispatch = dispatch + (slot_rows == slot_of[None, :, pick]).astype(jnp.bfloat16)
        combine = combine + jnp.where(
            slot_cols == slot_of[:, pick : pick + 1],
            route_weight[:, pick : pick + 1],
            jnp.zeros((), jnp.bfloat16),
        )
    outgoing = (
        jnp.dot(dispatch, normed_ffn, preferred_element_type=jnp.float32)
        .astype(jnp.bfloat16)
        .reshape(experts, capacity, width)
    )
    gate_local = expert_gate[0]
    up_local = expert_up[0]
    down_local = expert_down[0]
    arrived_rows = lax.all_to_all(outgoing, "ep", split_axis=0, concat_axis=0, tiled=True)
    sources, items, features = arrived_rows.shape
    rows = arrived_rows.reshape(sources * items, features)
    first = jnp.dot(rows, gate_local, preferred_element_type=jnp.float32)
    second = jnp.dot(rows, up_local, preferred_element_type=jnp.float32)
    act = (jax.nn.silu(first) * second).astype(jnp.bfloat16)
    partial_value = jnp.dot(act, down_local, preferred_element_type=jnp.float32)
    total = lax.psum(partial_value.astype(jnp.bfloat16), "tp")
    returned = lax.all_to_all(
        total.reshape(sources, items, total.shape[1]), "ep", split_axis=0, concat_axis=0, tiled=True
    )
    moe = jnp.dot(
        combine,
        returned.reshape(experts * capacity, returned.shape[2]),
        preferred_element_type=jnp.float32,
    )
    dense_arrived = lax.all_to_all(normed_ffn, "ep", split_axis=1, concat_axis=0, tiled=True)
    dense_joined = jnp.concatenate([dense_gate, dense_up], axis=1)
    dense_summed = lax.psum_scatter(
        jnp.dot(dense_arrived, dense_joined, preferred_element_type=jnp.float32).astype(
            jnp.bfloat16
        ),
        "ep",
        scatter_dimension=0,
        tiled=True,
    ).astype(jnp.float32)
    dense_first = dense_summed[:, : dense_gate.shape[1]]
    dense_second = dense_summed[:, dense_gate.shape[1] :]
    dense_act = (jax.nn.silu(dense_first) * dense_second).astype(jnp.bfloat16)
    dense_part = jnp.dot(
        dense_act,
        lax.all_gather(dense_down, "ep", axis=1, tiled=True),
        preferred_element_type=jnp.float32,
    )
    branch_weight = jax.nn.sigmoid(
        jnp.dot(normed_ffn, branch_gate, preferred_element_type=jnp.float32)
    )
    dense_sum = lax.psum(dense_part.astype(jnp.bfloat16), "tp").astype(jnp.float32)
    layer_out = (resid.astype(jnp.float32) + moe + branch_weight[:, None] * dense_sum).astype(
        jnp.bfloat16
    )
    return (layer_out, new_state, new_conv_state)


def rcopy(src, dst, send, recv, ep, tp):
    return pltpu.make_async_remote_copy(
        src_ref=src,
        dst_ref=dst,
        send_sem=send,
        recv_sem=recv,
        device_id={"ep": ep, "tp": tp},
        device_id_type=pl.DeviceIdType.MESH,
    )


def dot(left, right):
    return jnp.dot(left, right, preferred_element_type=F32)


def layer_kernel(
    n, m, experts, tok_hbm, mg_hbm, fg_hbm, rt_hbm, st_hbm, cv_hbm, tap_hbm, rg_hbm, ig_hbm, dr_hbm,
    rw_hbm, bw_hbm, iw_hbm, gw_hbm, ow_hbm, dg_hbm, du_hbm, dd_hbm, eg, eu, ed, out, st_out, cv_out,
    toks, mgain, gain, rts, state, cvs, taps, rgb, igb, decay, rw, bw, maps, iw, gw, ow, dg, du, dd, wg, wu, wd,
    narr, psend, precv, pkeep, rsend, rrecv, pre, bd, mask, masks, mr, mall, osend, orecv, full, nfm,
    square, lacc, accg, accu, act, dpsend, dprecv, dkeep, drsend, drrecv, dact, dall,
    ysend, yrecv, kq, xsend, xrecv, xjoin, pbuf, zsend, zrecv, fblk, fin,
    lw, sent, tr, kr, r2, r3, ar, br, or_, zr, xr, mrv, r4, r5, cr, er, yr, hr, gr, fr,
):
    me, tp = lax.axis_index("ep"), lax.axis_index("tp")
    zs = n // 2
    z, c = me // 2, me % 2
    mate = 2 * z + 1 - c
    side = z // 2
    inner = lax.rem(z, 3) != 0
    outer = lax.rem(z, 3) == 0
    rows, width = out.shape
    q, ch = iw.shape
    g = q // m
    half = n * rows // 2
    h = dg.shape[1]

    def zp(k):
        return (z, z + 1 - 2 * lax.rem(z, 2), lax.rem(z + 2, zs), zs - 1 - z)[k]

    def tx(k):
        return (tp, tp + 1 - 2 * lax.rem(tp, 2), lax.rem(tp + 2, m), m - 1 - tp)[k]

    def lanes(e, size):
        return pl.ds(pl.multiple_of(e * size, LANES), size)

    count = [0]

    def load(src, dst):
        cp = pltpu.make_async_copy(src, dst, lw.at[count[0]])
        count[0] += 1
        cp.start()
        return cp

    sends = []

    def send(src, dst, recv, ep, t):
        cp = rcopy(src, dst, sent.at[0], recv, ep, t)
        cp.start()
        sends.append(cp)

    def arrive(buf, sem):
        rcopy(buf, buf, sem, sem, mate, tp).wait_recv()

    with jax.named_scope('enter'):
        ltok = load(tok_hbm, toks)
    lmain = [load(mg_hbm, mgain), load(iw_hbm, iw), load(gw_hbm, gw)]
    lrt = load(rt_hbm, rts)

    barrier = pltpu.get_barrier_semaphore()
    peers = [(lax.rem(me + d, n), tp) for d in range(1, n)]
    for k in range(1, m):
        peers += [(me, tx(k)), (mate, tx(k))]
    for ep, t in peers:
        pl.semaphore_signal(
            barrier, inc=1, device_id={"ep": ep, "tp": t}, device_id_type=pl.DeviceIdType.MESH
        )
    with jax.named_scope('tokwait'):
        ltok.wait()
    with jax.named_scope('greet'):
        pl.semaphore_wait(barrier, len(peers))

    send(toks.at[:, lanes(mate, q)], narr.at[me], tr.at[0], mate, tp)
    for k in (2, 1, 3):
        for core in range(2):
            to = 2 * zp(k) + core
            send(toks.at[:, lanes(to, q)], narr.at[me], tr.at[k], to, tp)
    narr[me] = toks[:, lanes(me, q)]
    lrt.wait()
    pair = jnp.concatenate([rts[...]] * zs, axis=1)
    line = lax.broadcasted_iota(jnp.int32, mask.shape, 0)
    lane = lax.broadcasted_iota(jnp.int32, mask.shape, 1) - lax.rem(me, zs) * rows
    taken = ((pair[0:1] == line) | (pair[1:2] == line)) & (lane >= 0) & (lane < rows)
    mask[...] = taken.astype(F32).astype(BF16)
    values = toks[...].astype(F32)
    inverse = lax.rsqrt(jnp.mean(values * values, axis=-1, keepdims=True) + epsilon)
    lsmall = [
        load(a, b)
        for a, b in (
            (cv_hbm, cvs), (tap_hbm, taps), (rg_hbm, rgb), (ig_hbm, igb), (st_hbm, state),
            (dr_hbm, decay), (fg_hbm, gain), (rw_hbm, rw), (bw_hbm, bw),
        )
    ]
    with jax.named_scope('lmain'):
        for cp in lmain:
            cp.wait()

    def reduction(psend, precv, keep, rsend, rrecv, r2, r3, part):
        def first(k):
            y = part(k)
            psend[k] = y[:rows].astype(BF16)
            send(psend.at[k], precv.at[k], r2.at[k], mate, tp)
            keep[k] = y[rows:]

        def target(k):
            return jnp.where(inner, zp(2), zp(1)) if k == 2 else zp(k)

        def out_of(k):
            return rcopy(
                rsend.at[k], rrecv.at[k], sent.at[0], r3.at[k], 2 * target(k) + c, tp
            )

        def second(k):
            arrive(precv.at[k], r2.at[k])
            if k == 0:
                keep[0] = keep[0] + precv[0].astype(F32)
                return
            rsend[k] = (keep[k] + precv[k].astype(F32)).astype(BF16)
            send(rsend.at[k], rrecv.at[k], r3.at[k], 2 * target(k) + c, tp)

        def last_outer():
            @pl.when(outer)
            def _():
                arrive(precv.at[3], r2.at[3])
                rsend[3] = (keep[3] + precv[3].astype(F32)).astype(BF16)
                out_of(3).start()

        def last_inner():
            @pl.when(inner)
            def _():
                arrive(precv.at[3], r2.at[3])
                arrive(rrecv.at[2], r3.at[2])
                total = keep[3] + precv[3].astype(F32) + rrecv[2].astype(F32)
                rsend[3] = total.astype(BF16)
                out_of(3).start()

            sends.append(out_of(3))

        def finish():
            with jax.named_scope("fin1"):
                arrive(rrecv.at[1], r3.at[1])
            keep[0] = keep[0] + rrecv[1].astype(F32)

            @pl.when(outer)
            def _():
                arrive(rrecv.at[2], r3.at[2])
                keep[0] = keep[0] + rrecv[2].astype(F32)

            with jax.named_scope("fin3"):
                arrive(rrecv.at[3], r3.at[3])
            return keep[0] + rrecv[3].astype(F32)

        return first, second, last_outer, last_inner, finish

    def part(k):
        zz = zp(k)
        arrive(narr.at[pl.ds(2 * zz, 2)] if k else narr.at[mate], tr.at[k])
        x = jnp.concatenate([narr[2 * zz + 1 - c], narr[2 * zz + c]], axis=0)
        x = (x.astype(F32) * mgain[me]).astype(BF16)
        return jnp.concatenate([dot(x, iw[...]), dot(x, gw[...])], axis=1)

    first, second, last_outer, last_inner, finish = reduction(
        psend, precv, pkeep, rsend, rrecv, r2, r3, part
    )
    with jax.named_scope("project"):
        first(0)
        lbig = [load(a, b) for a, b in ((ow_hbm, ow), (dg_hbm, dg), (du_hbm, du), (dd_hbm, dd))]
        lexp = [load(eg, wg), load(eu, wu)]
        for i in range(n):
            pltpu.make_async_copy(ed.at[:, pl.ds(i * q, q)], wd.at[i], lw.at[lw.shape[0] - 1]).start()
        for k in (2, 1):
            first(k)
            second(k)
        first(3)
        last_outer()
        last_inner()
        second(0)
    with jax.named_scope("prepare"):
        for cp in lsmall:
            cp.wait()
        per = LANES // rgb.shape[1]
        size = rgb.shape[1]
        place_r = lax.broadcasted_iota(jnp.int32, (size, LANES), 0)
        place_c = lax.broadcasted_iota(jnp.int32, (size, LANES), 1)
        for p in range(ch // LANES):
            for s in range(per):
                move = (place_c == place_r + s * size).astype(F32).astype(BF16)
                for gate, blocks in enumerate((rgb, igb)):
                    bd[p, s * size : (s + 1) * size, gate * LANES : (gate + 1) * LANES] = dot(
                        blocks[p * per + s], move
                    ).astype(BF16)
        taken = cvs.shape[0]
        total = cvs[0].astype(F32) * taps[0:1, :]
        for j in range(1, taken):
            total += cvs[j].astype(F32) * taps[j : j + 1, :]
        pre[...] = total
        for j in range(1, taken):
            cv_out[j - 1] = cvs[j]
        for e in range(n):
            at = slice(e * q, (e + 1) * q)
            line = jnp.broadcast_to(bw[...].astype(F32).reshape(1, width)[:, at], (experts, q))
            maps[:, at] = jnp.concatenate([rw[:, at].astype(F32), line], axis=0).astype(BF16)
        accg[...] = jnp.zeros_like(accg)
        accu[...] = jnp.zeros_like(accu)
        lacc[...] = jnp.zeros_like(lacc)
        square[...] = jnp.zeros_like(square)

    with jax.named_scope("recur"):
        both = finish() * inverse
        xb = both[:, :ch].astype(BF16)
        conv = (pre[...] + xb.astype(F32) * taps[taken : taken + 1, :]).astype(BF16)
        cv_out[taken - 1] = xb
        for p in range(ch // LANES):
            at = slice(p * LANES, (p + 1) * LANES)
            gates = jax.nn.sigmoid(dot(conv[:, at], bd[p]))
            log_decay = -decay_scale * gates[:, :LANES] * decay[:, at]
            ratio = jnp.tanh(-log_decay)
            scale = jnp.sqrt(2.0 * ratio / (1.0 + ratio))
            new = jnp.exp(log_decay) * state[:, at] + scale * gates[:, LANES:] * conv[:, at].astype(F32)
            st_out[:, at] = new
            gb = both[:, ch + p * LANES : ch + (p + 1) * LANES].astype(BF16).astype(F32)
            mr[:, at] = (new * jax.nn.gelu(gb)).astype(BF16)

    with jax.named_scope("mix"):
        send(mr, mall.at[me], br.at[0], mate, tp)
        for k in (1, 3, 2):
            send(mr, mall.at[me], ar.at[k], 2 * zp(k) + c, tp)
        mall[me] = mr[...]
        for cp in lbig:
            cp.wait()

        def pass_on(k):
            slot = 2 * zp(k) + c
            arrive(mall.at[slot], ar.at[k])
            send(mall.at[slot], mall.at[slot], br.at[k // 2], mate, tp)

        def mixed(i):
            arrive(mall.at[pl.ds(0, 2)], br.at[i])
            which = side if i == 0 else 1 - side
            x = mall[pl.ds(which * zs, zs)].reshape(half, ch)
            y = dot(x, ow[...]).astype(BF16)
            for t in range(m):
                osend[t, i] = y[:, t * g : (t + 1) * g]
            for k in (3, 1, 2):
                send(osend.at[tx(k), i], orecv.at[k, i], or_.at[i], me, tx(k))

        def summed(i):
            which = side if i == 0 else 1 - side
            raw = narr[pl.ds(which * zs, zs), :, lanes(tp, g)].reshape(half, g)
            total = raw.astype(F32) + osend[tp, i].astype(F32)
            arrive(orecv.at[pl.ds(1, m - 1), i], or_.at[i])
            for k in range(1, m):
                total += orecv[k, i].astype(F32)
            full[tp, me, which] = total.astype(BF16)

    direct = [(k, 1) for k in range(zs)] + [(0, 0)]

    def sided(k, i):
        return side if (k < 2) == (i == 0) else 1 - side

    def spread(k, i):
        slot, s = 2 * zp(k) + c, sided(k, i)
        at = full.at[tp, slot, s]
        for d in (3, 1, 2) if (k, i) in direct else (1, 2):
            send(at, at, xr.at[d - 1, k, s], me, tx(d))
        send(at, at, mrv.at[k, s], mate, tp)

    def own(i):
        at = full.at[tp, me, sided(0, i)]
        s = sided(0, i)
        for k in (3, 2, 1):
            send(at, at, zr.at[k, s], 2 * zp(k) + c, tp)
        spread(0, i)

    def landed(k, i):
        s = sided(k, i)
        arrive(full.at[tp, 2 * zp(k) + c, s], zr.at[k, s])
        spread(k, i)

    def relay(k, i):
        slot, s = 2 * zp(k) + c, sided(k, i)
        early = tx(1) * (1 - s) + tx(2) * s
        late = tx(2) * (1 - s) + tx(1) * s
        at = full.at[early, slot, s]
        arrive(at, xr.at[s, k, s])
        if (k, i) not in direct:
            send(at, at, xr.at[2, k, s], me, late)
        send(at, at, mrv.at[k, s], mate, tp)
        at = full.at[late, slot, s]
        arrive(at, xr.at[1 - s, k, s])
        send(at, at, mrv.at[k, s], mate, tp)

    def relay_far(k, i):
        slot, s = 2 * zp(k) + c, sided(k, i)
        at = full.at[tx(3), slot, s]
        arrive(at, xr.at[2, k, s])
        send(at, at, mrv.at[k, s], mate, tp)

    def absorb(e, s, keep):
        parts = []
        for t in range(m):
            at = slice(t * g, (t + 1) * g)
            v = full[t, e, s].astype(F32)
            square[s] += v * v
            parts.append((v * gain[e, :, at]).astype(BF16))
        x = jnp.concatenate(parts, axis=1)
        if keep:
            nfm[s] = x
        accg[s] += dot(x, wg[e])
        accu[s] += dot(x, wu[e])
        lacc[s] += lax.dot_general(
            x, maps[:, lanes(e, q)], (((1,), (1,)), ((), ())), preferred_element_type=F32
        )

    def absorb_own(k, i):
        absorb(2 * zp(k) + c, sided(k, i), k == 0)

    def absorb_mate(k, i):
        e, s = 2 * zp(k) + 1 - c, sided(k, i)
        arrive(full.at[:, e, s], mrv.at[k, s])
        absorb(e, s, False)

    def dpart(k):
        s = zp(k) // 2
        x = []
        for core in range(2):
            at = lax.rem(zp(k), 2) * 2 + (1 - c if core == 0 else c)
            x.append(nfm[s, pl.ds(pl.multiple_of(at * rows, rows), rows), :])
        x = jnp.concatenate(x, axis=0)
        return jnp.concatenate([dot(x, dg[...]), dot(x, du[...])], axis=1)

    dfirst, dsecond, dlast_outer, dlast_inner, dfinish = reduction(
        dpsend, dprecv, dkeep, drsend, drrecv, r4, r5, dpart
    )

    with jax.named_scope("mix_near"):
        pass_on(1)
        mixed(0)
        for k in range(zs):
            for core in range(2):
                if k or core:
                    to = 2 * zp(k) + (c if core == 0 else 1 - c)
                    send(mask, masks.at[me], kr.at[0], to, tp)
        masks[me] = mask[...]
    with jax.named_scope("mix_sum"):
        pass_on(2)
        summed(0)
    with jax.named_scope("gather"):
        own(0)
        pass_on(3)
        mixed(1)
        landed(1, 0)
        relay(0, 0)
        landed(2, 0)
        landed(3, 0)
        relay(1, 0)
        summed(1)
        own(1)
        relay(2, 0)
        relay_far(0, 0)
        for cp in lexp:
            cp.wait()
        absorb_own(0, 0)
        dfirst(0)
        relay(3, 0)
        absorb_mate(0, 0)
        relay_far(1, 0)
        dfirst(1)
        relay(0, 1)
        relay_far(0, 1)
        landed(1, 1)
        absorb_own(0, 1)
        dfirst(2)
        landed(2, 1)
        landed(3, 1)
        dsecond(1)
        dfirst(3)
        relay_far(2, 0)
        dsecond(2)
        dlast_outer()
        absorb_own(1, 0)
        absorb_mate(1, 0)
        relay(1, 1)
        absorb_own(2, 0)
        relay_far(3, 0)
        relay(2, 1)
        absorb_mate(2, 0)
        relay_far(1, 1)
        absorb_own(3, 0)
        relay(3, 1)
        relay_far(2, 1)
        absorb_mate(3, 0)
        relay_far(3, 1)
        dlast_inner()
        absorb_own(1, 1)
        absorb_mate(0, 1)
        absorb_own(2, 1)
        absorb_mate(1, 1)
        absorb_own(3, 1)
        absorb_mate(2, 1)
        dsecond(0)
        absorb_mate(3, 1)

    scale = []
    with jax.named_scope("dense_act"):
        for s in (1 - side, side):
            scale.append(
                lax.rsqrt(jnp.sum(square[s], axis=-1, keepdims=True) / width + epsilon)
            )
            square[s, :, 0:1] = scale[-1]
        at = pl.ds(pl.multiple_of(lax.rem(me, zs) * rows, rows), rows)
        both = dfinish() * square[side, at, 0:1]
        first_half = both[:, :h]
        dact[...] = (first_half * jax.nn.sigmoid(first_half) * both[:, h:]).astype(BF16)
        for k in (3, 2, 1):
            send(dact, dall.at[me], cr.at[k], 2 * zp(k) + c, tp)
        send(dact, dall.at[me], er.at[0], mate, tp)
        dall[me] = dact[...]
        arrive(masks.at[pl.ds(0, n - 1)], kr.at[0])
    weight, branch = [], []

    def activate(ih):
        s = 1 - side if ih == 0 else side
        logits = lacc[s] * scale[ih]
        chosen = jnp.sum(masks[pl.ds(s * zs, zs)].astype(F32), axis=0).T
        named = logits * chosen
        other = jnp.sum(named, axis=-1, keepdims=True) - named
        share = (jax.nn.sigmoid(logits - other) * chosen).astype(BF16).astype(F32)
        at = lax.broadcasted_iota(jnp.int32, share.shape, 1)
        weight.append(jnp.sum(jnp.where(at == me, share, 0.0), axis=-1, keepdims=True))
        branch.append(jax.nn.sigmoid(logits[:, experts : experts + 1]))
        gate = accg[s] * scale[ih]
        act[ih] = (gate * jax.nn.sigmoid(gate) * (accu[s] * scale[ih])).astype(BF16)

    order = [lax.rem(z + 1 + i, m) for i in range(m)]

    def down(ih):
        for i in range(m):
            y = dot(act[ih], wd[2 * order[i] + 1 - c]) * weight[ih]
            ysend[i, ih] = y.astype(BF16)
            send(ysend.at[i, ih], yrecv.at[i, ih], yr.at[i, ih], mate, tp)
        for i in range(m):
            y = dot(act[ih], wd[2 * order[i] + c]) * weight[ih]
            for t in range(m):
                kq[i, ih, t] = y[:, t * g : (t + 1) * g]

    joined = [(i, 1) for i in range(m - 1)]

    def pass_part(k, i, ih, part, to):
        send(part, xrecv.at[k, i, ih], hr.at[1 if k == 3 and (i, ih) in joined else 0, i, ih], me, tx(to))

    def join(i, ih):
        lead = 1 + (i + ih) % 2
        arrive(xrecv.at[3, i, ih], hr.at[1, i, ih])
        total = kq[i, ih, tx(3 - lead)] + xrecv[3, i, ih].astype(F32)
        xjoin[i, ih] = total.astype(BF16)
        pass_part(3 - lead, i, ih, xjoin.at[i, ih], 3 - lead)

    def forward(i, ih, extra=None):
        arrive(yrecv.at[i, ih], yr.at[i, ih])
        for t in range(m):
            at = slice(t * g, (t + 1) * g)
            total = kq[i, ih, t] + yrecv[i, ih, :, at].astype(F32)
            if extra is not None:
                total += extra[:, at]
            kq[i, ih, t] = total
            xsend[i, ih, t] = total.astype(BF16)
        if (i, ih) not in joined:
            for k in (3, 1, 2):
                pass_part(k, i, ih, xsend.at[i, ih, tx(k)], k)
        else:
            lead = 1 + (i + ih) % 2
            pass_part(3, i, ih, xsend.at[i, ih, tx(3)], lead)
            pass_part(lead, i, ih, xsend.at[i, ih, tx(lead)], lead)

    def settle(i, ih):
        total = kq[i, ih, tp]
        many = 2 if (i, ih) in joined else m - 1
        arrive(xrecv.at[pl.ds(1, many), i, ih], hr.at[0, i, ih])
        for k in (1, 2) if (i, ih) in joined else range(1, m):
            total += xrecv[k, i, ih].astype(F32)
        pbuf[i, ih] = total.reshape(2, 2 * rows, g)
        for k in (2, 3) if ih == 0 else (1,):
            zsend[k, i] = pbuf[i, ih, lax.rem(zp(k), 2)].astype(BF16)

    def away(k, i):
        send(zsend.at[k, i], zrecv.at[k, i], gr.at[0], 2 * zp(k) + c, tp)

    pltpu.make_async_copy(wd, wd, lw.at[lw.shape[0] - 1]).wait()
    with jax.named_scope("down_far"):
        activate(0)
        down(0)
        activate(1)
    def dense_pass():
        for k in (1, 2, 3):
            slot = 2 * zp(k) + c
            arrive(dall.at[slot], cr.at[k])
            send(dall.at[slot], dall.at[slot], er.at[0], mate, tp)

    def dense_ready():
        arrive(dall.at[pl.ds(0, zs)], er.at[0])

    def dense_forward(ih):
        s = 1 - side if ih == 0 else side
        x = dall[pl.ds(s * zs, zs)].reshape(half, h)
        forward(m - 1, ih, dot(x, dd[...]) * branch[ih])

    def leave(i, ih):
        settle(i, ih)
        for k in (3, 2) if ih == 0 else (1,):
            away(k, i)

    with jax.named_scope("tail"):
        with jax.named_scope("f00"):
            forward(0, 0)
        with jax.named_scope("f10"):
            forward(1, 0)
        with jax.named_scope("f20"):
            forward(2, 0)
        with jax.named_scope("d1"):
            down(1)
        with jax.named_scope("f01"):
            forward(0, 1)
        with jax.named_scope("f11"):
            forward(1, 1)
        with jax.named_scope("f21"):
            forward(2, 1)
        with jax.named_scope("l00"):
            leave(0, 0)
        with jax.named_scope("dp"):
            dense_pass()
        with jax.named_scope("l10"):
            leave(1, 0)
        with jax.named_scope("l20"):
            leave(2, 0)
        with jax.named_scope("dr"):
            dense_ready()
        with jax.named_scope("df0"):
            dense_forward(0)
        with jax.named_scope("df1"):
            dense_forward(1)
        with jax.named_scope("j01"):
            join(0, 1)
        with jax.named_scope("j11"):
            join(1, 1)
        with jax.named_scope("j21"):
            join(2, 1)
        with jax.named_scope("l30"):
            leave(3, 0)
        with jax.named_scope("l01"):
            leave(0, 1)
        with jax.named_scope("l11"):
            leave(1, 1)
        with jax.named_scope("l21"):
            leave(2, 1)
        with jax.named_scope("l31"):
            leave(3, 1)

    with jax.named_scope("last_sum"):
        arrive(zrecv.at[pl.ds(1, zs - 1)], gr.at[0])
        spot = lax.rem(z, 2)
        for j in range(m):
            total = pbuf[lax.rem(j - z - 1 + 2 * m, m), 1, spot]
            for k in range(1, zs):
                total += zrecv[k, lax.rem(j - zp(k) - 1 + 2 * m, m)].astype(F32)
            resid = full[tp, 2 * j + c, side, pl.ds(pl.multiple_of(2 * rows * spot, rows), 2 * rows), :]
            total = (total + resid.astype(F32)).astype(BF16)
            for core in range(2):
                fblk[core, j] = total[core * rows : (core + 1) * rows]
    with jax.named_scope("last_gather"):
        for k in (3, 1, 2, 0):
            for dc in range(2):
                if k or dc:
                    core = c if dc == 0 else 1 - c
                    send(
                        fblk.at[core], fin.at[c * m + tp], fr.at[0], 2 * z + core, tx(k)
                    )
        fin[c * m + tp] = fblk[c]
        arrive(fin.at[pl.ds(0, 2 * m - 1)], fr.at[0])
        for core in range(2):
            for t in range(m):
                for j in range(m):
                    base = (2 * j + core) * q + t * g
                    out[:, base : base + g] = fin[core * m + t, j]
    with jax.named_scope("drain"):
        for cp in sends:
            cp.wait_send()


def deliver_kernel(a, b, c, to_a, to_b, to_c, sems):
    copies = [
        pltpu.make_async_copy(src, dst, sems.at[i])
        for i, (src, dst) in enumerate(((a, to_a), (b, to_b), (c, to_c)))
    ]
    for cp in copies:
        cp.start()
    for cp in copies:
        cp.wait()


def in_kernel(
    n, m, tokens, recur_state, conv_state, mix_gain, in_weight, gate_weight, conv_taps,
    recur_gate_blocks, input_gate_blocks, decay_rate, out_weight, ffn_gain, router_weight, routes,
    expert_gate, expert_up, expert_down, dense_gate, dense_up, dense_down, branch_gate,
):
    rows, width = tokens.shape
    q, ch = in_weight.shape
    experts = router_weight.shape[1]
    h, f = dense_gate.shape[1], expert_down.shape[1]
    g, zs, b = q // m, n // 2, n * rows
    half = b // 2
    lines = 2 * experts
    past = (conv_state.shape[1], rows, ch)
    hbm = pl.BlockSpec(memory_space=pl.ANY)
    vm = pl.BlockSpec(memory_space=pltpu.VMEM)
    v = pltpu.VMEM

    def flags(*shapes):
        return [pltpu.SemaphoreType.DMA(s) for s in shapes]

    operands = (
        tokens, mix_gain.reshape(n, 1, q), ffn_gain.reshape(n, 1, q), routes.T, recur_state,
        conv_state.transpose(1, 0, 2), conv_taps, recur_gate_blocks, input_gate_blocks,
        decay_rate.reshape(1, ch), router_weight.T, branch_gate,
        in_weight, gate_weight, out_weight, dense_gate, dense_up, dense_down,
        expert_gate.reshape(n, q, f), expert_up.reshape(n, q, f), expert_down[0],
    )
    results = (
        jax.ShapeDtypeStruct((rows, width), BF16),
        jax.ShapeDtypeStruct((rows, ch), F32),
        jax.ShapeDtypeStruct(past, BF16),
    )
    layer_out, new_state, window = pl.pallas_call(
        functools.partial(layer_kernel, n, m, experts),
        out_shape=tuple(pltpu.VMEM(r.shape, r.dtype) for r in results),
        in_specs=[hbm] * len(operands),
        out_specs=(vm, vm, vm),
        scratch_shapes=[
            v((rows, width), BF16), v((n, 1, q), F32), v((n, 1, q), F32), v(routes.shape[::-1], jnp.int32),
            v((rows, ch), F32), v(past, BF16), v(conv_taps.shape, F32),
            v(recur_gate_blocks.shape, BF16), v(input_gate_blocks.shape, BF16), v((1, ch), F32),
            v((experts, width), BF16), v((width,), BF16), v((lines, width), BF16), v((q, ch), BF16), v((q, ch), BF16), v((ch, q), BF16),
            v((q, h), BF16), v((q, h), BF16), v((h, q), BF16),
            v((n, q, f), BF16), v((n, q, f), BF16), v((n, f, q), BF16),
            v((n, rows, q), BF16), v((zs, rows, 2 * ch), BF16), v((zs, rows, 2 * ch), BF16),
            v((zs, rows, 2 * ch), F32), v((zs, rows, 2 * ch), BF16), v((zs, rows, 2 * ch), BF16),
            v((rows, ch), F32), v((ch // LANES, LANES, 2 * LANES), BF16),
            v((lines, half), BF16), v((n, lines, half), BF16),
            v((rows, ch), BF16), v((n, rows, ch), BF16),
            v((m, 2, half, g), BF16), v((m, 2, half, g), BF16),
            v((m, n, 2, half, g), BF16), v((2, half, q), BF16),
            v((2, half, g), F32), v((2, half, lines), F32),
            v((2, half, f), F32), v((2, half, f), F32), v((2, half, f), BF16),
            v((zs, rows, 2 * h), BF16), v((zs, rows, 2 * h), BF16), v((zs, rows, 2 * h), F32),
            v((zs, rows, 2 * h), BF16), v((zs, rows, 2 * h), BF16),
            v((rows, h), BF16), v((n, rows, h), BF16),
            v((m, 2, half, q), BF16), v((m, 2, half, q), BF16), v((m, 2, m, half, g), F32),
            v((m, 2, m, half, g), BF16), v((m, m, 2, half, g), BF16), v((m - 1, 2, half, g), BF16),
            v((m, 2, 2, 2 * rows, g), F32),
            v((zs, m, 2 * rows, g), BF16), v((zs, m, 2 * rows, g), BF16),
            v((2, m, rows, g), BF16), v((2 * m, m, rows, g), BF16),
        ]
        + flags(
            (21,), (1,), (zs,), (1,), (zs,), (zs,), (zs,), (2,), (2,), (zs, 2), (m - 1, zs, 2), (zs, 2),
            (zs,), (zs,), (zs,), (1,), (m, 2), (2, m, 2), (1,), (1,),
        ),
        compiler_params=pltpu.CompilerParams(
            collective_id=0, has_side_effects=True, vmem_limit_bytes=58 * 1024 * 1024
        ),
        name="layer",
    )(*operands)
    held = [pltpu.with_memory_space_constraint(a, pltpu.VMEM) for a in (layer_out, new_state, window)]
    layer_out, new_state, window = pl.pallas_call(
        deliver_kernel,
        out_shape=results,
        in_specs=[vm] * 3,
        out_specs=(hbm,) * 3,
        scratch_shapes=[pltpu.SemaphoreType.DMA((3,))],
        name="deliver",
    )(*held)
    return (layer_out, new_state, window.transpose(1, 0, 2))


def solution(mesh):
    in_specs = (
        P("ep", None),
        P("ep", "tp"),
        P("ep", None, "tp"),
        P(),
        P("ep", "tp"),
        P("ep", "tp"),
        P(None, "tp"),
        P("tp", None, None),
        P("tp", None, None),
        P("tp"),
        P("tp", "ep"),
        P(),
        P(),
        P("ep", None),
        P("ep", None, "tp"),
        P("ep", None, "tp"),
        P("ep", "tp", None),
        P("ep", "tp"),
        P("ep", "tp"),
        P("tp", "ep"),
        P(),
    )
    out_specs = (P("ep", None), P("ep", "tp"), P("ep", None, "tp"))
    n, m = mesh.shape["ep"], mesh.shape["tp"]

    def body(*args):
        tokens, blocks, router, dense = args[0], args[7], args[12], args[17]
        q = tokens.shape[1] // n
        fits = m == 4 and n == 2 * m and n == router.shape[1] and q % (m * LANES) == 0
        fits = fits and tokens.shape[0] % 16 == 0 and dense.shape[1] % LANES == 0
        fits = fits and LANES % blocks.shape[1] == 0
        if fits:
            return in_kernel(n, m, *args)
        return on_device(*args)

    return jax.shard_map(
        body, mesh=mesh, in_specs=in_specs, out_specs=out_specs, check_vma=False
    )
```
